512 devices in a mesh: sp: 64 (over z, y), fs: 4 (over x), tp: 2 (over core).
Axes of the slice: x: 4, y: 8, z: 8, core: 2. Of those that a mesh axis runs over, the one named last changes fastest.
Arguments:
- tokens: bfloat16 [32768, 2048], P(('fs', 'sp'), 'tp'), parts along dimension 0, may hold values from -450 to 450
- documents: int32 [32768], P(('fs', 'sp')), parts along dimension 0, may hold values from 0 to 7, never falling along the last dimension, each value on 1 to 4096 neighbouring positions
- norm_gain: bfloat16 [2048], P('tp'), may hold values from 0.099609375 to 1.8984375
- out_gate_weight: bfloat16 [2048, 1024], P('sp', 'tp'), may hold values from -0.125 to 0.125
- in_gate_weight: bfloat16 [2048, 1024], P('sp', 'tp'), may hold values from -0.125 to 0.125
- value_weight: bfloat16 [2048, 1024], P('sp', 'tp'), may hold values from -0.125 to 0.125
- conv_taps: bfloat16 [3, 1024], P(None, 'tp'), may hold values from -3.5 to 3.5
- state_in_weight: bfloat16 [2048, 1024], P('sp', 'tp'), may hold values from -0.125 to 0.125
- decay_rate: float32 [64, 64], P('tp'), may hold values from 4e-05 to 2.01
- frequency: float32 [64, 64], P('tp'), may hold values from 0 to 32
- step_log: float32 [64], P('tp'), may hold values from -3.9121 to -1.6094
- input_real: float32 [64, 64, 16], P('tp'), may hold values from -1 to 1
- input_imag: float32 [64, 64, 16], P('tp'), may hold values from -1 to 1
- readout_real: float32 [64, 16, 64], P('tp'), may hold values from -0.75 to 0.75
- readout_imag: float32 [64, 16, 64], P('tp'), may hold values from -0.75 to 0.75
- skip_gain: float32 [1024], P('tp'), may hold values from -4 to 4
- conv_out_weight: bfloat16 [1024, 2048], P('tp', 'sp'), may hold values from -0.125 to 0.125
- state_out_weight: bfloat16 [1024, 2048], P('tp', 'sp'), may hold values from -0.125 to 0.125
Outputs:
- mixed: bfloat16 [32768, 2048], P(('fs', 'sp', 'tp')), parts along dimension 0
The draws below stay inside these ranges and needn't reach their ends.
There are 4 independent parts, one for each index of `fs`. The reference program is written for one: setup_inputs(seed, part) draws one part's arguments, and reference() takes and returns one part's arrays. A program takes and returns all parts, laid end to end along the dimension named above; an argument that names none is the same for every part. Nothing has to cross between parts.
All inputs are finite; a program needn't handle non-finite values.
Results may differ from the reference program's by a relative error of at most 0.015.
Values may be sent and summed in bfloat16 or wider, within the bound.
A program may use at most 64 MiB of HBM per device.

```python
import math
import jax
import jax.numpy as jnp
import numpy as np
from jax import lax

D = 2048
CONV = 1024
SSM = 1024
GROUP = 16
STATE = 64
TAPS = 3
BLOCK = 64
TOKENS = 8192
GROUPS = 64
DOCS = 8
DOC_MOST = 4096
N_TP = 2


def draw_tokens(key, part):
    streams = jax.random.split(jax.random.fold_in(key, 11), 4)
    noise = jnp.clip(jax.random.normal(streams[0], (TOKENS, D), jnp.float32), -5.0, 5.0)
    row_scale = jnp.exp(jax.random.uniform(streams[1], (TOKENS, 1), jnp.float32, 0.0, math.log(10.0)))
    col_scale = jnp.exp(jax.random.uniform(streams[2], (1, D), jnp.float32, 0.0, math.log(3.0)))
    upper_half = jnp.arange(D) >= D // 2
    swapped = jax.random.bernoulli(streams[3])
    half_scale = jnp.where(jnp.logical_xor(upper_half, swapped), 3.0, 1.0)
    return (noise * row_scale * col_scale * half_scale[None, :]).astype(jnp.bfloat16)


def rate_table(key):
    streams = jax.random.split(jax.random.fold_in(key, 23), 4)
    step_log = jax.random.uniform(streams[0], (GROUPS,), jnp.float32, math.log(0.02), math.log(0.2))
    share = 0.5
    slow_mask = jax.random.uniform(streams[1], (GROUPS, 1), jnp.float32) < share
    slow_part = jnp.exp(jax.random.uniform(streams[2], (GROUPS, STATE), jnp.float32, math.log(1e-05), math.log(5e-05)))
    fast_part = jnp.exp(jax.random.uniform(streams[3], (GROUPS, STATE), jnp.float32, math.log(0.02), math.log(0.04)))
    product = jnp.where(slow_mask, slow_part, fast_part)
    return (step_log, product / jnp.exp(step_log)[:, None])


def draw_step_log(key, part):
    return rate_table(key)[0]


def draw_decay_rate(key, part):
    return rate_table(key)[1]


def block_levels(key, dims, cuts, low, high):
    loudness, own = 1.0, jax.random.fold_in(key, 6)
    for position, parts in cuts:
        draws = jnp.exp(jax.random.uniform(jax.random.fold_in(own, position), (parts,), jnp.float32, low / len(cuts), high / len(cuts)))
        loudness = loudness * jnp.repeat(draws, dims[position] // parts).reshape([-1 if axis == position else 1 for axis in range(len(dims))])
    return loudness


def split_up(count, total, most, lean):
    loads = [(1 << 20) // math.isqrt(rank ** lean) + 1 for rank in range(2, count + 1)]
    surplus, given = total - most - (count - 1), [1] * (count - 1)
    while surplus > 0:
        candidates = [i for i in range(count - 1) if given[i] < most]
        whole, remaining = sum([loads[i] for i in candidates]), surplus
        for i in candidates:
            more = min(most - given[i], max(1, remaining * loads[i] // whole), surplus)
            given[i] = given[i] + more
            surplus = surplus - more
    return np.array([most] + given)


def uneven(rng, number_of, total, bound, lean):
    if number_of == 2:
        one = jax.random.randint(rng, (), max(1, total - bound), min(bound, total - 1) + 1)
        return jnp.stack([one, total - one])
    tallies = jnp.asarray(split_up(number_of, total, bound, lean), jnp.int32)
    pairs = (number_of - 1) // 2
    giver, receiver = tallies[1:1 + 2 * pairs:2], tallies[2:2 + 2 * pairs:2]
    room = jnp.minimum(giver - 1, bound - receiver)
    passed = jax.random.randint(jax.random.fold_in(rng, 1), (pairs,), 0, 1 << 20) % (room + 1)
    tallies = tallies.at[1:1 + 2 * pairs:2].set(giver - passed).at[2:2 + 2 * pairs:2].set(receiver + passed)
    return tallies[jax.random.permutation(jax.random.fold_in(rng, 2), number_of)]


def bell_draw(stream_key, shape, deviation, reach, cuts=(), held_as=jnp.bfloat16):
    values = deviation * jax.random.normal(stream_key, shape, jnp.float32)
    if cuts:
        values = values * block_levels(stream_key, shape, cuts, -0.22, 0.18)
    return jnp.clip(values, -reach, reach).astype(held_as)


def setup_inputs(seed: int = 0, part: int = 0) -> dict:
    key_list = jax.random.split(jax.random.key(seed), 19)
    part_keys = jax.random.split(jax.random.fold_in(key_list[18], part), 19)
    tokens = draw_tokens(jax.random.fold_in(jax.random.fold_in(key_list[18], part), 71), part)
    documents = jnp.searchsorted(jnp.cumsum(uneven(part_keys[1], DOCS, TOKENS, DOC_MOST, 0)), jnp.arange(TOKENS), side="right").astype(jnp.int32)
    norm_gain = jnp.clip(1.0 + 0.18 * jax.random.normal(key_list[2], (D,), jnp.float32), 0.099609375, 1.8984375).astype(jnp.bfloat16)
    out_gate_weight = bell_draw(key_list[3], (D, CONV), D ** -0.5, 0.125, ((0, 64), (1, 2)))
    in_gate_weight = bell_draw(key_list[4], (D, CONV), D ** -0.5, 0.125, ((0, 64), (1, 2)))
    value_weight = bell_draw(key_list[5], (D, CONV), D ** -0.5, 0.125, ((0, 64), (1, 2)))
    conv_taps = bell_draw(key_list[6], (TAPS, CONV), TAPS ** -0.5, 3.5, ((1, 2),))
    state_in_weight = bell_draw(key_list[7], (D, SSM), D ** -0.5, 0.125, ((0, 64), (1, 2)))
    decay_rate = draw_decay_rate(jax.random.fold_in(key_list[18], 71), part)
    frequency = jnp.clip(32.0 * jax.random.uniform(key_list[9], (GROUPS, STATE), jnp.float32) ** block_levels(key_list[9], (GROUPS, STATE), ((0, 2),), -0.2, 0.2), 0.0, 32.0)
    step_log = draw_step_log(jax.random.fold_in(key_list[18], 71), part)
    input_real = bell_draw(key_list[11], (GROUPS, STATE, GROUP), (2 * GROUP) ** -0.5, 1.0, ((0, 2),), jnp.float32)
    input_imag = bell_draw(key_list[12], (GROUPS, STATE, GROUP), (2 * GROUP) ** -0.5, 1.0, ((0, 2),), jnp.float32)
    readout_real = bell_draw(key_list[13], (GROUPS, GROUP, STATE), STATE ** -0.5, 0.75, ((0, 2),), jnp.float32)
    readout_imag = bell_draw(key_list[14], (GROUPS, GROUP, STATE), STATE ** -0.5, 0.75, ((0, 2),), jnp.float32)
    skip_gain = bell_draw(key_list[15], (SSM,), 1.0, 4.0, ((0, 2),), jnp.float32)
    conv_out_weight = bell_draw(key_list[16], (CONV, D), (CONV + SSM) ** -0.5, 0.125, ((0, 2), (1, 64)))
    state_out_weight = bell_draw(key_list[17], (SSM, D), (CONV + SSM) ** -0.5, 0.125, ((0, 2), (1, 64)))
    return {"tokens": tokens, "documents": documents, "norm_gain": norm_gain, "out_gate_weight": out_gate_weight, "in_gate_weight": in_gate_weight, "value_weight": value_weight, "conv_taps": conv_taps, "state_in_weight": state_in_weight, "decay_rate": decay_rate, "frequency": frequency, "step_log": step_log, "input_real": input_real, "input_imag": input_imag, "readout_real": readout_real, "readout_imag": readout_imag, "skip_gain": skip_gain, "conv_out_weight": conv_out_weight, "state_out_weight": state_out_weight}


EPS = 1e-06

def pair_step(earlier, later):
    dec_real, dec_imag, sum_real, sum_imag = earlier
    late_dec_real, late_dec_imag, late_sum_real, late_sum_imag = later
    return (late_dec_real * dec_real - late_dec_imag * dec_imag, late_dec_real * dec_imag + late_dec_imag * dec_real, late_dec_real * sum_real - late_dec_imag * sum_imag + late_sum_real, late_dec_real * sum_imag + late_dec_imag * sum_real + late_sum_imag)

def ssm_constants(decay_rate, frequency, step_log, input_real, input_imag):
    step_size = jnp.exp(step_log)[:, None]
    damping = decay_rate * step_size
    turning = frequency * step_size
    fading = jnp.exp(-damping)
    coef_real = fading * jnp.cos(turning)
    coef_imag = fading * jnp.sin(turning)
    half_sine = jnp.sin(turning / 2.0)
    less_real = jnp.expm1(-damping) * jnp.cos(turning) - 2.0 * half_sine * half_sine
    denominator = decay_rate * decay_rate + frequency * frequency
    ratio_real = (-less_real * decay_rate + coef_imag * frequency) / denominator
    ratio_imag = (-coef_imag * decay_rate - less_real * frequency) / denominator
    bbar_real = ratio_real[..., None] * input_real - ratio_imag[..., None] * input_imag
    bbar_imag = ratio_real[..., None] * input_imag + ratio_imag[..., None] * input_real
    return (coef_real.reshape(-1), coef_imag.reshape(-1), bbar_real, bbar_imag)

def complex_scan(coef_real, coef_imag, bbar_real, bbar_imag, driven, keep_rows, carry_real, carry_imag, readout_real, readout_imag, block):
    groups, group_size, state_size = readout_real.shape
    row_count = driven.shape[0]
    blocks = row_count // block

    def one_block(carry, pieces):
        start_real, start_imag = carry
        inputs, keeps = pieces
        split_rows = inputs.reshape(block, groups, group_size)
        push_real = jnp.einsum('tgh,gph->tgp', split_rows, bbar_real, precision=lax.Precision.HIGHEST).reshape(block, groups * state_size)
        push_imag = jnp.einsum('tgh,gph->tgp', split_rows, bbar_imag, precision=lax.Precision.HIGHEST).reshape(block, groups * state_size)
        dec_real = coef_real[None, :] * keeps[:, None]
        dec_imag = coef_imag[None, :] * keeps[:, None]
        prod_real, prod_imag, sum_real, sum_imag = lax.associative_scan(pair_step, (dec_real, dec_imag, push_real, push_imag), axis=0)
        held_real = sum_real + prod_real * start_real[None, :] - prod_imag * start_imag[None, :]
        held_imag = sum_imag + prod_real * start_imag[None, :] + prod_imag * start_real[None, :]
        result = jnp.einsum('tgp,ghp->tgh', held_real.reshape(block, groups, state_size), readout_real, precision=lax.Precision.HIGHEST)
        result = result - jnp.einsum('tgp,ghp->tgh', held_imag.reshape(block, groups, state_size), readout_imag, precision=lax.Precision.HIGHEST)
        return ((held_real[-1], held_imag[-1]), result.reshape(block, groups * group_size))
    _, outputs = lax.scan(one_block, (carry_real, carry_imag), (driven.reshape(blocks, block, -1), keep_rows.reshape(blocks, block)))
    return outputs.reshape(row_count, groups * group_size)

def reference(tokens, documents, norm_gain, out_gate_weight, in_gate_weight, value_weight, conv_taps, state_in_weight, decay_rate, frequency, step_log, input_real, input_imag, readout_real, readout_imag, skip_gain, conv_out_weight, state_out_weight):
    values = tokens.astype(jnp.float32)
    scale = lax.rsqrt(lax.optimization_barrier(jnp.mean(values * values, axis=1, keepdims=True)) + EPS)
    normed = (values * scale * norm_gain.astype(jnp.float32)).astype(jnp.bfloat16)
    out_gate = jnp.dot(normed, out_gate_weight, preferred_element_type=jnp.float32).astype(jnp.bfloat16)
    in_gate = jnp.dot(normed, in_gate_weight, preferred_element_type=jnp.float32).astype(jnp.bfloat16)
    value = jnp.dot(normed, value_weight, preferred_element_type=jnp.float32).astype(jnp.bfloat16)
    driven = jnp.dot(normed, state_in_weight, preferred_element_type=jnp.float32).astype(jnp.bfloat16)
    product = (in_gate.astype(jnp.float32) * value.astype(jnp.float32)).astype(jnp.bfloat16)
    margin = TAPS - 1
    padded = jnp.concatenate([jnp.zeros((margin, product.shape[1]), jnp.bfloat16), product], axis=0)
    padded_docs = jnp.concatenate([jnp.full((margin,), -1, jnp.int32), documents], axis=0)
    total = jnp.zeros(product.shape, jnp.float32)
    for index in range(TAPS):
        same_doc = (padded_docs[index:index + TOKENS] == documents).astype(jnp.float32)
        total = total + conv_taps[index].astype(jnp.float32)[None, :] * padded[index:index + TOKENS].astype(jnp.float32) * same_doc[:, None]
    conv_out = (out_gate.astype(jnp.float32) * total).astype(jnp.bfloat16)
    coef_real, coef_imag, bbar_real, bbar_imag = ssm_constants(decay_rate, frequency, step_log, input_real, input_imag)
    keep_rows = jnp.concatenate([jnp.zeros((1,), jnp.float32), (documents[1:] == documents[:-1]).astype(jnp.float32)], axis=0)
    driven_wide = driven.astype(jnp.float32)
    zero_state = jnp.zeros(coef_real.shape, jnp.float32)
    readout = complex_scan(coef_real, coef_imag, bbar_real, bbar_imag, driven_wide, keep_rows, zero_state, zero_state, readout_real, readout_imag, BLOCK)
    ssm_out = jax.nn.gelu(readout + skip_gain[None, :] * driven_wide, approximate=True).astype(jnp.bfloat16)
    conv_width = CONV // N_TP
    ssm_width = SSM // N_TP
    summed = jnp.zeros((TOKENS, D), jnp.float32)
    for index in range(N_TP):
        conv_part = jnp.dot(conv_out[:, index * conv_width:(index + 1) * conv_width], conv_out_weight[index * conv_width:(index + 1) * conv_width], preferred_element_type=jnp.float32)
        ssm_part = jnp.dot(ssm_out[:, index * ssm_width:(index + 1) * ssm_width], state_out_weight[index * ssm_width:(index + 1) * ssm_width], preferred_element_type=jnp.float32)
        summed = summed + (conv_part + ssm_part).astype(jnp.bfloat16).astype(jnp.float32)
    return summed.astype(jnp.bfloat16)
```

```python
import functools

import jax
import jax.numpy as jnp
from jax import lax
from jax.experimental import pallas as pl
from jax.experimental.pallas import tpu as pltpu
from jax.sharding import Mesh
from jax.sharding import PartitionSpec as P

SP = ("sp_0", "sp_1")
FS_SP = ("fs", "sp_0", "sp_1")
FS_SP_TP = ("fs", "sp_0", "sp_1", "tp")
EPS = 1e-06
PARTS = 4
ROWS = 128
LANES = 128
STATES = 512
ALL = PARTS * ROWS
BF16 = jnp.bfloat16
F32 = jnp.float32


def nn(a, b):
    return jnp.dot(a, b, preferred_element_type=F32)


def nt(a, b):
    return lax.dot_general(a, b, (((1,), (1,)), ((), ())), preferred_element_type=F32)


def ones_where(mask):
    return jnp.where(mask, 1.0, 0.0)


def mixer_kernel(
    nz, ny, depth, tok_in, w_in, doc_in, gain_in, in_ri, read_ri, lam, chan, out,
    tok, gains, docs, wall, wpeer, normed, perm, unperm, bmat, rmat, driven, pushed,
    docext, prodext, gate, ends, chain1, chain2, links, rim_out, rim_in, acts, pacts,
    part, relay, final, local_sem, tok_s, tok_r, d2d_s, d2d_r, doc_s, doc_r, one_s, one_r,
    ph_s, ph_r, st_s, st_r, ring_s, ring_r, ch_s, ch_r, rs_s, rs_r,
):
    z, y = lax.axis_index("sp_0"), lax.axis_index("sp_1")
    x, c = lax.axis_index("fs"), lax.axis_index("tp")
    half = depth // 2
    other = 1 - c
    sent = []

    def wrap(v, n):
        return lax.rem(v + 4 * n, n)

    def send(src, dst, ssem, rsem, **where):
        names = {"z": "sp_0", "y": "sp_1", "x": "fs", "c": "tp"}
        copy = pltpu.make_async_remote_copy(
            src_ref=src, dst_ref=dst, send_sem=ssem, recv_sem=rsem,
            device_id={names[k]: v for k, v in where.items()},
            device_id_type=pl.DeviceIdType.MESH,
        )
        copy.start()
        sent.append(copy)

    def arrived(dst, rsem):
        pltpu.make_async_copy(dst, dst, rsem).wait()

    xp, xm, xo = wrap(x + 1, PARTS), wrap(x - 1, PARTS), wrap(x + 2, PARTS)
    here = z * ny + y
    after, before = wrap(here + 1, nz * ny), wrap(here - 1, nz * ny)
    after_z, after_y = lax.div(after, ny), lax.rem(after, ny)
    before_z, before_y = lax.div(before, ny), lax.rem(before, ny)

    barrier = pltpu.get_barrier_semaphore()
    count = 0

    def greet(**where):
        names = {"z": "sp_0", "y": "sp_1", "x": "fs", "c": "tp"}
        pl.semaphore_signal(
            barrier, inc=1, device_id={names[k]: v for k, v in where.items()},
            device_id_type=pl.DeviceIdType.MESH,
        )
        return 1

    for d in range(1, ny):
        count += greet(y=wrap(y + d, ny))
    for d in range(1, nz):
        count += greet(z=wrap(z + d, nz))
    for v in (xp, xm, xo):
        count += greet(x=v)
    count += greet(c=other)
    count += greet(z=after_z, y=after_y)
    count += greet(z=before_z, y=before_y)

    local = [
        pltpu.make_async_copy(tok_in, tok.at[x, c], local_sem.at[0]),
        pltpu.make_async_copy(w_in, wall.at[z, y], local_sem.at[1]),
        pltpu.make_async_copy(doc_in, docs.at[x], local_sem.at[2]),
        pltpu.make_async_copy(gain_in, gains.at[c], local_sem.at[3]),
    ]
    for copy in local:
        copy.start()
    for copy in local:
        copy.wait()
    pl.semaphore_wait(barrier, count)

    low, high = pl.ds(0, ROWS // 2), pl.ds(ROWS // 2, ROWS // 2)

    def token_send(block, rows, way):
        ref = tok.at[block, c, rows]
        return ref, (xp if way == 0 else xm)

    def token_start(block, rows, way, turn):
        ref, target = token_send(block, rows, way)
        send(ref, ref, tok_s.at[way, turn], tok_r.at[way, turn], x=target)

    def token_wait(block, rows, way, turn):
        arrived(tok.at[block, c, rows], tok_r.at[way, turn])

    def pass_over(block, turn):
        ref = tok.at[block, c]
        send(ref, ref, d2d_s.at[turn], d2d_r.at[turn], c=other)

    def passed_over(block, turn):
        arrived(tok.at[block, other], d2d_r.at[turn])

    for turn, v in enumerate((xp, xm, xo)):
        send(docs.at[x], docs.at[x], doc_s.at[turn], doc_r.at[turn], x=v)
    send(gains.at[c], gains.at[c], one_s.at[0], one_r.at[0], c=other)
    token_start(x, low, 0, 0)
    token_start(x, high, 1, 0)
    rows_a, rows_b = pl.ds(0, half), pl.ds(half, half)
    for d in range(1, ny):
        ref = wall.at[z, y, rows_a]
        send(ref, ref, ph_s.at[0, d], ph_r.at[0, d], y=wrap(y + d, ny))
    for d in range(1, nz):
        ref = wall.at[z, y, rows_b]
        send(ref, ref, ph_s.at[1, d], ph_r.at[1, d], z=wrap(z + d, nz))
    token_start(x, high, 0, 1)
    token_start(x, low, 1, 1)
    pass_over(x, 0)

    shape = (ALL, ALL)
    r, n = lax.broadcasted_iota(jnp.int32, shape, 0), lax.broadcasted_iota(jnp.int32, shape, 1)
    natural = (r & 3) * ROWS + ((r >> 2) & 7) * 16 + (r >> 5)
    perm[...] = ones_where(n == natural).astype(BF16)
    t = (r >> 8) * (ROWS // 2) + (r & 63)
    turned = (t & 15) * 32 + (t >> 4) * 4 + ((r >> 6) & 3)
    unperm[...] = ones_where(n == turned).astype(BF16)
    spread = ones_where(
        (lax.broadcasted_iota(jnp.int32, (16, LANES), 1) & 15)
        == lax.broadcasted_iota(jnp.int32, (16, LANES), 0)
    ).astype(BF16)
    own_group = ones_where(
        (lax.broadcasted_iota(jnp.int32, (STATES, LANES), 0) >> 6)
        == (lax.broadcasted_iota(jnp.int32, (STATES, LANES), 1) >> 4)
    )
    for k in range(2):
        bmat[k * STATES : (k + 1) * STATES] = (nn(in_ri[k].astype(BF16), spread) * own_group).astype(BF16)
    spread_p = ones_where(
        (lax.broadcasted_iota(jnp.int32, (64, STATES), 1) & 63)
        == lax.broadcasted_iota(jnp.int32, (64, STATES), 0)
    ).astype(BF16)
    own_state = ones_where(
        (lax.broadcasted_iota(jnp.int32, (LANES, STATES), 0) >> 4)
        == (lax.broadcasted_iota(jnp.int32, (LANES, STATES), 1) >> 6)
    )
    for k in range(2):
        rmat[:, k * STATES : (k + 1) * STATES] = (nn(read_ri[k].astype(BF16), spread_p) * own_state).astype(BF16)

    def ring_ref(ab, source, lanes, piece):
        count = (ny, nz)[ab]
        cut = {0: pl.ds(0, count), 1: pl.ds(0, count // 2), 2: pl.ds(count // 2, count // 2)}[piece]
        if ab == 0:
            return wall.at[source, cut, rows_a, lanes]
        return wall.at[cut, source, rows_b, lanes]

    lanes_of = (pl.ds(LANES, 3 * LANES), pl.ds(4 * LANES, 2 * LANES))

    def ring_piece(ab, k, way):
        size = (nz, ny)[ab]
        return 0 if k < size // 2 - 1 else 1 + way

    def ring_start(which, k):
        for ab in range(2):
            me, size = ((z, nz), (y, ny))[ab]
            if k >= size // 2:
                continue
            for way in range(2):
                sign = 1 - 2 * way
                ref = ring_ref(ab, wrap(me - sign * k, size), lanes_of[which], ring_piece(ab, k, way))
                target = wrap(me + sign, size)
                send(
                    ref, ref, ring_s.at[which, ab, way, k], ring_r.at[which, ab, way, k],
                    **{"zy"[ab]: target},
                )

    def ring_wait(which, k):
        for ab in range(2):
            me, size = ((z, nz), (y, ny))[ab]
            if k >= size // 2:
                continue
            for way in range(2):
                sign = 1 - 2 * way
                ref = ring_ref(ab, wrap(me - sign * (k + 1), size), lanes_of[which], ring_piece(ab, k, way))
                arrived(ref, ring_r.at[which, ab, way, k])

    token_wait(xm, low, 0, 0)
    token_start(xm, low, 0, 2)
    token_wait(xp, high, 1, 0)
    token_start(xp, high, 1, 2)

    first_lanes = pl.ds(0, LANES)
    for d in range(1, ny):
        arrived(wall.at[z, wrap(y - d, ny), rows_a], ph_r.at[0, d])
    for d in range(1, nz):
        ref = wall.at[z, :, rows_a, first_lanes]
        send(ref, ref, st_s.at[0, d], st_r.at[0, d], z=wrap(z + d, nz))
    for d in range(1, nz):
        arrived(wall.at[wrap(z - d, nz), y, rows_b], ph_r.at[1, d])
    for d in range(1, ny):
        ref = wall.at[:, y, rows_b, first_lanes]
        send(ref, ref, st_s.at[1, d], st_r.at[1, d], y=wrap(y + d, ny))
    ring_start(0, 0)
    ring_start(1, 0)

    arrived(gains.at[other], one_r.at[0])
    g_low, g_high = gains[0], gains[1]
    width = 2 * tok.shape[3]

    def norm(block):
        def some_rows(i, carry):
            rows = pl.ds(pl.multiple_of(i * 32, 32), 32)
            a, b = tok[block, 0, rows, :].astype(F32), tok[block, 1, rows, :].astype(F32)
            mean = (jnp.sum(a * a, axis=1, keepdims=True) + jnp.sum(b * b, axis=1, keepdims=True)) / width
            scale = lax.rsqrt(mean + EPS)
            target = pl.ds(pl.multiple_of(block * ROWS + i * 32, 32), 32)
            normed[target, : width // 2] = (a * scale * g_low).astype(BF16)
            normed[target, width // 2 :] = (b * scale * g_high).astype(BF16)
            return carry

        lax.fori_loop(0, ROWS // 32, some_rows, 0)

    passed_over(x, 0)
    norm(x)
    token_wait(xm, high, 0, 1)
    pass_over(xm, 1)
    token_wait(xp, low, 1, 1)
    pass_over(xp, 2)
    ring_wait(0, 0)
    ring_start(0, 1)
    passed_over(xm, 1)
    norm(xm)
    passed_over(xp, 2)
    norm(xp)
    ring_wait(1, 0)
    ring_start(1, 1)
    token_wait(xo, low, 0, 2)
    token_wait(xo, high, 1, 2)
    pass_over(xo, 3)

    for turn, v in enumerate((xm, xp, xo)):
        arrived(docs.at[v], doc_r.at[turn])
    row = lax.broadcasted_iota(jnp.int32, (ALL, ROWS), 0)
    lane = lax.broadcasted_iota(jnp.int32, (ALL, ROWS), 1)
    pick_t = ones_where(lane == ((row >> 2) & 7) * 16 + (row >> 5))
    part_row = lax.broadcasted_iota(jnp.int32, (ROWS, ROWS), 0)
    spread_docs = jnp.zeros((ROWS, ROWS), F32)
    for q in range(PARTS):
        spread_docs = jnp.where(part_row == q, docs[q], spread_docs)
    by_part = nt(pick_t.astype(BF16), spread_docs.astype(BF16))
    by_part = by_part * ones_where(lane == (row & 3))
    docext[64:] = nn(by_part.astype(BF16), jnp.ones((ROWS, LANES), BF16))
    docext[4:32] = docext[64 + 448 : 64 + 476]
    docext[36:64] = docext[64 + 480 : 64 + 508]

    passed_over(xo, 3)
    norm(xo)
    ring_wait(0, 1)
    ring_start(0, 2)

    for d in range(1, nz):
        arrived(wall.at[wrap(z - d, nz), :, rows_a, first_lanes], st_r.at[0, d])
    for d in range(1, ny):
        arrived(wall.at[:, wrap(y - d, ny), rows_b, first_lanes], st_r.at[1, d])
    total_depth = nz * ny * depth
    state_in = wall[:, :, :, :LANES].reshape(total_depth, LANES)
    in_order = nn(perm[...], nn(normed[...], state_in).astype(BF16))
    driven[...] = in_order
    pushed[...] = nt(in_order.astype(BF16), bmat[...])

    def lane_cut(k):
        return slice(k * LANES, (k + 1) * LANES), slice(STATES + k * LANES, STATES + (k + 1) * LANES)

    def rows_at(k):
        return slice(k * 32, (k + 1) * 32)

    def docs_at(k):
        return docext[64 + k * 32 : 96 + k * 32]

    for cut in range(STATES // LANES):
        re, im = lane_cut(cut)
        a_re, a_im = lam[0:1, re], lam[1:2, re]
        s_re, s_im = pushed[0:32, re], pushed[0:32, im]
        for k in range(1, 16):
            keep = ones_where(docs_at(k) == docs_at(k - 1))
            s_re, s_im = (
                pushed[rows_at(k), re] + keep * (a_re * s_re - a_im * s_im),
                pushed[rows_at(k), im] + keep * (a_re * s_im + a_im * s_re),
            )
            pushed[rows_at(k), re] = s_re
            pushed[rows_at(k), im] = s_im
    for seg in range(8):
        rows = slice(480 + seg * 4, 484 + seg * 4)
        ends[seg, 0:4, :STATES] = pushed[rows, :STATES]
        ends[seg, 4:8, :STATES] = pushed[rows, STATES:]
        last = docext[544 + seg * 4 : 548 + seg * 4]
        ends[seg, 0:4, STATES:] = last
        ends[seg, 4:8, STATES:] = last

    sign = jnp.where(lax.broadcasted_iota(jnp.int32, (8, STATES), 0) < 4, -1.0, 1.0)

    def joined(carry, piece, power):
        held, doc = carry
        now = piece[:, STATES:]
        link = ones_where(now == doc)
        link = jnp.concatenate([link] * (STATES // LANES), axis=1)
        a_re, a_im = lam[2 * power : 2 * power + 1, :], lam[2 * power + 1 : 2 * power + 2, :]
        moved = a_re * held + (a_im * sign) * pltpu.roll(held, 4, 0)
        return piece[:, :STATES] + link * moved, now

    def fold(carry, pieces, count, limit, power):
        def step(k, carry):
            new = joined(carry, pieces[k], power)
            return tuple(jnp.where(k < limit, a, b) for a, b in zip(new, carry))

        return lax.fori_loop(0, count, step, carry)

    nothing = (jnp.zeros((8, STATES), F32), jnp.full((8, LANES), -1.0, F32))
    end, end_doc = fold(nothing, ends, 8, 8, 1)
    chain1[y, :, :STATES] = end
    chain1[y, :, STATES:] = end_doc
    ring_wait(1, 1)
    ring_start(1, 2)
    for d in range(1, ny):
        send(chain1.at[y], chain1.at[y], ch_s.at[0, d], ch_r.at[0, d], y=wrap(y + d, ny))

    for k in range(2, max(nz, ny) // 2):
        ring_wait(0, k)
        ring_start(0, k + 1)
    if max(nz, ny) // 2 <= 2:
        pass
    conv_in = wall[:, :, :, LANES : 4 * LANES].reshape(total_depth, 3 * LANES)
    projected = nn(perm[...], nn(normed[...], conv_in).astype(BF16))
    gate[...] = projected[:, :LANES]
    prodext[64:] = (projected[:, LANES : 2 * LANES] * projected[:, 2 * LANES :]).astype(BF16).astype(F32)
    prodext[4:32] = prodext[64 + 448 : 64 + 476]
    prodext[36:64] = prodext[64 + 480 : 64 + 508]
    rim_out[0:4, :LANES] = prodext[64 + 476 : 64 + 480]
    rim_out[4:8, :LANES] = prodext[64 + 508 : 64 + 512]
    rim_out[0:4, LANES:] = docext[64 + 476 : 64 + 480]
    rim_out[4:8, LANES:] = docext[64 + 508 : 64 + 512]

    for d in range(1, ny):
        arrived(chain1.at[wrap(y - d, ny)], ch_r.at[0, d])
    end, end_doc = fold(nothing, chain1, ny, ny, 2)
    chain2[z, :, :STATES] = end
    chain2[z, :, STATES:] = end_doc
    send(rim_out, rim_in, one_s.at[1], one_r.at[1], z=after_z, y=after_y)
    for d in range(1, nz):
        send(chain2.at[z], chain2.at[z], ch_s.at[1, d], ch_r.at[1, d], z=wrap(z + d, nz))

    for k in range(2, max(nz, ny) // 2):
        ring_wait(1, k)
        ring_start(1, k + 1)
    out_lanes = lanes_of[1]
    send(wall.at[:, :, :, out_lanes], wpeer, one_s.at[2], one_r.at[2], c=other)

    arrived(rim_in, one_r.at[1])
    first = here == 0
    prodext[0:4] = rim_in[0:4, :LANES]
    prodext[32:36] = rim_in[4:8, :LANES]
    docext[0:4] = jnp.where(first, -1.0, rim_in[0:4, LANES:])
    docext[32:36] = jnp.where(first, -1.0, rim_in[4:8, LANES:])
    now = docext[64:]
    mixed = (
        chan[0:1] * prodext[0:ALL] * ones_where(docext[0:ALL] == now)
        + chan[1:2] * prodext[32 : 32 + ALL] * ones_where(docext[32 : 32 + ALL] == now)
        + chan[2:3] * prodext[64:]
    )
    conv_out = (gate[...] * mixed).astype(BF16)
    acts[:, :LANES] = nn(unperm[...], conv_out).astype(BF16)
    mine, theirs = (pl.ds(pl.multiple_of(v * (ALL // 2), ALL // 2), ALL // 2) for v in (c, other))
    conv_lanes, ssm_lanes = pl.ds(0, LANES), pl.ds(LANES, LANES)

    for d in range(1, nz):
        arrived(chain2.at[wrap(z - d, nz)], ch_r.at[1, d])
    send(acts.at[theirs, conv_lanes], pacts.at[:, conv_lanes], one_s.at[3], one_r.at[3], c=other)
    state = fold(nothing, chain2, nz, z, 3)
    state = fold(state, chain1, ny, y, 2)
    for seg in range(8):
        links[seg] = state[0]
        state = joined(state, ends[seg], 1)
    for seg in range(8):
        rim_state = slice(seg * 4, seg * 4 + 4)
        links[8 + seg // 2, (seg % 2) * 4 : (seg % 2) * 4 + 4] = links[seg, 0:4]
        links[12 + seg // 2, (seg % 2) * 4 : (seg % 2) * 4 + 4] = links[seg, 4:8]
    previous = docext[32:64]
    for cut in range(STATES // LANES):
        re, im = lane_cut(cut)
        a_re, a_im = lam[0:1, re], lam[1:2, re]
        w_re = links[8:12, :, re].reshape(32, LANES)
        w_im = links[12:16, :, re].reshape(32, LANES)
        for k in range(16):
            w_re, w_im = a_re * w_re - a_im * w_im, a_re * w_im + a_im * w_re
            reach = ones_where(docs_at(k) == previous)
            pushed[rows_at(k), re] = pushed[rows_at(k), re] + reach * w_re
            pushed[rows_at(k), im] = pushed[rows_at(k), im] + reach * w_im
    reading = nt(pushed[...].astype(BF16), rmat[...]) + chan[3:4] * driven[...]
    inner = 0.7978845608028654 * (reading + 0.044715 * (reading * reading * reading))
    ssm_out = (0.5 * reading * (1.0 + jnp.tanh(inner))).astype(BF16)
    acts[:, LANES:] = nn(unperm[...], ssm_out).astype(BF16)
    send(acts.at[theirs, ssm_lanes], pacts.at[:, ssm_lanes], one_s.at[4], one_r.at[4], c=other)

    arrived(wpeer, one_r.at[2])
    arrived(pacts.at[:, conv_lanes], one_r.at[3])
    columns = total_depth // 2
    own_weight = wall.at[:, :, :, out_lanes]
    arrived(pacts.at[:, ssm_lanes], one_r.at[4])
    for h in range(2):
        cut = slice(h * nz // 2, (h + 1) * nz // 2)
        total = nt(acts[mine, :], wall[cut, :, :, 4 * LANES :].reshape(columns, 2 * LANES))
        total = total + nt(pacts[...], wpeer[cut].reshape(columns, 2 * LANES))
        part[h] = total.astype(BF16).reshape(PARTS, ROWS // 2, columns)
        if h == 0:
            send(part.at[0, xo], relay.at[0], rs_s.at[0, 0], rs_r.at[0, 0], x=xp)
            send(part.at[0, xm], final.at[1, 0], rs_s.at[1, 1], rs_r.at[1, 1], x=xm)
        else:
            send(part.at[1, xo], relay.at[1], rs_s.at[1, 0], rs_r.at[1, 0], x=xm)
            send(part.at[1, xp], final.at[0, 1], rs_s.at[0, 1], rs_r.at[0, 1], x=xp)
    arrived(relay.at[0], rs_r.at[0, 0])
    part[0, xp] = (part[0, xp].astype(F32) + relay[0].astype(F32)).astype(BF16)
    send(part.at[0, xp], final.at[0, 0], rs_s.at[0, 2], rs_r.at[0, 2], x=xp)
    arrived(relay.at[1], rs_r.at[1, 0])
    part[1, xm] = (part[1, xm].astype(F32) + relay[1].astype(F32)).astype(BF16)
    send(part.at[1, xm], final.at[1, 1], rs_s.at[1, 2], rs_r.at[1, 2], x=xm)
    for h, turns in ((1, (1, 2)), (0, (2, 1))):
        arrived(final.at[0, h], rs_r.at[0, turns[0]])
        arrived(final.at[1, h], rs_r.at[1, turns[1]])
        value = part[h, x].astype(F32) + final[0, h].astype(F32) + final[1, h].astype(F32)
        out[:, h * columns : (h + 1) * columns] = value.astype(BF16)
    for copy in sent:
        copy.wait_send()


def state_tables(decay_rate, frequency, step_log, input_real, input_imag, lengths):
    step_size = jnp.exp(step_log)[:, None]
    damping = decay_rate * step_size
    turning = frequency * step_size
    fading = jnp.exp(-damping)
    coef_imag = fading * jnp.sin(turning)
    half_sine = jnp.sin(turning / 2.0)
    less_real = jnp.expm1(-damping) * jnp.cos(turning) - 2.0 * half_sine * half_sine
    denominator = decay_rate * decay_rate + frequency * frequency
    ratio_real = (-less_real * decay_rate + coef_imag * frequency) / denominator
    ratio_imag = (-coef_imag * decay_rate - less_real * frequency) / denominator
    bbar_real = ratio_real[..., None] * input_real - ratio_imag[..., None] * input_imag
    bbar_imag = ratio_real[..., None] * input_imag + ratio_imag[..., None] * input_real
    rows = []
    for length in lengths:
        fade = jnp.exp(-length * damping)
        rows += [fade * jnp.cos(length * turning), fade * jnp.sin(length * turning)]
    powers = jnp.stack(rows).reshape(len(rows), -1)
    bbar = jnp.stack([bbar_real, bbar_imag]).reshape(2, -1, input_real.shape[2])
    return powers, bbar


def shards(
    nz, ny, tokens, documents, norm_gain, out_gate_weight, in_gate_weight, value_weight,
    conv_taps, state_in_weight, decay_rate, frequency, step_log, input_real, input_imag,
    readout_real, readout_imag, skip_gain, conv_out_weight, state_out_weight,
):
    x = lax.axis_index("fs")
    depth = state_in_weight.shape[0]
    width = tokens.shape[1]

    def own(array, dim):
        size = array.shape[dim] // PARTS
        return lax.dynamic_slice_in_dim(array, x * size, size, dim)

    weights = jnp.concatenate(
        [own(w, 1) for w in (state_in_weight, out_gate_weight, in_gate_weight, value_weight)]
        + [own(w, 0).T for w in (conv_out_weight, state_out_weight)],
        axis=1,
    )
    powers, bbar = state_tables(
        own(decay_rate, 0), own(frequency, 0), own(step_log, 0), own(input_real, 0),
        own(input_imag, 0), (1.0, 16.0, float(ROWS), float(ROWS * ny)),
    )
    readout = jnp.stack([own(readout_real, 0), -own(readout_imag, 0)]).reshape(2, LANES, -1)
    channels = jnp.concatenate(
        [own(conv_taps, 1).astype(F32), own(skip_gain, 0)[None, :], jnp.zeros((4, LANES), F32)]
    )
    doc_row = documents.astype(F32)[None, :]
    gain_row = norm_gain.astype(F32)[None, :]
    columns = nz * ny * depth // 2
    vmem = pl.BlockSpec(memory_space=pltpu.VMEM)
    anywhere = pl.BlockSpec(memory_space=pl.ANY)
    dma = pltpu.SemaphoreType.DMA
    steps = max(nz, ny) // 2
    most = max(nz, ny)
    return pl.pallas_call(
        functools.partial(mixer_kernel, nz, ny, depth),
        out_shape=jax.ShapeDtypeStruct((ROWS // 2, 2 * columns), BF16),
        in_specs=[anywhere] * 4 + [vmem] * 4,
        out_specs=vmem,
        scratch_shapes=[
            pltpu.VMEM((PARTS, 2, ROWS, width), BF16),
            pltpu.VMEM((2, 1, width), F32),
            pltpu.VMEM((PARTS, 1, ROWS), F32),
            pltpu.VMEM((nz, ny, depth, 6 * LANES), BF16),
            pltpu.VMEM((nz, ny, depth, 2 * LANES), BF16),
            pltpu.VMEM((ALL, 2 * width), BF16),
            pltpu.VMEM((ALL, ALL), BF16),
            pltpu.VMEM((ALL, ALL), BF16),
            pltpu.VMEM((2 * STATES, LANES), BF16),
            pltpu.VMEM((LANES, 2 * STATES), BF16),
            pltpu.VMEM((ALL, LANES), F32),
            pltpu.VMEM((ALL, 2 * STATES), F32),
            pltpu.VMEM((64 + ALL, LANES), F32),
            pltpu.VMEM((64 + ALL, LANES), F32),
            pltpu.VMEM((ALL, LANES), F32),
            pltpu.VMEM((8, 8, STATES + LANES), F32),
            pltpu.VMEM((ny, 8, STATES + LANES), F32),
            pltpu.VMEM((nz, 8, STATES + LANES), F32),
            pltpu.VMEM((16, 8, STATES), F32),
            pltpu.VMEM((8, 2 * LANES), F32),
            pltpu.VMEM((8, 2 * LANES), F32),
            pltpu.VMEM((ALL, 2 * LANES), BF16),
            pltpu.VMEM((ALL // 2, 2 * LANES), BF16),
            pltpu.VMEM((2, PARTS, ROWS // 2, columns), BF16),
            pltpu.VMEM((2, ROWS // 2, columns), BF16),
            pltpu.VMEM((2, 2, ROWS // 2, columns), BF16),
            dma((4,)),
            dma((2, 3)), dma((2, 3)),
            dma((4,)), dma((4,)),
            dma((3,)), dma((3,)),
            dma((5,)), dma((5,)),
            dma((2, most)), dma((2, most)),
            dma((2, most)), dma((2, most)),
            dma((2, 2, 2, steps)), dma((2, 2, 2, steps)),
            dma((2, most)), dma((2, most)),
            dma((2, 3)), dma((2, 3)),
        ],
        compiler_params=pltpu.CompilerParams(
            collective_id=0, has_side_effects=True, vmem_limit_bytes=60 * 1024 * 1024
        ),
        name="mixer",
    )(tokens, weights, doc_row, gain_row, bbar, readout, powers, channels)


def solution(mesh, nz=8, ny=8):
    torus = Mesh(
        mesh.devices.reshape(nz, ny, mesh.shape["fs"], mesh.shape["tp"]), ("sp_0", "sp_1", "fs", "tp")
    )
    in_specs = (
        P(FS_SP, "tp"),
        P(FS_SP),
        P("tp"),
        P(SP, "tp"),
        P(SP, "tp"),
        P(SP, "tp"),
        P(None, "tp"),
        P(SP, "tp"),
        P("tp", None),
        P("tp", None),
        P("tp"),
        P("tp", None, None),
        P("tp", None, None),
        P("tp", None, None),
        P("tp", None, None),
        P("tp"),
        P("tp", SP),
        P("tp", SP),
    )
    return jax.shard_map(
        functools.partial(shards, nz, ny), mesh=torus, in_specs=in_specs,
        out_specs=P(FS_SP_TP, None), check_vma=False,
    )
```

```python
import functools

import jax
import jax.numpy as jnp
from jax import lax
from jax.experimental import pallas as pl
from jax.experimental.pallas import tpu as pltpu
from jax.sharding import Mesh
from jax.sharding import PartitionSpec as P

SP = ("sp_0", "sp_1")
FS_SP = ("fs", "sp_0", "sp_1")
FS_SP_TP = ("fs", "sp_0", "sp_1", "tp")
EPS = 1e-06
PARTS = 4
ROWS = 128
LANES = 128
STATES = 512
ALL = PARTS * ROWS
BF16 = jnp.bfloat16
F32 = jnp.float32


def nn(a, b):
    return jnp.dot(a, b, preferred_element_type=F32)


def nt(a, b):
    return lax.dot_general(a, b, (((1,), (1,)), ((), ())), preferred_element_type=F32)


def ones_where(mask):
    return jnp.where(mask, 1.0, 0.0)


def mixer_kernel(
    nz, ny, depth, tok_in, w_in_0, w_in_1, w_in_2, w_in_3, w_in_4, w_in_5, doc_in, gain_in,
    decay_in, freq_in, step_in, in_re, in_im, read_re, read_im, taps_in, skip_in, out,
    rates, step_row, mats, taps, skip, lam, tok, gains, docs, wall, wpeer, normed, perm, unperm, bmat, rmat, driven, pushed,
    docext, prodext, gate, ends, chain1, chain2, links, rim_out, rim_in, acts, pacts,
    part, relay, final, local_sem, tok_s, tok_r, d2d_s, d2d_r, doc_s, doc_r, one_s, one_r,
    ph_s, ph_r, st_s, st_r, ring_s, ring_r, ch_s, ch_r, rs_s, rs_r,
):
    z, y = lax.axis_index("sp_0"), lax.axis_index("sp_1")
    x, c = lax.axis_index("fs"), lax.axis_index("tp")
    half = depth // 2
    other = 1 - c
    sent, scopes = [], []

    def phase(name):
        if scopes:
            scopes.pop().__exit__(None, None, None)
        if name:
            scopes.append(jax.named_scope(name))
            scopes[-1].__enter__()

    def wrap(v, n):
        return lax.rem(v + 4 * n, n)

    def send(src, dst, ssem, rsem, **where):
        names = {"z": "sp_0", "y": "sp_1", "x": "fs", "c": "tp"}
        copy = pltpu.make_async_remote_copy(
            src_ref=src, dst_ref=dst, send_sem=ssem, recv_sem=rsem,
            device_id={names[k]: v for k, v in where.items()},
            device_id_type=pl.DeviceIdType.MESH,
        )
        copy.start()
        sent.append(copy)

    def arrived(dst, rsem):
        pltpu.make_async_copy(dst, dst, rsem).wait()

    xp, xm, xo = wrap(x + 1, PARTS), wrap(x - 1, PARTS), wrap(x + 2, PARTS)
    here = z * ny + y
    after, before = wrap(here + 1, nz * ny), wrap(here - 1, nz * ny)
    after_z, after_y = lax.div(after, ny), lax.rem(after, ny)
    before_z, before_y = lax.div(before, ny), lax.rem(before, ny)

    phase("greet")
    barrier = pltpu.get_barrier_semaphore()
    count = 0

    def greet(**where):
        names = {"z": "sp_0", "y": "sp_1", "x": "fs", "c": "tp"}
        pl.semaphore_signal(
            barrier, inc=1, device_id={names[k]: v for k, v in where.items()},
            device_id_type=pl.DeviceIdType.MESH,
        )
        return 1

    for d in range(1, ny):
        count += greet(y=wrap(y + d, ny))
    for d in range(1, nz):
        count += greet(z=wrap(z + d, nz))
    for v in (xp, xm, xo):
        count += greet(x=v)
    count += greet(c=other)
    count += greet(z=after_z, y=after_y)
    count += greet(z=before_z, y=before_y)

    own_channels = pl.ds(pl.multiple_of(x * LANES, LANES), LANES)
    own_groups = pl.ds(pl.multiple_of(x * 8, 8), 8)
    moves = [(tok_in, tok.at[x, c]), (doc_in, docs.at[x]), (gain_in, gains.at[c])]
    for k, w in enumerate((w_in_0, w_in_1, w_in_2, w_in_3, w_in_4, w_in_5)):
        moves.append((w.at[:, own_channels], wall.at[z, y, :, pl.ds(k * LANES, LANES)]))
    early = len(moves)
    moves += [(decay_in.at[own_groups], rates.at[0]), (freq_in.at[own_groups], rates.at[1])]
    moves += [(step_in, step_row), (taps_in.at[:, own_channels], taps), (skip_in.at[:, own_channels], skip)]
    for k, m in enumerate((in_re, in_im, read_re, read_im)):
        moves.append((m.at[own_groups], mats.at[k]))
    local = [pltpu.make_async_copy(a, b, local_sem.at[k]) for k, (a, b) in enumerate(moves)]
    for copy in local:
        copy.start()
    phase("enter")
    for copy in local[:early]:
        copy.wait()
    phase("barrier")
    pl.semaphore_wait(barrier, count)

    low, high = pl.ds(0, ROWS // 2), pl.ds(ROWS // 2, ROWS // 2)

    def token_send(block, rows, way):
        ref = tok.at[block, c, rows]
        return ref, (xp if way == 0 else xm)

    def token_start(block, rows, way, turn):
        ref, target = token_send(block, rows, way)
        send(ref, ref, tok_s.at[way, turn], tok_r.at[way, turn], x=target)

    def token_wait(block, rows, way, turn):
        arrived(tok.at[block, c, rows], tok_r.at[way, turn])

    def pass_over(block, turn):
        ref = tok.at[block, c]
        send(ref, ref, d2d_s.at[turn], d2d_r.at[turn], c=other)

    def passed_over(block, turn):
        arrived(tok.at[block, other], d2d_r.at[turn])

    phase("first_sends")
    for turn, v in enumerate((xp, xm, xo)):
        send(docs.at[x], docs.at[x], doc_s.at[turn], doc_r.at[turn], x=v)
    send(gains.at[c], gains.at[c], one_s.at[0], one_r.at[0], c=other)
    token_start(x, low, 0, 0)
    token_start(x, high, 1, 0)
    rows_a, rows_b = pl.ds(0, half), pl.ds(half, half)
    for d in range(1, ny):
        ref = wall.at[z, y, rows_a]
        send(ref, ref, ph_s.at[0, d], ph_r.at[0, d], y=wrap(y + d, ny))
    for d in range(1, nz):
        ref = wall.at[z, y, rows_b]
        send(ref, ref, ph_s.at[1, d], ph_r.at[1, d], z=wrap(z + d, nz))
    token_start(x, high, 0, 1)
    token_start(x, low, 1, 1)
    pass_over(x, 0)

    phase("tables")
    shape = (ALL, ALL)
    r, n = lax.broadcasted_iota(jnp.int32, shape, 0), lax.broadcasted_iota(jnp.int32, shape, 1)
    natural = (r & 3) * ROWS + ((r >> 2) & 7) * 16 + (r >> 5)
    perm[...] = ones_where(n == natural).astype(BF16)
    t = (r >> 8) * (ROWS // 2) + (r & 63)
    turned = (t & 15) * 32 + (t >> 4) * 4 + ((r >> 6) & 3)
    unperm[...] = ones_where(n == turned).astype(BF16)
    for copy in local[early:]:
        copy.wait()
    group = lax.broadcasted_iota(jnp.int32, (8, 32), 0) + x * 8
    step_log = jnp.broadcast_to(step_row[...], (8, 32))
    mine_only = lax.broadcasted_iota(jnp.int32, (8, 32), 1) == group
    step = jnp.exp(jnp.sum(jnp.where(mine_only, step_log, 0.0), axis=1, keepdims=True))
    decay, frequency = rates[0], rates[1]
    damping, turning = decay * step, frequency * step
    fading = jnp.exp(-damping)
    coef_real, coef_imag = fading * jnp.cos(turning), fading * jnp.sin(turning)
    half_sine = jnp.sin(turning * 0.5)
    series = jnp.ones_like(damping)
    for k in range(11, 1, -1):
        series = 1.0 - damping * (1.0 / k) * series
    less_real = -damping * series * jnp.cos(turning) - 2.0 * half_sine * half_sine
    denominator = decay * decay + frequency * frequency
    ratio_real = (-less_real * decay + coef_imag * frequency) / denominator
    ratio_imag = (-coef_imag * decay - less_real * frequency) / denominator

    def widened(value):
        value = jnp.concatenate([value, value], axis=1)
        return jnp.concatenate([value] * (STATES // LANES), axis=1)

    own_lane = (
        lax.broadcasted_iota(jnp.int32, (8, STATES), 1) >> 6
    ) == lax.broadcasted_iota(jnp.int32, (8, STATES), 0)

    def flat(value):
        return jnp.sum(jnp.where(own_lane, widened(value), 0.0), axis=0, keepdims=True)

    power_re, power_im, squared = coef_real, coef_imag, 1
    for index, length in enumerate((1, 16, ROWS, ROWS * ny)):
        while squared < length:
            power_re, power_im = power_re * power_re - power_im * power_im, 2.0 * power_re * power_im
            squared *= 2
        lam[2 * index : 2 * index + 1, :] = flat(power_re)
        lam[2 * index + 1 : 2 * index + 2, :] = flat(power_im)
    ratio_real, ratio_imag = flat(ratio_real), flat(ratio_imag)
    own_state = (lax.broadcasted_iota(jnp.int32, (LANES, STATES), 0) >> 4) == (
        lax.broadcasted_iota(jnp.int32, (LANES, STATES), 1) >> 6
    )
    input_real, input_imag = (widened(mats[k].reshape(LANES, 64)) for k in range(2))
    bmat[:, :STATES] = jnp.where(own_state, ratio_real * input_real - ratio_imag * input_imag, 0.0).astype(BF16)
    bmat[:, STATES:] = jnp.where(own_state, ratio_real * input_imag + ratio_imag * input_real, 0.0).astype(BF16)
    rmat[:, :STATES] = jnp.where(own_state, widened(mats[2].reshape(LANES, 64)), 0.0).astype(BF16)
    rmat[:, STATES:] = jnp.where(own_state, -widened(mats[3].reshape(LANES, 64)), 0.0).astype(BF16)

    def ring_ref(ab, source, lanes, piece):
        count = (ny, nz)[ab]
        cut = {0: pl.ds(0, count), 1: pl.ds(0, count // 2), 2: pl.ds(count // 2, count // 2)}[piece]
        if ab == 0:
            return wall.at[source, cut, rows_a, lanes]
        return wall.at[cut, source, rows_b, lanes]

    lanes_of = (pl.ds(LANES, 3 * LANES), pl.ds(4 * LANES, 2 * LANES))

    def ring_piece(ab, k, way):
        size = (nz, ny)[ab]
        return 0 if k < size // 2 - 1 else 1 + way

    def ring_start(which, k):
        for ab in range(2):
            me, size = ((z, nz), (y, ny))[ab]
            if k >= size // 2:
                continue
            for way in range(2):
                sign = 1 - 2 * way
                ref = ring_ref(ab, wrap(me - sign * k, size), lanes_of[which], ring_piece(ab, k, way))
                target = wrap(me + sign, size)
                send(
                    ref, ref, ring_s.at[which, ab, way, k], ring_r.at[which, ab, way, k],
                    **{"zy"[ab]: target},
                )

    def ring_wait(which, k):
        for ab in range(2):
            me, size = ((z, nz), (y, ny))[ab]
            if k >= size // 2:
                continue
            for way in range(2):
                sign = 1 - 2 * way
                ref = ring_ref(ab, wrap(me - sign * (k + 1), size), lanes_of[which], ring_piece(ab, k, way))
                arrived(ref, ring_r.at[which, ab, way, k])

    phase("tok_forward")
    token_wait(xm, low, 0, 0)
    token_start(xm, low, 0, 2)
    token_wait(xp, high, 1, 0)
    token_start(xp, high, 1, 2)

    phase("phase1_wait")
    first_lanes = pl.ds(0, LANES)
    for d in range(1, ny):
        arrived(wall.at[z, wrap(y - d, ny), rows_a], ph_r.at[0, d])
    for d in range(1, nz):
        ref = wall.at[z, :, rows_a, first_lanes]
        send(ref, ref, st_s.at[0, d], st_r.at[0, d], z=wrap(z + d, nz))
    for d in range(1, nz):
        arrived(wall.at[wrap(z - d, nz), y, rows_b], ph_r.at[1, d])
    for d in range(1, ny):
        ref = wall.at[:, y, rows_b, first_lanes]
        send(ref, ref, st_s.at[1, d], st_r.at[1, d], y=wrap(y + d, ny))
    ring_start(0, 0)
    ring_start(1, 0)

    phase("gain_wait")
    arrived(gains.at[other], one_r.at[0])
    g_low, g_high = gains[0].astype(F32), gains[1].astype(F32)
    width = 2 * tok.shape[3]

    def norm(block):
        def some_rows(i, carry):
            rows = pl.ds(pl.multiple_of(i * 32, 32), 32)
            a, b = tok[block, 0, rows, :].astype(F32), tok[block, 1, rows, :].astype(F32)
            mean = (jnp.sum(a * a, axis=1, keepdims=True) + jnp.sum(b * b, axis=1, keepdims=True)) / width
            scale = lax.rsqrt(mean + EPS)
            target = pl.ds(pl.multiple_of(block * ROWS + i * 32, 32), 32)
            normed[target, : width // 2] = (a * scale * g_low).astype(BF16)
            normed[target, width // 2 :] = (b * scale * g_high).astype(BF16)
            return carry

        lax.fori_loop(0, ROWS // 32, some_rows, 0)

    phase("norm_own")
    passed_over(x, 0)
    norm(x)
    phase("tok_wait1")
    token_wait(xm, high, 0, 1)
    pass_over(xm, 1)
    token_wait(xp, low, 1, 1)
    pass_over(xp, 2)
    phase("ring00")
    ring_wait(0, 0)
    ring_start(0, 1)
    phase("norm_mid")
    passed_over(xm, 1)
    norm(xm)
    passed_over(xp, 2)
    norm(xp)
    phase("ring10")
    ring_wait(1, 0)
    ring_start(1, 1)
    phase("tok_wait2")
    token_wait(xo, low, 0, 2)
    token_wait(xo, high, 1, 2)
    pass_over(xo, 3)

    phase("documents")
    for turn, v in enumerate((xm, xp, xo)):
        arrived(docs.at[v], doc_r.at[turn])
    row = lax.broadcasted_iota(jnp.int32, (ALL, ROWS), 0)
    lane = lax.broadcasted_iota(jnp.int32, (ALL, ROWS), 1)
    pick_t = ones_where(lane == ((row >> 2) & 7) * 16 + (row >> 5))
    part_row = lax.broadcasted_iota(jnp.int32, (ROWS, ROWS), 0)
    spread_docs = jnp.zeros((ROWS, ROWS), F32)
    for q in range(PARTS):
        spread_docs = jnp.where(part_row == q, docs[q].astype(F32), spread_docs)
    by_part = nt(pick_t.astype(BF16), spread_docs.astype(BF16))
    by_part = by_part * ones_where(lane == (row & 3))
    docext[64:] = nn(by_part.astype(BF16), jnp.ones((ROWS, LANES), BF16))
    docext[4:32] = docext[64 + 448 : 64 + 476]
    docext[36:64] = docext[64 + 480 : 64 + 508]

    phase("norm_last")
    passed_over(xo, 3)
    norm(xo)
    phase("ring01")
    ring_wait(0, 1)
    ring_start(0, 2)

    phase("state_w_wait")
    for d in range(1, nz):
        arrived(wall.at[wrap(z - d, nz), :, rows_a, first_lanes], st_r.at[0, d])
    for d in range(1, ny):
        arrived(wall.at[:, wrap(y - d, ny), rows_b, first_lanes], st_r.at[1, d])
    phase("state_in")
    total_depth = nz * ny * depth
    state_in = wall[:, :, :, :LANES].reshape(total_depth, LANES)
    in_order = nn(perm[...], nn(normed[...], state_in).astype(BF16))
    driven[...] = in_order
    pushed[...] = nn(in_order.astype(BF16), bmat[...])

    def lane_cut(k):
        return slice(k * LANES, (k + 1) * LANES), slice(STATES + k * LANES, STATES + (k + 1) * LANES)

    def rows_at(k):
        return slice(k * 32, (k + 1) * 32)

    def docs_at(k):
        return docext[64 + k * 32 : 96 + k * 32]

    phase("scan")
    for cut in range(STATES // LANES):
        re, im = lane_cut(cut)
        a_re, a_im = lam[0:1, re], lam[1:2, re]
        s_re, s_im = pushed[0:32, re], pushed[0:32, im]
        for k in range(1, 16):
            keep = ones_where(docs_at(k) == docs_at(k - 1))
            s_re, s_im = (
                pushed[rows_at(k), re] + keep * (a_re * s_re - a_im * s_im),
                pushed[rows_at(k), im] + keep * (a_re * s_im + a_im * s_re),
            )
            pushed[rows_at(k), re] = s_re
            pushed[rows_at(k), im] = s_im
    for seg in range(8):
        rows = slice(480 + seg * 4, 484 + seg * 4)
        ends[seg, 0:4, :STATES] = pushed[rows, :STATES]
        ends[seg, 4:8, :STATES] = pushed[rows, STATES:]
        last = docext[544 + seg * 4 : 548 + seg * 4]
        ends[seg, 0:4, STATES:] = last
        ends[seg, 4:8, STATES:] = last

    phase("fold_local")
    sign = jnp.where(lax.broadcasted_iota(jnp.int32, (8, STATES), 0) < 4, -1.0, 1.0)

    def joined(carry, piece, power):
        held, doc = carry
        now = piece[:, STATES:]
        link = ones_where(now == doc)
        link = jnp.concatenate([link] * (STATES // LANES), axis=1)
        a_re, a_im = lam[2 * power : 2 * power + 1, :], lam[2 * power + 1 : 2 * power + 2, :]
        moved = a_re * held + (a_im * sign) * pltpu.roll(held, 4, 0)
        return piece[:, :STATES] + link * moved, now

    def fold(carry, pieces, count, limit, power):
        def step(k, carry):
            new = joined(carry, pieces[k], power)
            return tuple(jnp.where(k < limit, a, b) for a, b in zip(new, carry))

        return lax.fori_loop(0, count, step, carry)

    nothing = (jnp.zeros((8, STATES), F32), jnp.full((8, LANES), -1.0, F32))
    end, end_doc = fold(nothing, ends, 8, 8, 1)
    chain1[y, :, :STATES] = end
    chain1[y, :, STATES:] = end_doc
    phase("ring11")
    ring_wait(1, 1)
    ring_start(1, 2)
    for d in range(1, ny):
        send(chain1.at[y], chain1.at[y], ch_s.at[0, d], ch_r.at[0, d], y=wrap(y + d, ny))

    phase("ring02_03")
    for k in range(2, max(nz, ny) // 2):
        ring_wait(0, k)
        ring_start(0, k + 1)
    if max(nz, ny) // 2 <= 2:
        pass
    phase("conv_in")
    conv_in = wall[:, :, :, LANES : 4 * LANES].reshape(total_depth, 3 * LANES)
    projected = nn(perm[...], nn(normed[...], conv_in).astype(BF16))
    gate[...] = projected[:, :LANES]
    prodext[64:] = (projected[:, LANES : 2 * LANES] * projected[:, 2 * LANES :]).astype(BF16).astype(F32)
    prodext[4:32] = prodext[64 + 448 : 64 + 476]
    prodext[36:64] = prodext[64 + 480 : 64 + 508]
    rim_out[0:4, :LANES] = prodext[64 + 476 : 64 + 480]
    rim_out[4:8, :LANES] = prodext[64 + 508 : 64 + 512]
    rim_out[0:4, LANES:] = docext[64 + 476 : 64 + 480]
    rim_out[4:8, LANES:] = docext[64 + 508 : 64 + 512]

    phase("chain1_wait")
    for d in range(1, ny):
        arrived(chain1.at[wrap(y - d, ny)], ch_r.at[0, d])
    phase("chain1_fold")
    end, end_doc = fold(nothing, chain1, ny, ny, 2)
    chain2[z, :, :STATES] = end
    chain2[z, :, STATES:] = end_doc
    send(rim_out, rim_in, one_s.at[1], one_r.at[1], z=after_z, y=after_y)
    for d in range(1, nz):
        send(chain2.at[z], chain2.at[z], ch_s.at[1, d], ch_r.at[1, d], z=wrap(z + d, nz))

    phase("ring12_13")
    for k in range(2, max(nz, ny) // 2):
        ring_wait(1, k)
        ring_start(1, k + 1)
    out_lanes = lanes_of[1]
    send(wall.at[:, :, :, out_lanes], wpeer, one_s.at[2], one_r.at[2], c=other)

    phase("rim_wait")
    arrived(rim_in, one_r.at[1])
    phase("conv")
    first = here == 0
    prodext[0:4] = rim_in[0:4, :LANES]
    prodext[32:36] = rim_in[4:8, :LANES]
    docext[0:4] = jnp.where(first, -1.0, rim_in[0:4, LANES:])
    docext[32:36] = jnp.where(first, -1.0, rim_in[4:8, LANES:])
    now = docext[64:]
    mixed = (
        taps[0:1].astype(F32) * prodext[0:ALL] * ones_where(docext[0:ALL] == now)
        + taps[1:2].astype(F32) * prodext[32 : 32 + ALL] * ones_where(docext[32 : 32 + ALL] == now)
        + taps[2:3].astype(F32) * prodext[64:]
    )
    conv_out = (gate[...] * mixed).astype(BF16)
    acts[:, :LANES] = nn(unperm[...], conv_out).astype(BF16)
    mine, theirs = (pl.ds(pl.multiple_of(v * (ALL // 2), ALL // 2), ALL // 2) for v in (c, other))
    conv_lanes, ssm_lanes = pl.ds(0, LANES), pl.ds(LANES, LANES)

    phase("chain2_wait")
    for d in range(1, nz):
        arrived(chain2.at[wrap(z - d, nz)], ch_r.at[1, d])
    phase("chain2_fold")
    send(acts.at[theirs, conv_lanes], pacts.at[:, conv_lanes], one_s.at[3], one_r.at[3], c=other)
    state = fold(nothing, chain2, nz, z, 3)
    state = fold(state, chain1, ny, y, 2)
    for seg in range(8):
        links[seg] = state[0]
        state = joined(state, ends[seg], 1)
    for seg in range(8):
        rim_state = slice(seg * 4, seg * 4 + 4)
        links[8 + seg // 2, (seg % 2) * 4 : (seg % 2) * 4 + 4] = links[seg, 0:4]
        links[12 + seg // 2, (seg % 2) * 4 : (seg % 2) * 4 + 4] = links[seg, 4:8]
    phase("fixup")
    previous = docext[32:64]
    for cut in range(STATES // LANES):
        re, im = lane_cut(cut)
        a_re, a_im = lam[0:1, re], lam[1:2, re]
        w_re = links[8:12, :, re].reshape(32, LANES)
        w_im = links[12:16, :, re].reshape(32, LANES)
        for k in range(16):
            w_re, w_im = a_re * w_re - a_im * w_im, a_re * w_im + a_im * w_re
            reach = ones_where(docs_at(k) == previous)
            pushed[rows_at(k), re] = pushed[rows_at(k), re] + reach * w_re
            pushed[rows_at(k), im] = pushed[rows_at(k), im] + reach * w_im
    phase("readout")
    reading = nt(pushed[...].astype(BF16), rmat[...]) + skip[...] * driven[...]
    inner = 0.7978845608028654 * (reading + 0.044715 * (reading * reading * reading))
    ssm_out = (0.5 * reading * (1.0 + jnp.tanh(inner))).astype(BF16)
    acts[:, LANES:] = nn(unperm[...], ssm_out).astype(BF16)
    send(acts.at[theirs, ssm_lanes], pacts.at[:, ssm_lanes], one_s.at[4], one_r.at[4], c=other)

    phase("pact_wait")
    arrived(wpeer, one_r.at[2])
    arrived(pacts.at[:, conv_lanes], one_r.at[3])
    columns = total_depth // 2
    own_weight = wall.at[:, :, :, out_lanes]
    arrived(pacts.at[:, ssm_lanes], one_r.at[4])
    phase("out_proj")
    for h in range(2):
        cut = slice(h * nz // 2, (h + 1) * nz // 2)
        total = nt(acts[mine, :], wall[cut, :, :, 4 * LANES :].reshape(columns, 2 * LANES))
        total = total + nt(pacts[...], wpeer[cut].reshape(columns, 2 * LANES))
        part[h] = total.astype(BF16).reshape(PARTS, ROWS // 2, columns)
        if h == 0:
            send(part.at[0, xo], relay.at[0], rs_s.at[0, 0], rs_r.at[0, 0], x=xp)
            send(part.at[0, xm], final.at[1, 0], rs_s.at[1, 1], rs_r.at[1, 1], x=xm)
        else:
            send(part.at[1, xo], relay.at[1], rs_s.at[1, 0], rs_r.at[1, 0], x=xm)
            send(part.at[1, xp], final.at[0, 1], rs_s.at[0, 1], rs_r.at[0, 1], x=xp)
    phase("relay0")
    arrived(relay.at[0], rs_r.at[0, 0])
    part[0, xp] = (part[0, xp].astype(F32) + relay[0].astype(F32)).astype(BF16)
    send(part.at[0, xp], final.at[0, 0], rs_s.at[0, 2], rs_r.at[0, 2], x=xp)
    phase("relay1")
    arrived(relay.at[1], rs_r.at[1, 0])
    part[1, xm] = (part[1, xm].astype(F32) + relay[1].astype(F32)).astype(BF16)
    send(part.at[1, xm], final.at[1, 1], rs_s.at[1, 2], rs_r.at[1, 2], x=xm)
    phase("final")
    for h, turns in ((1, (1, 2)), (0, (2, 1))):
        arrived(final.at[0, h], rs_r.at[0, turns[0]])
        arrived(final.at[1, h], rs_r.at[1, turns[1]])
        value = part[h, x].astype(F32) + final[0, h].astype(F32) + final[1, h].astype(F32)
        out[:, h * columns : (h + 1) * columns] = value.astype(BF16)
    phase("drain")
    for copy in sent:
        copy.wait_send()
    phase(None)


def shards(
    nz, ny, tokens, documents, norm_gain, out_gate_weight, in_gate_weight, value_weight,
    conv_taps, state_in_weight, decay_rate, frequency, step_log, input_real, input_imag,
    readout_real, readout_imag, skip_gain, conv_out_weight, state_out_weight,
):
    depth = state_in_weight.shape[0]
    width = tokens.shape[1]
    columns = nz * ny * depth // 2
    vmem = pl.BlockSpec(memory_space=pltpu.VMEM)
    anywhere = pl.BlockSpec(memory_space=pl.ANY)
    dma = pltpu.SemaphoreType.DMA
    steps = max(nz, ny) // 2
    most = max(nz, ny)
    return pl.pallas_call(
        functools.partial(mixer_kernel, nz, ny, depth),
        out_shape=jax.ShapeDtypeStruct((ROWS // 2, 2 * columns), BF16),
        in_specs=[anywhere] * 18,
        out_specs=vmem,
        scratch_shapes=[
            pltpu.VMEM((2, 8, 64), F32),
            pltpu.VMEM((1, 32), F32),
            pltpu.VMEM((4, 8, 16, 64), F32),
            pltpu.VMEM((3, LANES), BF16),
            pltpu.VMEM((1, LANES), F32),
            pltpu.VMEM((8, STATES), F32),
            pltpu.VMEM((PARTS, 2, ROWS, width), BF16),
            pltpu.VMEM((2, 1, width), norm_gain.dtype),
            pltpu.VMEM((PARTS, 1, ROWS), jnp.int32),
            pltpu.VMEM((nz, ny, depth, 6 * LANES), BF16),
            pltpu.VMEM((nz, ny, depth, 2 * LANES), BF16),
            pltpu.VMEM((ALL, 2 * width), BF16),
            pltpu.VMEM((ALL, ALL), BF16),
            pltpu.VMEM((ALL, ALL), BF16),
            pltpu.VMEM((LANES, 2 * STATES), BF16),
            pltpu.VMEM((LANES, 2 * STATES), BF16),
            pltpu.VMEM((ALL, LANES), F32),
            pltpu.VMEM((ALL, 2 * STATES), F32),
            pltpu.VMEM((64 + ALL, LANES), F32),
            pltpu.VMEM((64 + ALL, LANES), F32),
            pltpu.VMEM((ALL, LANES), F32),
            pltpu.VMEM((8, 8, STATES + LANES), F32),
            pltpu.VMEM((ny, 8, STATES + LANES), F32),
            pltpu.VMEM((nz, 8, STATES + LANES), F32),
            pltpu.VMEM((16, 8, STATES), F32),
            pltpu.VMEM((8, 2 * LANES), F32),
            pltpu.VMEM((8, 2 * LANES), F32),
            pltpu.VMEM((ALL, 2 * LANES), BF16),
            pltpu.VMEM((ALL // 2, 2 * LANES), BF16),
            pltpu.VMEM((2, PARTS, ROWS // 2, columns), BF16),
            pltpu.VMEM((2, ROWS // 2, columns), BF16),
            pltpu.VMEM((2, 2, ROWS // 2, columns), BF16),
            dma((18,)),
            dma((2, 3)), dma((2, 3)),
            dma((4,)), dma((4,)),
            dma((3,)), dma((3,)),
            dma((5,)), dma((5,)),
            dma((2, most)), dma((2, most)),
            dma((2, most)), dma((2, most)),
            dma((2, 2, 2, steps)), dma((2, 2, 2, steps)),
            dma((2, most)), dma((2, most)),
            dma((2, 3)), dma((2, 3)),
        ],
        compiler_params=pltpu.CompilerParams(
            collective_id=0, has_side_effects=True, vmem_limit_bytes=60 * 1024 * 1024
        ),
        name="mixer",
    )(
        tokens, state_in_weight, out_gate_weight, in_gate_weight, value_weight, conv_out_weight.T,
        state_out_weight.T, documents[None, :], norm_gain[None, :], decay_rate, frequency,
        step_log[None, :], input_real.transpose(0, 2, 1), input_imag.transpose(0, 2, 1),
        readout_real, readout_imag, conv_taps, skip_gain[None, :],
    )


def solution(mesh, nz=8, ny=8):
    torus = Mesh(
        mesh.devices.reshape(nz, ny, mesh.shape["fs"], mesh.shape["tp"]), ("sp_0", "sp_1", "fs", "tp")
    )
    in_specs = (
        P(FS_SP, "tp"),
        P(FS_SP),
        P("tp"),
        P(SP, "tp"),
        P(SP, "tp"),
        P(SP, "tp"),
        P(None, "tp"),
        P(SP, "tp"),
        P("tp", None),
        P("tp", None),
        P("tp"),
        P("tp", None, None),
        P("tp", None, None),
        P("tp", None, None),
        P("tp", None, None),
        P("tp"),
        P("tp", SP),
        P("tp", SP),
    )
    return jax.shard_map(
        functools.partial(shards, nz, ny), mesh=torus, in_specs=in_specs,
        out_specs=P(FS_SP_TP, None), check_vma=False,
    )
```

```python
import functools

import jax
import jax.numpy as jnp
from jax import lax
from jax.experimental import pallas as pl
from jax.experimental.pallas import tpu as pltpu
from jax.sharding import Mesh
from jax.sharding import PartitionSpec as P

SP = ("sp_0", "sp_1")
FS_SP = ("fs", "sp_0", "sp_1")
FS_SP_TP = ("fs", "sp_0", "sp_1", "tp")
EPS = 1e-06
PARTS = 4
ROWS = 128
LANES = 128
STATES = 512
ALL = PARTS * ROWS
BF16 = jnp.bfloat16
F32 = jnp.float32


def nn(a, b):
    return jnp.dot(a, b, preferred_element_type=F32)


def nt(a, b):
    return lax.dot_general(a, b, (((1,), (1,)), ((), ())), preferred_element_type=F32)


def ones_where(mask):
    return jnp.where(mask, 1.0, 0.0)


def mixer_kernel(
    nz, ny, depth, tok_in, w_in_0, w_in_1, w_in_2, w_in_3, w_in_4, w_in_5, doc_in, gain_in,
    decay_in, freq_in, step_in, in_re, in_im, read_re, read_im, taps_in, skip_in, out,
    rates, step_row, mats, taps, skip, lam, tok, gains, gain_rows, docs, wall, wpeer, normed, perm, unperm, bmat, rmat, driven, pushed,
    docext, prodext, gate, ends, chain1, chain2, links, rim_out, rim_in, acts, pacts,
    part, relay, final, local_sem, tok_s, tok_r, d2d_s, d2d_r, doc_s, doc_r, one_s, one_r,
    ph_s, ph_r, st_s, st_r, ring_s, ring_r, peer_s, peer_r, ch_s, ch_r, rs_s, rs_r,
):
    z, y = lax.axis_index("sp_0"), lax.axis_index("sp_1")
    x, c = lax.axis_index("fs"), lax.axis_index("tp")
    half = depth // 2
    most = max(nz, ny)
    other = 1 - c
    sent, scopes = [], []

    def phase(name):
        if scopes:
            scopes.pop().__exit__(None, None, None)
        if name:
            scopes.append(jax.named_scope(name))
            scopes[-1].__enter__()

    def wrap(v, n):
        return lax.rem(v + 4 * n, n)

    def send(src, dst, ssem, rsem, **where):
        names = {"z": "sp_0", "y": "sp_1", "x": "fs", "c": "tp"}
        copy = pltpu.make_async_remote_copy(
            src_ref=src, dst_ref=dst, send_sem=ssem, recv_sem=rsem,
            device_id={names[k]: v for k, v in where.items()},
            device_id_type=pl.DeviceIdType.MESH,
        )
        copy.start()
        sent.append(copy)

    def arrived(dst, rsem):
        pltpu.make_async_copy(dst, dst, rsem).wait()

    xp, xm, xo = wrap(x + 1, PARTS), wrap(x - 1, PARTS), wrap(x + 2, PARTS)
    here = z * ny + y
    after, before = wrap(here + 1, nz * ny), wrap(here - 1, nz * ny)
    after_z, after_y = lax.div(after, ny), lax.rem(after, ny)
    before_z, before_y = lax.div(before, ny), lax.rem(before, ny)

    phase("greet")
    barrier = pltpu.get_barrier_semaphore()
    count = 0

    def greet(**where):
        names = {"z": "sp_0", "y": "sp_1", "x": "fs", "c": "tp"}
        pl.semaphore_signal(
            barrier, inc=1, device_id={names[k]: v for k, v in where.items()},
            device_id_type=pl.DeviceIdType.MESH,
        )
        return 1

    for d in range(1, ny):
        count += greet(y=wrap(y + d, ny))
    for d in range(1, nz):
        count += greet(z=wrap(z + d, nz))
    for v in (xp, xm, xo):
        count += greet(x=v)
    count += greet(c=other)
    count += greet(z=after_z, y=after_y)
    count += greet(z=before_z, y=before_y)

    own_channels = pl.ds(pl.multiple_of(x * LANES, LANES), LANES)
    own_groups = pl.ds(pl.multiple_of(x * 8, 8), 8)
    moves = [(tok_in, tok.at[x, c]), (doc_in, docs.at[x]), (gain_in, gains.at[c])]
    for k, w in enumerate((w_in_0, w_in_1, w_in_2, w_in_3, w_in_4, w_in_5)):
        moves.append((w.at[:, own_channels], wall.at[z, y, :, pl.ds(k * LANES, LANES)]))
    early = len(moves)
    moves += [(decay_in.at[own_groups], rates.at[0]), (freq_in.at[own_groups], rates.at[1])]
    moves += [(step_in, step_row), (taps_in.at[:, own_channels], taps), (skip_in.at[:, own_channels], skip)]
    for k, m in enumerate((in_re, in_im, read_re, read_im)):
        moves.append((m.at[own_groups], mats.at[k]))
    local = [pltpu.make_async_copy(a, b, local_sem.at[k]) for k, (a, b) in enumerate(moves)]
    for copy in local:
        copy.start()
    phase("enter")
    for copy in local[:early]:
        copy.wait()
    phase("barrier")
    pl.semaphore_wait(barrier, count)

    low, high = pl.ds(0, ROWS // 2), pl.ds(ROWS // 2, ROWS // 2)

    def token_send(block, rows, way):
        ref = tok.at[block, c, rows]
        return ref, (xp if way == 0 else xm)

    def token_start(block, rows, way, turn):
        ref, target = token_send(block, rows, way)
        send(ref, ref, tok_s.at[way, turn], tok_r.at[way, turn], x=target)

    def token_wait(block, rows, way, turn):
        arrived(tok.at[block, c, rows], tok_r.at[way, turn])

    def pass_over(block, turn):
        ref = tok.at[block, c]
        send(ref, ref, d2d_s.at[turn], d2d_r.at[turn], c=other)

    def passed_over(block, turn):
        arrived(tok.at[block, other], d2d_r.at[turn])

    phase("first_sends")
    rows_a, rows_b = pl.ds(0, half), pl.ds(half, half)
    first_lanes, later_lanes = pl.ds(0, LANES), pl.ds(LANES, 5 * LANES)

    def spread_out(turn, lanes):
        for d in range(1, ny):
            ref = wall.at[z, y, rows_a, lanes]
            send(ref, ref, ph_s.at[turn, 0, d], ph_r.at[turn, 0, d], y=wrap(y + d, ny))
        for d in range(1, nz):
            ref = wall.at[z, y, rows_b, lanes]
            send(ref, ref, ph_s.at[turn, 1, d], ph_r.at[turn, 1, d], z=wrap(z + d, nz))

    def spread_in(turn, lanes, ab):
        for d in range(1, (ny, nz)[ab]):
            block = (z, wrap(y - d, ny), rows_a) if ab == 0 else (wrap(z - d, nz), y, rows_b)
            arrived(wall.at[(*block, lanes)], ph_r.at[turn, ab, d])

    for turn, v in enumerate((xp, xm, xo)):
        send(docs.at[x], docs.at[x], doc_s.at[turn], doc_r.at[turn], x=v)
    send(gains.at[c], gains.at[c], one_s.at[0], one_r.at[0], c=other)
    spread_out(0, first_lanes)
    token_start(x, low, 0, 0)
    token_start(x, high, 1, 0)
    pass_over(x, 0)
    spread_out(1, later_lanes)
    token_start(x, high, 0, 1)
    token_start(x, low, 1, 1)

    phase("tables")
    shape = (ALL, ALL)
    r, n = lax.broadcasted_iota(jnp.int32, shape, 0), lax.broadcasted_iota(jnp.int32, shape, 1)
    natural = (r & 3) * ROWS + ((r >> 2) & 7) * 16 + (r >> 5)
    perm[...] = ones_where(n == natural).astype(BF16)
    t = (r >> 8) * (ROWS // 2) + (r & 63)
    turned = (t & 15) * 32 + (t >> 4) * 4 + ((r >> 6) & 3)
    unperm[...] = ones_where(n == turned).astype(BF16)
    for copy in local[early:]:
        copy.wait()
    group = lax.broadcasted_iota(jnp.int32, (8, 32), 0) + x * 8
    step_log = jnp.broadcast_to(step_row[...], (8, 32))
    mine_only = lax.broadcasted_iota(jnp.int32, (8, 32), 1) == group
    step = jnp.exp(jnp.sum(jnp.where(mine_only, step_log, 0.0), axis=1, keepdims=True))
    decay, frequency = rates[0], rates[1]
    damping, turning = decay * step, frequency * step
    fading = jnp.exp(-damping)
    coef_real, coef_imag = fading * jnp.cos(turning), fading * jnp.sin(turning)
    half_sine = jnp.sin(turning * 0.5)
    series = jnp.ones_like(damping)
    for k in range(11, 1, -1):
        series = 1.0 - damping * (1.0 / k) * series
    less_real = -damping * series * jnp.cos(turning) - 2.0 * half_sine * half_sine
    denominator = decay * decay + frequency * frequency
    ratio_real = (-less_real * decay + coef_imag * frequency) / denominator
    ratio_imag = (-coef_imag * decay - less_real * frequency) / denominator

    def widened(value):
        value = jnp.concatenate([value, value], axis=1)
        return jnp.concatenate([value] * (STATES // LANES), axis=1)

    own_lane = (
        lax.broadcasted_iota(jnp.int32, (8, STATES), 1) >> 6
    ) == lax.broadcasted_iota(jnp.int32, (8, STATES), 0)

    def flat(value):
        return jnp.sum(jnp.where(own_lane, widened(value), 0.0), axis=0, keepdims=True)

    power_re, power_im, squared = coef_real, coef_imag, 1
    for index, length in enumerate((1, 16, ROWS, ROWS * ny)):
        while squared < length:
            power_re, power_im = power_re * power_re - power_im * power_im, 2.0 * power_re * power_im
            squared *= 2
        lam[2 * index : 2 * index + 1, :] = flat(power_re)
        lam[2 * index + 1 : 2 * index + 2, :] = flat(power_im)
    ratio_real, ratio_imag = flat(ratio_real), flat(ratio_imag)
    own_state = (lax.broadcasted_iota(jnp.int32, (LANES, STATES), 0) >> 4) == (
        lax.broadcasted_iota(jnp.int32, (LANES, STATES), 1) >> 6
    )
    input_real, input_imag = (widened(mats[k].reshape(LANES, 64)) for k in range(2))
    bmat[:, :STATES] = jnp.where(own_state, ratio_real * input_real - ratio_imag * input_imag, 0.0).astype(BF16)
    bmat[:, STATES:] = jnp.where(own_state, ratio_real * input_imag + ratio_imag * input_real, 0.0).astype(BF16)
    rmat[:, :STATES] = jnp.where(own_state, widened(mats[2].reshape(LANES, 64)), 0.0).astype(BF16)
    rmat[:, STATES:] = jnp.where(own_state, -widened(mats[3].reshape(LANES, 64)), 0.0).astype(BF16)

    def ring_ref(ab, source, lanes, piece):
        count = (ny, nz)[ab]
        cut = {0: pl.ds(0, count), 1: pl.ds(0, count // 2), 2: pl.ds(count // 2, count // 2)}[piece]
        if ab == 0:
            return wall.at[source, cut, rows_a, lanes]
        return wall.at[cut, source, rows_b, lanes]

    lanes_of = (pl.ds(LANES, 3 * LANES), pl.ds(LANES, 3 * LANES), pl.ds(4 * LANES, 2 * LANES))
    out_lanes = lanes_of[2]

    def ring_hops(which, k):
        for ab in range(2):
            me, size = ((z, nz), (y, ny))[ab]
            last = size // 2 - 1
            for way in range(2):
                if k > last or (k == last and which == 1 - way):
                    continue
                piece = which + 1 if which < 2 else (1 + way if k == last else 0)
                yield ab, way, me, size, piece

    def ring_start(which, k):
        for ab, way, me, size, piece in ring_hops(which, k):
            sign = 1 - 2 * way
            ref = ring_ref(ab, wrap(me - sign * k, size), lanes_of[which], piece)
            send(
                ref, ref, ring_s.at[which, ab, way, k], ring_r.at[which, ab, way, k],
                **{"zy"[ab]: wrap(me + sign, size)},
            )

    def ring_source(which, k):
        for ab, way, me, size, piece in ring_hops(which, k):
            sign = 1 - 2 * way
            yield ab, way, ring_ref(ab, wrap(me - sign * (k + 1), size), lanes_of[which], piece)

    def ring_wait(which, k):
        for ab, way, ref in ring_source(which, k):
            arrived(ref, ring_r.at[which, ab, way, k])

    def service(which, k):
        ring_wait(which, k)
        ring_start(which, k + 1)

    def peer_pieces(turn, mine_or_not):
        if turn == 0:
            pieces = [(z, slice(None), rows_a), (slice(None), y, rows_b)]
            return [(2 * k, p) for k, p in enumerate(pieces)]
        found = []
        for ab, way, me, size, piece in ring_hops(2, turn - 1):
            source = wrap(me - (1 - 2 * way) * turn, size)
            span = (ny, nz)[ab]
            cut = {0: pl.ds(0, span), 1: pl.ds(0, span // 2), 2: pl.ds(span // 2, span // 2)}[piece]
            found.append((2 * ab + way, (source, cut, rows_a) if ab == 0 else (cut, source, rows_b)))
        return found

    def peer_start(turn):
        for k, p in peer_pieces(turn, True):
            send(wall.at[(*p, out_lanes)], wpeer.at[p], peer_s.at[turn, k], peer_r.at[turn, k], c=other)

    def peer_wait(turn):
        for k, p in peer_pieces(turn, False):
            arrived(wpeer.at[p], peer_r.at[turn, k])

    width = 2 * tok.shape[3]

    def norm(block):
        def some_rows(i, carry):
            rows = pl.ds(pl.multiple_of(i * 32, 32), 32)
            a, b = tok[block, 0, rows, :].astype(F32), tok[block, 1, rows, :].astype(F32)
            mean = (jnp.sum(a * a, axis=1, keepdims=True) + jnp.sum(b * b, axis=1, keepdims=True)) / width
            scale = lax.rsqrt(mean + EPS)
            target = pl.ds(pl.multiple_of(block * ROWS + i * 32, 32), 32)
            normed[target, : width // 2] = (a * scale * gain_rows[0]).astype(BF16)
            normed[target, width // 2 :] = (b * scale * gain_rows[1]).astype(BF16)
            return carry

        lax.fori_loop(0, ROWS // 32, some_rows, 0)

    phase("norm_own")
    arrived(gains.at[other], one_r.at[0])
    for k in range(2):
        wide = gains[k].astype(F32)
        gain_rows[k] = jnp.concatenate([wide[i : i + 1] for i in range(wide.shape[0])], axis=1)
    passed_over(x, 0)
    norm(x)
    phase("phase1_state")
    spread_in(0, first_lanes, 0)
    for d in range(1, nz):
        ref = wall.at[z, :, rows_a, first_lanes]
        send(ref, ref, st_s.at[0, d], st_r.at[0, d], z=wrap(z + d, nz))
    spread_in(0, first_lanes, 1)
    for d in range(1, ny):
        ref = wall.at[:, y, rows_b, first_lanes]
        send(ref, ref, st_s.at[1, d], st_r.at[1, d], y=wrap(y + d, ny))
    phase("tok_forward")
    token_wait(xm, low, 0, 0)
    token_start(xm, low, 0, 2)
    token_wait(xp, high, 1, 0)
    token_start(xp, high, 1, 2)
    phase("phase1_rest")
    spread_in(1, later_lanes, 0)
    spread_in(1, later_lanes, 1)
    for which in range(3):
        ring_start(which, 0)
    peer_start(0)
    phase("tok_wait1")
    token_wait(xm, high, 0, 1)
    pass_over(xm, 1)
    token_wait(xp, low, 1, 1)
    pass_over(xp, 2)

    phase("documents")
    for turn, v in enumerate((xm, xp, xo)):
        arrived(docs.at[v], doc_r.at[turn])
    row = lax.broadcasted_iota(jnp.int32, (ALL, ROWS), 0)
    lane = lax.broadcasted_iota(jnp.int32, (ALL, ROWS), 1)
    pick_t = ones_where(lane == ((row >> 2) & 7) * 16 + (row >> 5))
    part_row = lax.broadcasted_iota(jnp.int32, (ROWS, ROWS), 0)
    spread_docs = jnp.zeros((ROWS, ROWS), F32)
    for q in range(PARTS):
        spread_docs = jnp.where(part_row == q, docs[q].astype(F32), spread_docs)
    by_part = nt(pick_t.astype(BF16), spread_docs.astype(BF16))
    by_part = by_part * ones_where(lane == (row & 3))
    docext[64:] = nn(by_part.astype(BF16), jnp.ones((ROWS, LANES), BF16))
    docext[4:32] = docext[64 + 448 : 64 + 476]
    docext[36:64] = docext[64 + 480 : 64 + 508]

    phase("norm_mid")
    passed_over(xm, 1)
    norm(xm)
    passed_over(xp, 2)
    norm(xp)
    phase("tok_wait2")
    token_wait(xo, low, 0, 2)
    token_wait(xo, high, 1, 2)
    pass_over(xo, 3)
    phase("norm_last")
    passed_over(xo, 3)
    norm(xo)

    phase("state_w_wait")
    for d in range(1, nz):
        arrived(wall.at[wrap(z - d, nz), :, rows_a, first_lanes], st_r.at[0, d])
    for d in range(1, ny):
        arrived(wall.at[:, wrap(y - d, ny), rows_b, first_lanes], st_r.at[1, d])
    phase("state_in")
    total_depth = nz * ny * depth
    state_in = wall[:, :, :, :LANES].reshape(total_depth, LANES)
    in_order = nn(perm[...], nn(normed[...], state_in).astype(BF16))
    driven[...] = in_order
    phase("ring_ab0")
    service(0, 0)
    service(1, 0)
    phase("push")
    pushed[...] = nn(in_order.astype(BF16), bmat[...])

    def lane_cut(k):
        return slice(k * LANES, (k + 1) * LANES), slice(STATES + k * LANES, STATES + (k + 1) * LANES)

    def rows_at(k):
        return slice(k * 32, (k + 1) * 32)

    def docs_at(k):
        return docext[64 + k * 32 : 96 + k * 32]

    phase("scan")
    for cut in range(STATES // LANES):
        re, im = lane_cut(cut)
        a_re, a_im = lam[0:1, re], lam[1:2, re]
        s_re, s_im = pushed[0:32, re], pushed[0:32, im]
        for k in range(1, 16):
            keep = ones_where(docs_at(k) == docs_at(k - 1))
            s_re, s_im = (
                pushed[rows_at(k), re] + keep * (a_re * s_re - a_im * s_im),
                pushed[rows_at(k), im] + keep * (a_re * s_im + a_im * s_re),
            )
            pushed[rows_at(k), re] = s_re
            pushed[rows_at(k), im] = s_im
    for seg in range(8):
        rows = slice(480 + seg * 4, 484 + seg * 4)
        ends[seg, 0:4, :STATES] = pushed[rows, :STATES]
        ends[seg, 4:8, :STATES] = pushed[rows, STATES:]
        last = docext[544 + seg * 4 : 548 + seg * 4]
        ends[seg, 0:4, STATES:] = last
        ends[seg, 4:8, STATES:] = last

    phase("fold_local")
    sign = jnp.where(lax.broadcasted_iota(jnp.int32, (8, STATES), 0) < 4, -1.0, 1.0)

    def joined(carry, piece, power):
        held, doc = carry
        now = piece[:, STATES:]
        link = ones_where(now == doc)
        link = jnp.concatenate([link] * (STATES // LANES), axis=1)
        a_re, a_im = lam[2 * power : 2 * power + 1, :], lam[2 * power + 1 : 2 * power + 2, :]
        moved = a_re * held + (a_im * sign) * pltpu.roll(held, 4, 0)
        return piece[:, :STATES] + link * moved, now

    def fold(carry, pieces, count, limit, power):
        def step(k, carry):
            new = joined(carry, pieces[k], power)
            return tuple(jnp.where(k < limit, a, b) for a, b in zip(new, carry))

        return lax.fori_loop(0, count, step, carry)

    nothing = (jnp.zeros((8, STATES), F32), jnp.full((8, LANES), -1.0, F32))
    end, end_doc = fold(nothing, ends, 8, 8, 1)
    chain1[y, :, :STATES] = end
    chain1[y, :, STATES:] = end_doc
    for d in range(1, ny):
        send(chain1.at[y], chain1.at[y], ch_s.at[0, d], ch_r.at[0, d], y=wrap(y + d, ny))
    phase("ring_ab1")
    service(0, 1)
    service(1, 1)
    phase("ring_o0")
    service(2, 0)
    peer_start(1)

    phase("chain1_wait")
    for d in range(1, ny):
        arrived(chain1.at[wrap(y - d, ny)], ch_r.at[0, d])
    end, end_doc = fold(nothing, chain1, ny, ny, 2)
    chain2[z, :, :STATES] = end
    chain2[z, :, STATES:] = end_doc
    for d in range(1, nz):
        send(chain2.at[z], chain2.at[z], ch_s.at[1, d], ch_r.at[1, d], z=wrap(z + d, nz))
    phase("ring_ab2")
    service(0, 2)
    service(1, 2)
    phase("ring_o1")
    service(2, 1)
    peer_start(2)
    phase("ring_ab3")
    for k in range(3, most // 2):
        service(0, k)
        service(1, k)

    phase("conv_in")
    conv_in = wall[:, :, :, LANES : 4 * LANES].reshape(total_depth, 3 * LANES)
    projected = nn(perm[...], nn(normed[...], conv_in).astype(BF16))
    gate[...] = projected[:, :LANES]
    prodext[64:] = (projected[:, LANES : 2 * LANES] * projected[:, 2 * LANES :]).astype(BF16).astype(F32)
    prodext[4:32] = prodext[64 + 448 : 64 + 476]
    prodext[36:64] = prodext[64 + 480 : 64 + 508]
    rim_out[0:4, :LANES] = prodext[64 + 476 : 64 + 480]
    rim_out[4:8, :LANES] = prodext[64 + 508 : 64 + 512]
    rim_out[0:4, LANES:] = docext[64 + 476 : 64 + 480]
    rim_out[4:8, LANES:] = docext[64 + 508 : 64 + 512]

    send(rim_out, rim_in, one_s.at[1], one_r.at[1], z=after_z, y=after_y)
    phase("ring_o2")
    service(2, 2)
    peer_start(3)

    phase("rim_wait")
    arrived(rim_in, one_r.at[1])
    phase("conv")
    first = here == 0
    prodext[0:4] = rim_in[0:4, :LANES]
    prodext[32:36] = rim_in[4:8, :LANES]
    docext[0:4] = jnp.where(first, -1.0, rim_in[0:4, LANES:])
    docext[32:36] = jnp.where(first, -1.0, rim_in[4:8, LANES:])
    now = docext[64:]
    mixed = (
        taps[0:1].astype(F32) * prodext[0:ALL] * ones_where(docext[0:ALL] == now)
        + taps[1:2].astype(F32) * prodext[32 : 32 + ALL] * ones_where(docext[32 : 32 + ALL] == now)
        + taps[2:3].astype(F32) * prodext[64:]
    )
    conv_out = (gate[...] * mixed).astype(BF16)
    acts[:, :LANES] = nn(unperm[...], conv_out).astype(BF16)
    mine, theirs = (pl.ds(pl.multiple_of(v * (ALL // 2), ALL // 2), ALL // 2) for v in (c, other))
    conv_lanes, ssm_lanes = pl.ds(0, LANES), pl.ds(LANES, LANES)

    phase("chain2_wait")
    for d in range(1, nz):
        arrived(chain2.at[wrap(z - d, nz)], ch_r.at[1, d])
    phase("chain2_fold")
    send(acts.at[theirs, conv_lanes], pacts.at[:, conv_lanes], one_s.at[3], one_r.at[3], c=other)
    state = fold(nothing, chain2, nz, z, 3)
    state = fold(state, chain1, ny, y, 2)
    for seg in range(8):
        links[seg] = state[0]
        state = joined(state, ends[seg], 1)
    for seg in range(8):
        rim_state = slice(seg * 4, seg * 4 + 4)
        links[8 + seg // 2, (seg % 2) * 4 : (seg % 2) * 4 + 4] = links[seg, 0:4]
        links[12 + seg // 2, (seg % 2) * 4 : (seg % 2) * 4 + 4] = links[seg, 4:8]
    phase("fixup")
    previous = docext[32:64]
    for cut in range(STATES // LANES):
        re, im = lane_cut(cut)
        a_re, a_im = lam[0:1, re], lam[1:2, re]
        w_re = links[8:12, :, re].reshape(32, LANES)
        w_im = links[12:16, :, re].reshape(32, LANES)
        for k in range(16):
            w_re, w_im = a_re * w_re - a_im * w_im, a_re * w_im + a_im * w_re
            reach = ones_where(docs_at(k) == previous)
            pushed[rows_at(k), re] = pushed[rows_at(k), re] + reach * w_re
            pushed[rows_at(k), im] = pushed[rows_at(k), im] + reach * w_im
    phase("readout")
    reading = nt(pushed[...].astype(BF16), rmat[...]) + skip[...] * driven[...]
    inner = 0.7978845608028654 * (reading + 0.044715 * (reading * reading * reading))
    ssm_out = (0.5 * reading * (1.0 + jnp.tanh(inner))).astype(BF16)
    acts[:, LANES:] = nn(unperm[...], ssm_out).astype(BF16)
    send(acts.at[theirs, ssm_lanes], pacts.at[:, ssm_lanes], one_s.at[4], one_r.at[4], c=other)

    phase("ring_o3")
    for k in range(3, most // 2):
        service(2, k)
        peer_start(k + 1)
    phase("peer_w_wait")
    for turn in range(most // 2 + 1):
        peer_wait(turn)
    phase("pact_wait")
    arrived(pacts.at[:, conv_lanes], one_r.at[3])
    columns = total_depth // 4
    arrived(pacts.at[:, ssm_lanes], one_r.at[4])

    def quarter(ref, cut, lanes):
        if nz % 4 == 0:
            return ref[cut * nz // 4 : (cut + 1) * nz // 4, :, :, lanes].reshape(columns, 2 * LANES)
        return ref[cut // 2, cut % 2, :, lanes]

    for cut in (0, 2, 1, 3):
        phase(f"out_proj{cut}")
        total = nt(acts[mine, :], quarter(wall, cut, slice(4 * LANES, 6 * LANES)))
        total = total + nt(pacts[...], quarter(wpeer, cut, slice(None)))
        part[cut] = total.astype(BF16).reshape(PARTS, ROWS // 2, columns)
        way, turn = cut // 2, cut % 2
        target = (xp, xm)[way]
        send(part.at[cut, xo], relay.at[way, turn], rs_s.at[way, turn], rs_r.at[way, turn], x=target)
    for turn in range(2):
        send(part.at[2 + turn, xp], final.at[0, 2 + turn], rs_s.at[0, 2 + turn], rs_r.at[0, 2 + turn], x=xp)
        send(part.at[turn, xm], final.at[1, turn], rs_s.at[1, 2 + turn], rs_r.at[1, 2 + turn], x=xm)
    for turn in range(2):
        for way, target in ((0, xp), (1, xm)):
            phase(f"relay{way}{turn}")
            cut = 2 * way + turn
            arrived(relay.at[way, turn], rs_r.at[way, turn])
            both = part[cut, target].astype(F32) + relay[way, turn].astype(F32)
            part[cut, target] = both.astype(BF16)
            send(part.at[cut, target], final.at[way, cut], rs_s.at[way, 4 + turn], rs_r.at[way, 4 + turn], x=target)
    for cut in (0, 2, 1, 3):
        phase(f"final{cut}")
        summed_way, turn = cut // 2, cut % 2
        arrived(final.at[1 - summed_way, cut], rs_r.at[1 - summed_way, 2 + turn])
        arrived(final.at[summed_way, cut], rs_r.at[summed_way, 4 + turn])
        value = part[cut, x].astype(F32) + final[0, cut].astype(F32) + final[1, cut].astype(F32)
        out[:, cut * columns : (cut + 1) * columns] = value.astype(BF16)
    phase("drain")
    for copy in sent:
        copy.wait_send()
    phase(None)


def shards(
    nz, ny, tokens, documents, norm_gain, out_gate_weight, in_gate_weight, value_weight,
    conv_taps, state_in_weight, decay_rate, frequency, step_log, input_real, input_imag,
    readout_real, readout_imag, skip_gain, conv_out_weight, state_out_weight,
):
    depth = state_in_weight.shape[0]
    width = tokens.shape[1]
    columns = nz * ny * depth // 4
    vmem = pl.BlockSpec(memory_space=pltpu.VMEM)
    hbm = pl.BlockSpec(memory_space=pltpu.HBM)
    dma = pltpu.SemaphoreType.DMA
    steps = max(nz, ny) // 2
    most = max(nz, ny)
    return pl.pallas_call(
        functools.partial(mixer_kernel, nz, ny, depth),
        out_shape=jax.ShapeDtypeStruct((ROWS // 2, 4 * columns), BF16),
        in_specs=[hbm] * 18,
        out_specs=vmem,
        scratch_shapes=[
            pltpu.VMEM((2, 8, 64), F32),
            pltpu.VMEM((1, 32), F32),
            pltpu.VMEM((4, 8, 16, 64), F32),
            pltpu.VMEM((3, LANES), BF16),
            pltpu.VMEM((1, LANES), F32),
            pltpu.VMEM((8, STATES), F32),
            pltpu.VMEM((PARTS, 2, ROWS, width), BF16),
            pltpu.VMEM((2, width // LANES, LANES), BF16),
            pltpu.VMEM((2, 1, width), F32),
            pltpu.VMEM((PARTS, 1, ROWS), jnp.int32),
            pltpu.VMEM((nz, ny, depth, 6 * LANES), BF16),
            pltpu.VMEM((nz, ny, depth, 2 * LANES), BF16),
            pltpu.VMEM((ALL, 2 * width), BF16),
            pltpu.VMEM((ALL, ALL), BF16),
            pltpu.VMEM((ALL, ALL), BF16),
            pltpu.VMEM((LANES, 2 * STATES), BF16),
            pltpu.VMEM((LANES, 2 * STATES), BF16),
            pltpu.VMEM((ALL, LANES), F32),
            pltpu.VMEM((ALL, 2 * STATES), F32),
            pltpu.VMEM((64 + ALL, LANES), F32),
            pltpu.VMEM((64 + ALL, LANES), F32),
            pltpu.VMEM((ALL, LANES), F32),
            pltpu.VMEM((8, 8, STATES + LANES), F32),
            pltpu.VMEM((ny, 8, STATES + LANES), F32),
            pltpu.VMEM((nz, 8, STATES + LANES), F32),
            pltpu.VMEM((16, 8, STATES), F32),
            pltpu.VMEM((8, 2 * LANES), F32),
            pltpu.VMEM((8, 2 * LANES), F32),
            pltpu.VMEM((ALL, 2 * LANES), BF16),
            pltpu.VMEM((ALL // 2, 2 * LANES), BF16),
            pltpu.VMEM((4, PARTS, ROWS // 2, columns), BF16),
            pltpu.VMEM((2, 2, ROWS // 2, columns), BF16),
            pltpu.VMEM((2, 4, ROWS // 2, columns), BF16),
            dma((18,)),
            dma((2, 3)), dma((2, 3)),
            dma((4,)), dma((4,)),
            dma((3,)), dma((3,)),
            dma((5,)), dma((5,)),
            dma((2, 2, most)), dma((2, 2, most)),
            dma((2, most)), dma((2, most)),
            dma((3, 2, 2, steps)), dma((3, 2, 2, steps)),
            dma((steps + 1, 4)), dma((steps + 1, 4)),
            dma((2, most)), dma((2, most)),
            dma((2, 6)), dma((2, 6)),
        ],
        compiler_params=pltpu.CompilerParams(
            collective_id=0, has_side_effects=True, vmem_limit_bytes=40 * 1024 * 1024
        ),
        name="mixer",
    )(*(
        pltpu.with_memory_space_constraint(operand, pltpu.HBM) for operand in (
            tokens, state_in_weight, out_gate_weight, in_gate_weight, value_weight, conv_out_weight.T,
            state_out_weight.T, documents[None, :], norm_gain.reshape(-1, LANES), decay_rate, frequency,
            step_log[None, :], input_real.transpose(0, 2, 1), input_imag.transpose(0, 2, 1),
            readout_real, readout_imag, conv_taps, skip_gain[None, :],
        )
    ))


def solution(mesh, nz=8, ny=8):
    torus = Mesh(
        mesh.devices.reshape(nz, ny, mesh.shape["fs"], mesh.shape["tp"]), ("sp_0", "sp_1", "fs", "tp")
    )
    in_specs = (
        P(FS_SP, "tp"),
        P(FS_SP),
        P("tp"),
        P(SP, "tp"),
        P(SP, "tp"),
        P(SP, "tp"),
        P(None, "tp"),
        P(SP, "tp"),
        P("tp", None),
        P("tp", None),
        P("tp"),
        P("tp", None, None),
        P("tp", None, None),
        P("tp", None, None),
        P("tp", None, None),
        P("tp"),
        P("tp", SP),
        P("tp", SP),
    )
    return jax.shard_map(
        functools.partial(shards, nz, ny), mesh=torus, in_specs=in_specs,
        out_specs=P(FS_SP_TP, None), check_vma=False,
    )
```

```python
import functools

import jax
import jax.numpy as jnp
from jax import lax
from jax.experimental import pallas as pl
from jax.experimental.pallas import tpu as pltpu
from jax.sharding import Mesh
from jax.sharding import PartitionSpec as P

SP = ("sp_0", "sp_1")
FS_SP = ("fs", "sp_0", "sp_1")
FS_SP_TP = ("fs", "sp_0", "sp_1", "tp")
EPS = 1e-06
PARTS = 4
ROWS = 128
LANES = 128
STATES = 512
ALL = PARTS * ROWS
BF16 = jnp.bfloat16
F32 = jnp.float32


def nn(a, b):
    return jnp.dot(a, b, preferred_element_type=F32)


def halves(product, a, b):
    middle = a.shape[0] // 2
    return jnp.concatenate([product(a[:middle], b), product(a[middle:], b)])


def nt(a, b):
    return lax.dot_general(a, b, (((1,), (1,)), ((), ())), preferred_element_type=F32)


def ones_where(mask):
    return jnp.where(mask, 1.0, 0.0)


def mixer_kernel(
    nz, ny, depth, tok_in, w_in_0, w_in_1, w_in_2, w_in_3, w_in_4, w_in_5, doc_in, gain_in,
    decay_in, freq_in, step_in, in_re, in_im, read_re, read_im, taps_in, skip_in, out,
    rates, step_row, mats, taps, skip, lam, tok, gains, gain_rows, docs, wall, wpeer, normed, perm, unperm, bmat, rmat, driven, pushed,
    docext, prodext, gate, ends, chain1, chain2, incoming, links, rim_out, rim_in, acts, pacts,
    part, relay, final, local_sem, tok_s, tok_r, d2d_s, d2d_r, doc_s, doc_r, one_s, one_r,
    ph_s, ph_r, st_s, st_r, ring_s, ring_r, peer_s, peer_r, ch_s, ch_r, rs_s, rs_r,
):
    z, y = lax.axis_index("sp_0"), lax.axis_index("sp_1")
    x, c = lax.axis_index("fs"), lax.axis_index("tp")
    half = depth // 2
    most = max(nz, ny)
    other = 1 - c
    sent, scopes = [], []

    def phase(name):
        if scopes:
            scopes.pop().__exit__(None, None, None)
        if name:
            scopes.append(jax.named_scope(name))
            scopes[-1].__enter__()

    def wrap(v, n):
        return lax.rem(v + 4 * n, n)

    def send(src, dst, ssem, rsem, **where):
        names = {"z": "sp_0", "y": "sp_1", "x": "fs", "c": "tp"}
        copy = pltpu.make_async_remote_copy(
            src_ref=src, dst_ref=dst, send_sem=ssem, recv_sem=rsem,
            device_id={names[k]: v for k, v in where.items()},
            device_id_type=pl.DeviceIdType.MESH,
        )
        copy.start()
        sent.append(copy)

    def arrived(dst, rsem):
        pltpu.make_async_copy(dst, dst, rsem).wait()

    xp, xm, xo = wrap(x + 1, PARTS), wrap(x - 1, PARTS), wrap(x + 2, PARTS)
    here = z * ny + y
    after, before = wrap(here + 1, nz * ny), wrap(here - 1, nz * ny)
    after_z, after_y = lax.div(after, ny), lax.rem(after, ny)
    before_z, before_y = lax.div(before, ny), lax.rem(before, ny)

    phase("greet")
    barrier = pltpu.get_barrier_semaphore()
    count = 0

    def greet(**where):
        names = {"z": "sp_0", "y": "sp_1", "x": "fs", "c": "tp"}
        pl.semaphore_signal(
            barrier, inc=1, device_id={names[k]: v for k, v in where.items()},
            device_id_type=pl.DeviceIdType.MESH,
        )
        return 1

    for d in range(1, ny):
        count += greet(y=wrap(y + d, ny))
    for d in range(1, nz):
        count += greet(z=wrap(z + d, nz))
    for v in (xp, xm, xo):
        count += greet(x=v)
    count += greet(c=other)
    count += greet(z=after_z, y=after_y)
    count += greet(z=before_z, y=before_y)

    own_channels = pl.ds(pl.multiple_of(x * LANES, LANES), LANES)
    own_groups = pl.ds(pl.multiple_of(x * 8, 8), 8)
    moves = [(tok_in, tok.at[x, c]), (doc_in, docs.at[x]), (gain_in, gains.at[c])]
    for k, w in enumerate((w_in_0, w_in_1, w_in_2, w_in_3, w_in_4, w_in_5)):
        moves.append((w.at[:, own_channels], wall.at[z, y, :, pl.ds(k * LANES, LANES)]))
    early = len(moves)
    moves += [(decay_in.at[own_groups], rates.at[0]), (freq_in.at[own_groups], rates.at[1])]
    moves += [(step_in, step_row), (taps_in.at[:, own_channels], taps), (skip_in.at[:, own_channels], skip)]
    for k, m in enumerate((in_re, in_im, read_re, read_im)):
        moves.append((m.at[own_groups], mats.at[k]))
    local = [pltpu.make_async_copy(a, b, local_sem.at[k]) for k, (a, b) in enumerate(moves)]
    for copy in local:
        copy.start()
    phase("enter")
    for copy in local[:early]:
        copy.wait()
    phase("barrier")
    pl.semaphore_wait(barrier, count)

    low, high = pl.ds(0, ROWS // 2), pl.ds(ROWS // 2, ROWS // 2)

    def column_copy(d):
        return pltpu.make_async_remote_copy(
            src_ref=chain2.at[z], dst_ref=chain2.at[z], send_sem=ch_s.at[1, d], recv_sem=ch_r.at[1, d],
            device_id={"sp_0": wrap(z + d, nz)}, device_id_type=pl.DeviceIdType.MESH,
        )

    def token_send(block, rows, way):
        ref = tok.at[block, c, rows]
        return ref, (xp if way == 0 else xm)

    def token_start(block, rows, way, turn):
        ref, target = token_send(block, rows, way)
        send(ref, ref, tok_s.at[way, turn], tok_r.at[way, turn], x=target)

    def token_wait(block, rows, way, turn):
        arrived(tok.at[block, c, rows], tok_r.at[way, turn])

    def pass_over(block, turn):
        ref = tok.at[block, c]
        send(ref, ref, d2d_s.at[turn], d2d_r.at[turn], c=other)

    def passed_over(block, turn):
        arrived(tok.at[block, other], d2d_r.at[turn])

    phase("first_sends")
    rows_a, rows_b = pl.ds(0, half), pl.ds(half, half)
    first_lanes, later_lanes = pl.ds(0, LANES), pl.ds(LANES, 5 * LANES)

    def spread_out(turn, lanes):
        for d in range(1, ny):
            ref = wall.at[z, y, rows_a, lanes]
            send(ref, ref, ph_s.at[turn, 0, d], ph_r.at[turn, 0, d], y=wrap(y + d, ny))
        for d in range(1, nz):
            ref = wall.at[z, y, rows_b, lanes]
            send(ref, ref, ph_s.at[turn, 1, d], ph_r.at[turn, 1, d], z=wrap(z + d, nz))

    def spread_in(turn, lanes, ab):
        for d in range(1, (ny, nz)[ab]):
            block = (z, wrap(y - d, ny), rows_a) if ab == 0 else (wrap(z - d, nz), y, rows_b)
            arrived(wall.at[(*block, lanes)], ph_r.at[turn, ab, d])

    for turn, v in enumerate((xp, xm, xo)):
        send(docs.at[x], docs.at[x], doc_s.at[turn], doc_r.at[turn], x=v)
    send(gains.at[c], gains.at[c], one_s.at[0], one_r.at[0], c=other)
    spread_out(0, first_lanes)
    token_start(x, low, 0, 0)
    token_start(x, high, 1, 0)
    pass_over(x, 0)
    spread_out(1, later_lanes)
    token_start(x, high, 0, 1)
    token_start(x, low, 1, 1)

    phase("tables")
    shape = (ALL, ALL)
    r, n = lax.broadcasted_iota(jnp.int32, shape, 0), lax.broadcasted_iota(jnp.int32, shape, 1)
    natural = (r & 3) * ROWS + ((r >> 2) & 7) * 16 + (r >> 5)
    perm[...] = ones_where(n == natural).astype(BF16)
    t = (r >> 8) * (ROWS // 2) + (r & 63)
    turned = (t & 15) * 32 + (t >> 4) * 4 + ((r >> 6) & 3)
    unperm[...] = ones_where(n == turned).astype(BF16)
    for copy in local[early:]:
        copy.wait()
    group = lax.broadcasted_iota(jnp.int32, (8, 32), 0) + x * 8
    step_log = jnp.broadcast_to(step_row[...], (8, 32))
    mine_only = lax.broadcasted_iota(jnp.int32, (8, 32), 1) == group
    step = jnp.exp(jnp.sum(jnp.where(mine_only, step_log, 0.0), axis=1, keepdims=True))
    decay, frequency = rates[0], rates[1]
    damping, turning = decay * step, frequency * step
    fading = jnp.exp(-damping)
    coef_real, coef_imag = fading * jnp.cos(turning), fading * jnp.sin(turning)
    half_sine = jnp.sin(turning * 0.5)
    series = jnp.ones_like(damping)
    for k in range(11, 1, -1):
        series = 1.0 - damping * (1.0 / k) * series
    less_real = -damping * series * jnp.cos(turning) - 2.0 * half_sine * half_sine
    denominator = decay * decay + frequency * frequency
    ratio_real = (-less_real * decay + coef_imag * frequency) / denominator
    ratio_imag = (-coef_imag * decay - less_real * frequency) / denominator

    def widened(value):
        value = jnp.concatenate([value, value], axis=1)
        return jnp.concatenate([value] * (STATES // LANES), axis=1)

    own_lane = (
        lax.broadcasted_iota(jnp.int32, (8, STATES), 1) >> 6
    ) == lax.broadcasted_iota(jnp.int32, (8, STATES), 0)

    def flat(value):
        return jnp.sum(jnp.where(own_lane, widened(value), 0.0), axis=0, keepdims=True)

    power_re, power_im, squared = coef_real, coef_imag, 1
    for index, length in enumerate((1, 16, ROWS, ROWS * ny)):
        while squared < length:
            power_re, power_im = power_re * power_re - power_im * power_im, 2.0 * power_re * power_im
            squared *= 2
        lam[2 * index : 2 * index + 1, :] = flat(power_re)
        lam[2 * index + 1 : 2 * index + 2, :] = flat(power_im)
    ratio_real, ratio_imag = flat(ratio_real), flat(ratio_imag)
    own_state = (lax.broadcasted_iota(jnp.int32, (LANES, STATES), 0) >> 4) == (
        lax.broadcasted_iota(jnp.int32, (LANES, STATES), 1) >> 6
    )
    input_real, input_imag = (widened(mats[k].reshape(LANES, 64)) for k in range(2))
    bmat[:, :STATES] = jnp.where(own_state, ratio_real * input_real - ratio_imag * input_imag, 0.0).astype(BF16)
    bmat[:, STATES:] = jnp.where(own_state, ratio_real * input_imag + ratio_imag * input_real, 0.0).astype(BF16)
    rmat[:, :STATES] = jnp.where(own_state, widened(mats[2].reshape(LANES, 64)), 0.0).astype(BF16)
    rmat[:, STATES:] = jnp.where(own_state, -widened(mats[3].reshape(LANES, 64)), 0.0).astype(BF16)

    def ring_ref(ab, source, lanes, piece):
        count = (ny, nz)[ab]
        cut = {0: pl.ds(0, count), 1: pl.ds(0, count // 2), 2: pl.ds(count // 2, count // 2)}[piece]
        if ab == 0:
            return wall.at[source, cut, rows_a, lanes]
        return wall.at[cut, source, rows_b, lanes]

    lanes_of = (pl.ds(LANES, 3 * LANES), pl.ds(LANES, 3 * LANES), pl.ds(4 * LANES, 2 * LANES))
    out_lanes = lanes_of[2]

    def ring_hops(which, k):
        for ab in range(2):
            me, size = ((z, nz), (y, ny))[ab]
            last = size // 2 - 1
            for way in range(2):
                if k > last or (k == last and which == 1 - way):
                    continue
                piece = which + 1 if which < 2 else (1 + way if k == last else 0)
                yield ab, way, me, size, piece

    def ring_start(which, k):
        for ab, way, me, size, piece in ring_hops(which, k):
            sign = 1 - 2 * way
            ref = ring_ref(ab, wrap(me - sign * k, size), lanes_of[which], piece)
            send(
                ref, ref, ring_s.at[which, ab, way, k], ring_r.at[which, ab, way, k],
                **{"zy"[ab]: wrap(me + sign, size)},
            )

    def ring_source(which, k):
        for ab, way, me, size, piece in ring_hops(which, k):
            sign = 1 - 2 * way
            yield ab, way, ring_ref(ab, wrap(me - sign * (k + 1), size), lanes_of[which], piece)

    def ring_wait(which, k):
        for ab, way, ref in ring_source(which, k):
            arrived(ref, ring_r.at[which, ab, way, k])

    def state_hops(ab, stage):
        me, size = ((z, nz), (y, ny))[ab]
        reach = 1 if size < 4 else 2
        for way in range(2):
            for d in range(1, size // 2 + 1):
                if (d > reach) != (stage == 1):
                    continue
                piece = 1 + way if d == size // 2 else 0
                yield way, d, piece, me, size

    def state_start(ab, stage):
        for way, d, piece, me, size in state_hops(ab, stage):
            sign = 1 - 2 * way
            source = wrap(me - sign * 2, size) if stage else me
            ref = ring_ref(ab, source, first_lanes, piece)
            send(
                ref, ref, st_s.at[ab, way, d], st_r.at[ab, way, d],
                **{"zy"[ab]: wrap(me + sign * (d - 2 * stage), size)},
            )

    def state_wait(ab, stage):
        for way, d, piece, me, size in state_hops(ab, stage):
            ref = ring_ref(ab, wrap(me - (1 - 2 * way) * d, size), first_lanes, piece)
            arrived(ref, st_r.at[ab, way, d])

    def service(which, k):
        ring_wait(which, k)
        ring_start(which, k + 1)

    def peer_pieces(turn, mine_or_not):
        if turn == 0:
            pieces = [(z, slice(None), rows_a), (slice(None), y, rows_b)]
            return [(2 * k, p) for k, p in enumerate(pieces)]
        found = []
        for ab, way, me, size, piece in ring_hops(2, turn - 1):
            source = wrap(me - (1 - 2 * way) * turn, size)
            span = (ny, nz)[ab]
            cut = {0: pl.ds(0, span), 1: pl.ds(0, span // 2), 2: pl.ds(span // 2, span // 2)}[piece]
            found.append((2 * ab + way, (source, cut, rows_a) if ab == 0 else (cut, source, rows_b)))
        return found

    def peer_start(turn):
        for k, p in peer_pieces(turn, True):
            send(wall.at[(*p, out_lanes)], wpeer.at[p], peer_s.at[turn, k], peer_r.at[turn, k], c=other)

    def peer_wait(turn):
        for k, p in peer_pieces(turn, False):
            arrived(wpeer.at[p], peer_r.at[turn, k])

    width = 2 * tok.shape[3]

    def norm(block):
        def some_rows(i, carry):
            rows = pl.ds(pl.multiple_of(i * 32, 32), 32)
            a, b = tok[block, 0, rows, :].astype(F32), tok[block, 1, rows, :].astype(F32)
            mean = (jnp.sum(a * a, axis=1, keepdims=True) + jnp.sum(b * b, axis=1, keepdims=True)) / width
            scale = lax.rsqrt(mean + EPS)
            target = pl.ds(pl.multiple_of(block * ROWS + i * 32, 32), 32)
            normed[target, : width // 2] = (a * scale * gain_rows[0]).astype(BF16)
            normed[target, width // 2 :] = (b * scale * gain_rows[1]).astype(BF16)
            return carry

        lax.fori_loop(0, ROWS // 32, some_rows, 0)

    phase("norm_own")
    arrived(gains.at[other], one_r.at[0])
    for k in range(2):
        wide = gains[k].astype(F32)
        gain_rows[k] = jnp.concatenate([wide[i : i + 1] for i in range(wide.shape[0])], axis=1)
    passed_over(x, 0)
    norm(x)
    phase("phase1_state")
    for ab in range(2):
        spread_in(0, first_lanes, ab)
        state_start(ab, 0)
    phase("tok_forward")
    token_wait(xm, low, 0, 0)
    token_start(xm, low, 0, 2)
    token_wait(xp, high, 1, 0)
    token_start(xp, high, 1, 2)
    phase("phase1_rest")
    spread_in(1, later_lanes, 0)
    spread_in(1, later_lanes, 1)
    for which in range(3):
        ring_start(which, 0)
    peer_start(0)
    phase("tok_wait1")
    token_wait(xm, high, 0, 1)
    pass_over(xm, 1)
    token_wait(xp, low, 1, 1)
    pass_over(xp, 2)

    phase("documents")
    for turn, v in enumerate((xm, xp, xo)):
        arrived(docs.at[v], doc_r.at[turn])
    row = lax.broadcasted_iota(jnp.int32, (ALL, ROWS), 0)
    lane = lax.broadcasted_iota(jnp.int32, (ALL, ROWS), 1)
    pick_t = ones_where(lane == ((row >> 2) & 7) * 16 + (row >> 5))
    part_row = lax.broadcasted_iota(jnp.int32, (ROWS, ROWS), 0)
    spread_docs = jnp.zeros((ROWS, ROWS), F32)
    for q in range(PARTS):
        spread_docs = jnp.where(part_row == q, docs[q].astype(F32), spread_docs)
    by_part = nt(pick_t.astype(BF16), spread_docs.astype(BF16))
    by_part = by_part * ones_where(lane == (row & 3))
    docext[64:] = nn(by_part.astype(BF16), jnp.ones((ROWS, LANES), BF16))
    docext[4:32] = docext[64 + 448 : 64 + 476]
    docext[36:64] = docext[64 + 480 : 64 + 508]

    phase("state_stage")
    for ab in range(2):
        state_wait(ab, 0)
        state_start(ab, 1)
    phase("norm_mid")
    passed_over(xm, 1)
    norm(xm)
    phase("tok_wait2")
    token_wait(xo, low, 0, 2)
    token_wait(xo, high, 1, 2)
    pass_over(xo, 3)
    phase("norm_mid2")
    passed_over(xp, 2)
    norm(xp)
    phase("ring_ab0")
    service(0, 0)
    service(1, 0)
    phase("norm_last")
    passed_over(xo, 3)
    norm(xo)

    phase("ring_o0")
    service(2, 0)
    peer_start(1)
    phase("state_w_wait")
    for ab in range(2):
        state_wait(ab, 1)
    phase("state_in")
    total_depth = nz * ny * depth
    state_in = wall[:, :, :, :LANES].reshape(total_depth, LANES)
    in_order = halves(nn, perm, halves(nn, normed, state_in).astype(BF16))
    driven[...] = in_order
    phase("ring_ab1")
    service(0, 1)
    service(1, 1)
    phase("push")
    pushed[...] = nn(in_order.astype(BF16), bmat[...])

    def lane_cut(k):
        return slice(k * LANES, (k + 1) * LANES), slice(STATES + k * LANES, STATES + (k + 1) * LANES)

    def rows_at(k):
        return slice(k * 32, (k + 1) * 32)

    def docs_at(k):
        return docext[64 + k * 32 : 96 + k * 32]

    phase("scan")
    for cut in range(STATES // LANES):
        re, im = lane_cut(cut)
        a_re, a_im = lam[0:1, re], lam[1:2, re]
        s_re, s_im = pushed[0:32, re], pushed[0:32, im]
        for k in range(1, 16):
            keep = ones_where(docs_at(k) == docs_at(k - 1))
            s_re, s_im = (
                pushed[rows_at(k), re] + keep * (a_re * s_re - a_im * s_im),
                pushed[rows_at(k), im] + keep * (a_re * s_im + a_im * s_re),
            )
            pushed[rows_at(k), re] = s_re
            pushed[rows_at(k), im] = s_im
    for seg in range(8):
        rows = slice(480 + seg * 4, 484 + seg * 4)
        ends[seg, 0:4, :STATES] = pushed[rows, :STATES]
        ends[seg, 4:8, :STATES] = pushed[rows, STATES:]
        last = docext[544 + seg * 4 : 548 + seg * 4]
        ends[seg, 0:4, STATES:] = last
        ends[seg, 4:8, STATES:] = last

    phase("fold_local")
    sign = jnp.where(lax.broadcasted_iota(jnp.int32, (8, STATES), 0) < 4, -1.0, 1.0)

    def joined(carry, piece, power):
        held, doc = carry
        piece, now = piece
        link = ones_where(now == doc)
        link = jnp.concatenate([link] * (STATES // LANES), axis=1)
        a_re, a_im = lam[2 * power : 2 * power + 1, :], lam[2 * power + 1 : 2 * power + 2, :]
        moved = a_re * held + (a_im * sign) * pltpu.roll(held, 4, 0)
        return piece + link * moved, now

    def of_ends(k):
        return ends[k, :, :STATES], ends[k, :, STATES:]

    wing = STATES // 2

    def pack(buffer, index, carry):
        held, doc = carry
        buffer[index, 0:8, :wing] = held[:, :wing].astype(BF16)
        buffer[index, 8:16, :wing] = held[:, wing:].astype(BF16)
        buffer[index, 0:8, wing:] = doc.astype(BF16)
        buffer[index, 8:16, wing:] = doc.astype(BF16)

    def of(buffer):
        def read(k):
            message = buffer[k].astype(F32)
            held = jnp.concatenate([message[0:8, :wing], message[8:16, :wing]], axis=1)
            return held, message[0:8, wing:]

        return read

    def fold(carry, pieces, count, limit, power):
        def step(k, carry):
            new = joined(carry, pieces(k), power)
            return tuple(jnp.where(k < limit, a, b) for a, b in zip(new, carry))

        return lax.fori_loop(0, count, step, carry)

    nothing = (jnp.zeros((8, STATES), F32), jnp.full((8, LANES), -1.0, F32))
    pack(chain1, y, fold(nothing, of_ends, 8, 8, 1))
    for d in range(1, ny):
        send(chain1.at[y], chain1.at[y], ch_s.at[0, d], ch_r.at[0, d], y=wrap(y + d, ny))
    phase("ring_o1")
    service(2, 1)
    peer_start(2)

    phase("ring_ab2")
    service(0, 2)
    service(1, 2)
    phase("chain1_wait")
    for d in range(1, ny):
        arrived(chain1.at[wrap(y - d, ny)], ch_r.at[0, d])
    pack(chain2, z, fold(nothing, of(chain1), ny, ny, 2))
    for d in range(1, nz):

        @pl.when(z + d < nz)
        def _(d=d):
            column_copy(d).start()
    phase("ring_o2")
    service(2, 2)
    peer_start(3)
    phase("ring_ab3")
    for k in range(3, most // 2):
        service(0, k)
        service(1, k)

    phase("conv_in")
    conv_in = wall[:, :, :, LANES : 4 * LANES].reshape(total_depth, 3 * LANES)
    projected = nn(perm[...], nn(normed[...], conv_in).astype(BF16))
    gate[...] = projected[:, :LANES]
    prodext[64:] = (projected[:, LANES : 2 * LANES] * projected[:, 2 * LANES :]).astype(BF16).astype(F32)
    rim_out[0:4, :LANES] = prodext[64 + 476 : 64 + 480]
    rim_out[4:8, :LANES] = prodext[64 + 508 : 64 + 512]
    rim_out[0:4, LANES:] = docext[64 + 476 : 64 + 480]
    rim_out[4:8, LANES:] = docext[64 + 508 : 64 + 512]
    prodext[4:32] = prodext[64 + 448 : 64 + 476]
    prodext[36:64] = prodext[64 + 480 : 64 + 508]
    send(rim_out, rim_in, one_s.at[1], one_r.at[1], z=after_z, y=after_y)
    phase("ring_o3")
    for k in range(3, most // 2):
        service(2, k)
        peer_start(k + 1)
    phase("chain2_wait")
    incoming[:, :STATES], incoming[:, STATES:] = nothing
    for d in range(1, nz):

        @pl.when(z >= d)
        def _(d=d):
            arrived(chain2.at[z - d], ch_r.at[1, d])

    phase("chain2_fold")

    @pl.when(z > 0)
    def _():
        def step(k, carry):
            return joined(carry, of(chain2)(k), 3)

        incoming[:, :STATES], incoming[:, STATES:] = lax.fori_loop(0, z, step, nothing)

    state = fold((incoming[:, :STATES], incoming[:, STATES:]), of(chain1), ny, y, 2)
    docext[32:36] = state[1][0:4]
    for seg in range(8):
        links[seg] = state[0]
        state = joined(state, of_ends(seg), 1)
    for seg in range(8):
        links[8 + seg // 2, (seg % 2) * 4 : (seg % 2) * 4 + 4] = links[seg, 0:4]
        links[12 + seg // 2, (seg % 2) * 4 : (seg % 2) * 4 + 4] = links[seg, 4:8]
    phase("fixup")
    previous = docext[32:64]
    for cut in range(STATES // LANES):
        re, im = lane_cut(cut)
        a_re, a_im = lam[0:1, re], lam[1:2, re]
        w_re = links[8:12, :, re].reshape(32, LANES)
        w_im = links[12:16, :, re].reshape(32, LANES)
        for k in range(16):
            w_re, w_im = a_re * w_re - a_im * w_im, a_re * w_im + a_im * w_re
            reach = ones_where(docs_at(k) == previous)
            pushed[rows_at(k), re] = pushed[rows_at(k), re] + reach * w_re
            pushed[rows_at(k), im] = pushed[rows_at(k), im] + reach * w_im
    phase("readout")
    reading = halves(nt, pushed[...].astype(BF16), rmat[...]) + skip[...] * driven[...]
    inner = 0.7978845608028654 * (reading + 0.044715 * (reading * reading * reading))
    ssm_out = (0.5 * reading * (1.0 + jnp.tanh(inner))).astype(BF16)
    acts[:, LANES:] = halves(nn, unperm, ssm_out).astype(BF16)
    mine, theirs = (pl.ds(pl.multiple_of(v * (ALL // 2), ALL // 2), ALL // 2) for v in (c, other))
    conv_lanes, ssm_lanes = pl.ds(0, LANES), pl.ds(LANES, LANES)
    send(acts.at[theirs, ssm_lanes], pacts.at[:, ssm_lanes], one_s.at[4], one_r.at[4], c=other)

    phase("rim_wait")
    docext[0:4] = jnp.full((4, LANES), -1.0, F32)
    prodext[0:4] = jnp.zeros((4, LANES), F32)
    prodext[32:36] = jnp.zeros((4, LANES), F32)

    @pl.when(here > 0)
    def _():
        arrived(rim_in, one_r.at[1])
        prodext[0:4] = rim_in[0:4, :LANES]
        prodext[32:36] = rim_in[4:8, :LANES]
        docext[0:4] = rim_in[0:4, LANES:]

    phase("conv")
    now = docext[64:]
    mixed = (
        taps[0:1].astype(F32) * prodext[0:ALL] * ones_where(docext[0:ALL] == now)
        + taps[1:2].astype(F32) * prodext[32 : 32 + ALL] * ones_where(docext[32 : 32 + ALL] == now)
        + taps[2:3].astype(F32) * prodext[64:]
    )
    conv_out = (gate[...] * mixed).astype(BF16)
    acts[:, :LANES] = halves(nn, unperm, conv_out).astype(BF16)
    send(acts.at[theirs, conv_lanes], pacts.at[:, conv_lanes], one_s.at[3], one_r.at[3], c=other)

    columns = total_depth // 4

    def quarter(ref, cut, lanes):
        if nz % 4 == 0:
            return ref[cut * nz // 4 : (cut + 1) * nz // 4, :, :, lanes].reshape(columns, 2 * LANES)
        return ref[cut // 2, cut % 2, :, lanes]

    phase("peer_w_wait")
    for turn in range(most // 2 + 1):
        peer_wait(turn)
    settled = len(sent)
    for cut in (0, 2, 1, 3):
        phase(f"out_proj{cut}")
        total = nt(acts[mine, :], quarter(wall, cut, slice(4 * LANES, 6 * LANES)))
        if cut == 0:
            phase("pact_wait")
            arrived(pacts.at[:, ssm_lanes], one_r.at[4])
            arrived(pacts.at[:, conv_lanes], one_r.at[3])
        total = total + nt(pacts[...], quarter(wpeer, cut, slice(None)))
        part[cut] = total.astype(BF16).reshape(PARTS, ROWS // 2, columns)
        way, turn = cut // 2, cut % 2
        target = (xp, xm)[way]
        send(part.at[cut, xo], relay.at[way, turn], rs_s.at[way, turn], rs_r.at[way, turn], x=target)
    for turn in range(2):
        send(part.at[2 + turn, xp], final.at[0, 2 + turn], rs_s.at[0, 2 + turn], rs_r.at[0, 2 + turn], x=xp)
        send(part.at[turn, xm], final.at[1, turn], rs_s.at[1, 2 + turn], rs_r.at[1, 2 + turn], x=xm)
    for copy in sent[:settled]:
        copy.wait_send()
    for turn in range(2):
        for way, target in ((0, xp), (1, xm)):
            phase(f"relay{way}{turn}")
            cut = 2 * way + turn
            arrived(relay.at[way, turn], rs_r.at[way, turn])
            both = part[cut, target].astype(F32) + relay[way, turn].astype(F32)
            part[cut, target] = both.astype(BF16)
            send(part.at[cut, target], final.at[way, cut], rs_s.at[way, 4 + turn], rs_r.at[way, 4 + turn], x=target)
    for cut in (0, 2, 1, 3):
        phase(f"final{cut}")
        summed_way, turn = cut // 2, cut % 2
        arrived(final.at[1 - summed_way, cut], rs_r.at[1 - summed_way, 2 + turn])
        arrived(final.at[summed_way, cut], rs_r.at[summed_way, 4 + turn])
        value = part[cut, x].astype(F32) + final[0, cut].astype(F32) + final[1, cut].astype(F32)
        out[:, cut * columns : (cut + 1) * columns] = value.astype(BF16)
    phase("drain")
    for copy in sent[settled:]:
        copy.wait_send()

    @pl.when(here == 0)
    def _():
        arrived(rim_in, one_r.at[1])

    for d in range(1, nz):

        @pl.when(z + d < nz)
        def _(d=d):
            column_copy(d).wait_send()

    phase(None)


def shards(
    nz, ny, tokens, documents, norm_gain, out_gate_weight, in_gate_weight, value_weight,
    conv_taps, state_in_weight, decay_rate, frequency, step_log, input_real, input_imag,
    readout_real, readout_imag, skip_gain, conv_out_weight, state_out_weight,
):
    depth = state_in_weight.shape[0]
    width = tokens.shape[1]
    columns = nz * ny * depth // 4
    vmem = pl.BlockSpec(memory_space=pltpu.VMEM)
    hbm = pl.BlockSpec(memory_space=pltpu.HBM)
    dma = pltpu.SemaphoreType.DMA
    steps = max(nz, ny) // 2
    most = max(nz, ny)
    return pl.pallas_call(
        functools.partial(mixer_kernel, nz, ny, depth),
        out_shape=jax.ShapeDtypeStruct((ROWS // 2, 4 * columns), BF16),
        in_specs=[hbm] * 18,
        out_specs=vmem,
        scratch_shapes=[
            pltpu.VMEM((2, 8, 64), F32),
            pltpu.VMEM((1, 32), F32),
            pltpu.VMEM((4, 8, 16, 64), F32),
            pltpu.VMEM((3, LANES), BF16),
            pltpu.VMEM((1, LANES), F32),
            pltpu.VMEM((8, STATES), F32),
            pltpu.VMEM((PARTS, 2, ROWS, width), BF16),
            pltpu.VMEM((2, width // LANES, LANES), BF16),
            pltpu.VMEM((2, 1, width), F32),
            pltpu.VMEM((PARTS, 1, ROWS), jnp.int32),
            pltpu.VMEM((nz, ny, depth, 6 * LANES), BF16),
            pltpu.VMEM((nz, ny, depth, 2 * LANES), BF16),
            pltpu.VMEM((ALL, 2 * width), BF16),
            pltpu.VMEM((ALL, ALL), BF16),
            pltpu.VMEM((ALL, ALL), BF16),
            pltpu.VMEM((LANES, 2 * STATES), BF16),
            pltpu.VMEM((LANES, 2 * STATES), BF16),
            pltpu.VMEM((ALL, LANES), F32),
            pltpu.VMEM((ALL, 2 * STATES), F32),
            pltpu.VMEM((64 + ALL, LANES), F32),
            pltpu.VMEM((64 + ALL, LANES), F32),
            pltpu.VMEM((ALL, LANES), F32),
            pltpu.VMEM((8, 8, STATES + LANES), F32),
            pltpu.VMEM((ny, 16, STATES // 2 + LANES), BF16),
            pltpu.VMEM((nz, 16, STATES // 2 + LANES), BF16),
            pltpu.VMEM((8, STATES + LANES), F32),
            pltpu.VMEM((16, 8, STATES), F32),
            pltpu.VMEM((8, 2 * LANES), F32),
            pltpu.VMEM((8, 2 * LANES), F32),
            pltpu.VMEM((ALL, 2 * LANES), BF16),
            pltpu.VMEM((ALL // 2, 2 * LANES), BF16),
            pltpu.VMEM((4, PARTS, ROWS // 2, columns), BF16),
            pltpu.VMEM((2, 2, ROWS // 2, columns), BF16),
            pltpu.VMEM((2, 4, ROWS // 2, columns), BF16),
            dma((18,)),
            dma((2, 3)), dma((2, 3)),
            dma((4,)), dma((4,)),
            dma((3,)), dma((3,)),
            dma((5,)), dma((5,)),
            dma((2, 2, most)), dma((2, 2, most)),
            dma((2, 2, steps + 1)), dma((2, 2, steps + 1)),
            dma((3, 2, 2, steps)), dma((3, 2, 2, steps)),
            dma((steps + 1, 4)), dma((steps + 1, 4)),
            dma((2, most)), dma((2, most)),
            dma((2, 6)), dma((2, 6)),
        ],
        compiler_params=pltpu.CompilerParams(
            collective_id=0, has_side_effects=True, vmem_limit_bytes=40 * 1024 * 1024
        ),
        name="mixer",
    )(*(
        pltpu.with_memory_space_constraint(operand, pltpu.HBM) for operand in (
            tokens, state_in_weight, out_gate_weight, in_gate_weight, value_weight, conv_out_weight.T,
            state_out_weight.T, documents[None, :], norm_gain.reshape(-1, LANES), decay_rate, frequency,
            step_log[None, :], input_real.transpose(0, 2, 1), input_imag.transpose(0, 2, 1),
            readout_real, readout_imag, conv_taps, skip_gain[None, :],
        )
    ))


def solution(mesh, nz=8, ny=8):
    torus = Mesh(
        mesh.devices.reshape(nz, ny, mesh.shape["fs"], mesh.shape["tp"]), ("sp_0", "sp_1", "fs", "tp")
    )
    in_specs = (
        P(FS_SP, "tp"),
        P(FS_SP),
        P("tp"),
        P(SP, "tp"),
        P(SP, "tp"),
        P(SP, "tp"),
        P(None, "tp"),
        P(SP, "tp"),
        P("tp", None),
        P("tp", None),
        P("tp"),
        P("tp", None, None),
        P("tp", None, None),
        P("tp", None, None),
        P("tp", None, None),
        P("tp"),
        P("tp", SP),
        P("tp", SP),
    )
    return jax.shard_map(
        functools.partial(shards, nz, ny), mesh=torus, in_specs=in_specs,
        out_specs=P(FS_SP_TP, None), check_vma=False,
    )
```

```python
import functools

import jax
import jax.numpy as jnp
from jax import lax
from jax.experimental import pallas as pl
from jax.experimental.pallas import tpu as pltpu
from jax.sharding import Mesh
from jax.sharding import PartitionSpec as P

SP = ("sp_0", "sp_1")
FS_SP = ("fs", "sp_0", "sp_1")
FS_SP_TP = ("fs", "sp_0", "sp_1", "tp")
EPS = 1e-06
PARTS = 4
ROWS = 128
LANES = 128
STATES = 512
ALL = PARTS * ROWS
BF16 = jnp.bfloat16
F32 = jnp.float32


def nn(a, b):
    return jnp.dot(a, b, preferred_element_type=F32)


def halves(product, a, b):
    middle = a.shape[0] // 2
    return jnp.concatenate([product(a[:middle], b), product(a[middle:], b)])


def nt(a, b):
    return lax.dot_general(a, b, (((1,), (1,)), ((), ())), preferred_element_type=F32)


def ones_where(mask):
    return jnp.where(mask, 1.0, 0.0)


def mixer_kernel(
    nz, ny, depth, tok_in, w_in_0, w_in_1, w_in_2, w_in_3, w_in_4, w_in_5, doc_in, gain_in,
    decay_in, freq_in, step_in, in_re, in_im, read_re, read_im, taps_in, skip_in, out,
    rates, step_row, mats, taps, skip, lam, tok, gains, gain_rows, docs, wall, wpeer, normed, perm, unperm, bmat, rmat, driven, pushed,
    docext, prodext, gate, ends, chain1, chain2, incoming, links, rim_out, rim_in, acts, pacts,
    part, relay, final, local_sem, tok_s, tok_r, d2d_s, d2d_r, doc_s, doc_r, one_s, one_r,
    ph_s, ph_r, st_s, st_r, ring_s, ring_r, peer_s, peer_r, ch_s, ch_r, rs_s, rs_r,
):
    z, y = lax.axis_index("sp_0"), lax.axis_index("sp_1")
    x, c = lax.axis_index("fs"), lax.axis_index("tp")
    half = depth // 2
    most = max(nz, ny)
    other = 1 - c
    owed, scopes = [], []

    def phase(name):
        if scopes:
            scopes.pop().__exit__(None, None, None)
        if name:
            scopes.append(jax.named_scope(name))
            scopes[-1].__enter__()

    def wrap(v, n):
        return lax.rem(v + 4 * n, n)

    def send(src, dst, ssem, rsem, **where):
        names = {"z": "sp_0", "y": "sp_1", "x": "fs", "c": "tp"}
        copy = pltpu.make_async_remote_copy(
            src_ref=src, dst_ref=dst, send_sem=ssem, recv_sem=rsem,
            device_id={names[k]: v for k, v in where.items()},
            device_id_type=pl.DeviceIdType.MESH,
        )
        copy.start()

    def arrived(dst, rsem):
        pltpu.make_async_copy(dst, dst, rsem).wait()

    def owe(view, ssem):
        owed.append((view, ssem))

    def settle():
        for view, ssem in owed:
            arrived(view, ssem)
        owed.clear()

    xp, xm, xo = wrap(x + 1, PARTS), wrap(x - 1, PARTS), wrap(x + 2, PARTS)
    here = z * ny + y
    after, before = wrap(here + 1, nz * ny), wrap(here - 1, nz * ny)
    after_z, after_y = lax.div(after, ny), lax.rem(after, ny)
    before_z, before_y = lax.div(before, ny), lax.rem(before, ny)

    phase("greet")
    barrier = pltpu.get_barrier_semaphore()
    count = 0

    def greet(**where):
        names = {"z": "sp_0", "y": "sp_1", "x": "fs", "c": "tp"}
        pl.semaphore_signal(
            barrier, inc=1, device_id={names[k]: v for k, v in where.items()},
            device_id_type=pl.DeviceIdType.MESH,
        )
        return 1

    for d in range(1, ny):
        count += greet(y=wrap(y + d, ny))
    for d in range(1, nz):
        count += greet(z=wrap(z + d, nz))
    for v in (xp, xm, xo):
        count += greet(x=v)
    count += greet(c=other)
    count += greet(z=after_z, y=after_y)
    count += greet(z=before_z, y=before_y)

    own_channels = pl.ds(pl.multiple_of(x * LANES, LANES), LANES)
    own_groups = pl.ds(pl.multiple_of(x * 8, 8), 8)
    moves = [(tok_in, tok.at[x, c], 0), (doc_in, docs.at[x], 1), (gain_in, gains.at[c], 2)]
    for k, w in enumerate((w_in_0, w_in_1, w_in_2, w_in_3, w_in_4, w_in_5)):
        moves.append((w.at[:, own_channels], wall.at[z, y, :, pl.ds(k * LANES, LANES)], 3))
    moves += [(decay_in.at[own_groups], rates.at[0], 4), (freq_in.at[own_groups], rates.at[1], 4)]
    for k, m in enumerate((in_re, in_im, read_re, read_im)):
        moves.append((m.at[own_groups], mats.at[k], 5))
    moves += [(step_in, step_row, 6), (taps_in.at[:, own_channels], taps, 7)]
    moves.append((skip_in.at[:, own_channels], skip, 8))
    for source, target, k in moves:
        pltpu.make_async_copy(source, target, local_sem.at[k]).start()
    phase("enter")
    for k, ref in enumerate((tok.at[x, c], docs.at[x], gains.at[c], wall.at[z, y])):
        arrived(ref, local_sem.at[k])
    phase("barrier")
    pl.semaphore_wait(barrier, count)

    low, high = pl.ds(0, ROWS // 2), pl.ds(ROWS // 2, ROWS // 2)

    def column_copy(d):
        return pltpu.make_async_remote_copy(
            src_ref=chain2.at[z], dst_ref=chain2.at[z], send_sem=ch_s.at[d], recv_sem=ch_r.at[d],
            device_id={"sp_0": wrap(z + d, nz)}, device_id_type=pl.DeviceIdType.MESH,
        )

    def token_send(block, rows, way):
        ref = tok.at[block, c, rows]
        return ref, (xp if way == 0 else xm)

    def token_start(block, rows, way, turn):
        ref, target = token_send(block, rows, way)
        send(ref, ref, tok_s.at[0], tok_r.at[way, turn], x=target)

    def token_wait(block, rows, way, turn):
        arrived(tok.at[block, c, rows], tok_r.at[way, turn])

    def pass_over(block, turn):
        ref = tok.at[block, c]
        send(ref, ref, d2d_s.at[0], d2d_r.at[turn], c=other)

    def passed_over(block, turn):
        arrived(tok.at[block, other], d2d_r.at[turn])

    phase("first_sends")
    rows_a, rows_b = pl.ds(0, half), pl.ds(half, half)
    first_lanes, later_lanes = pl.ds(0, LANES), pl.ds(LANES, 5 * LANES)

    def spread_view(lanes, ab):
        if ab == 0:
            return wall.at[0, pl.ds(0, ny - 1), rows_a, lanes]
        return wall.at[pl.ds(0, nz - 1), 0, rows_b, lanes]

    def spread_out(turn, lanes):
        for d in range(1, ny):
            ref = wall.at[z, y, rows_a, lanes]
            send(ref, ref, ph_s.at[turn, 0], ph_r.at[turn, 0], y=wrap(y + d, ny))
        for d in range(1, nz):
            ref = wall.at[z, y, rows_b, lanes]
            send(ref, ref, ph_s.at[turn, 1], ph_r.at[turn, 1], z=wrap(z + d, nz))
        for ab in range(2):
            owe(spread_view(lanes, ab), ph_s.at[turn, ab])

    def spread_in(turn, lanes, ab):
        arrived(spread_view(lanes, ab), ph_r.at[turn, ab])

    for v in (xp, xm, xo):
        send(docs.at[x], docs.at[x], doc_s.at[0], doc_r.at[0], x=v)
    owe(docs.at[pl.ds(0, PARTS - 1)], doc_s.at[0])
    send(gains.at[c], gains.at[c], one_s.at[0], one_r.at[0], c=other)
    owe(gains.at[c], one_s.at[0])
    owe(tok.at[pl.ds(0, PARTS - 1), 0], tok_s.at[0])
    owe(tok.at[:, 0], d2d_s.at[0])
    spread_out(0, first_lanes)
    token_start(x, low, 0, 0)
    token_start(x, high, 1, 0)
    pass_over(x, 0)
    spread_out(1, later_lanes)
    token_start(x, high, 0, 1)
    token_start(x, low, 1, 1)

    phase("tables")
    shape = (ALL, ALL)
    r, n = lax.broadcasted_iota(jnp.int32, shape, 0), lax.broadcasted_iota(jnp.int32, shape, 1)
    natural = (r & 3) * ROWS + ((r >> 2) & 7) * 16 + (r >> 5)
    perm[...] = ones_where(n == natural).astype(BF16)
    t = (r >> 8) * (ROWS // 2) + (r & 63)
    turned = (t & 15) * 32 + (t >> 4) * 4 + ((r >> 6) & 3)
    unperm[...] = ones_where(n == turned).astype(BF16)
    for k, ref in enumerate((rates, mats, step_row, taps, skip)):
        arrived(ref, local_sem.at[4 + k])
    group = lax.broadcasted_iota(jnp.int32, (8, 32), 0) + x * 8
    step_log = jnp.broadcast_to(step_row[...], (8, 32))
    mine_only = lax.broadcasted_iota(jnp.int32, (8, 32), 1) == group
    step = jnp.exp(jnp.sum(jnp.where(mine_only, step_log, 0.0), axis=1, keepdims=True))
    decay, frequency = rates[0], rates[1]
    damping, turning = decay * step, frequency * step
    fading = jnp.exp(-damping)
    coef_real, coef_imag = fading * jnp.cos(turning), fading * jnp.sin(turning)
    half_sine = jnp.sin(turning * 0.5)
    series = jnp.ones_like(damping)
    for k in range(11, 1, -1):
        series = 1.0 - damping * (1.0 / k) * series
    less_real = -damping * series * jnp.cos(turning) - 2.0 * half_sine * half_sine
    denominator = decay * decay + frequency * frequency
    ratio_real = (-less_real * decay + coef_imag * frequency) / denominator
    ratio_imag = (-coef_imag * decay - less_real * frequency) / denominator

    def widened(value):
        value = jnp.concatenate([value, value], axis=1)
        return jnp.concatenate([value] * (STATES // LANES), axis=1)

    own_lane = (
        lax.broadcasted_iota(jnp.int32, (8, STATES), 1) >> 6
    ) == lax.broadcasted_iota(jnp.int32, (8, STATES), 0)

    def flat(value):
        return jnp.sum(jnp.where(own_lane, widened(value), 0.0), axis=0, keepdims=True)

    power_re, power_im, squared = coef_real, coef_imag, 1
    for index, length in enumerate((1, 16, ROWS, ROWS * ny)):
        while squared < length:
            power_re, power_im = power_re * power_re - power_im * power_im, 2.0 * power_re * power_im
            squared *= 2
        lam[2 * index : 2 * index + 1, :] = flat(power_re)
        lam[2 * index + 1 : 2 * index + 2, :] = flat(power_im)
    ratio_real, ratio_imag = flat(ratio_real), flat(ratio_imag)
    own_state = (lax.broadcasted_iota(jnp.int32, (LANES, STATES), 0) >> 4) == (
        lax.broadcasted_iota(jnp.int32, (LANES, STATES), 1) >> 6
    )
    input_real, input_imag = (widened(mats[k].reshape(LANES, 64)) for k in range(2))
    bmat[:, :STATES] = jnp.where(own_state, ratio_real * input_real - ratio_imag * input_imag, 0.0).astype(BF16)
    bmat[:, STATES:] = jnp.where(own_state, ratio_real * input_imag + ratio_imag * input_real, 0.0).astype(BF16)
    rmat[:, :STATES] = jnp.where(own_state, widened(mats[2].reshape(LANES, 64)), 0.0).astype(BF16)
    rmat[:, STATES:] = jnp.where(own_state, -widened(mats[3].reshape(LANES, 64)), 0.0).astype(BF16)

    def ring_ref(ab, source, lanes, piece):
        count = (ny, nz)[ab]
        cut = {0: pl.ds(0, count), 1: pl.ds(0, count // 2), 2: pl.ds(count // 2, count // 2)}[piece]
        if ab == 0:
            return wall.at[source, cut, rows_a, lanes]
        return wall.at[cut, source, rows_b, lanes]

    lanes_of = (pl.ds(LANES, 3 * LANES), pl.ds(LANES, 3 * LANES), pl.ds(4 * LANES, 2 * LANES))
    out_lanes = lanes_of[2]

    def ring_hops(which, k):
        for ab in range(2):
            me, size = ((z, nz), (y, ny))[ab]
            last = size // 2 - 1
            for way in range(2):
                if k > last or (k == last and which == 1 - way):
                    continue
                piece = which + 1 if which < 2 else (1 + way if k == last else 0)
                yield ab, way, me, size, piece

    def ring_start(which, k):
        for ab, way, me, size, piece in ring_hops(which, k):
            sign = 1 - 2 * way
            ref = ring_ref(ab, wrap(me - sign * k, size), lanes_of[which], piece)
            send(ref, ref, ring_s.at[which], ring_r.at[which, k], **{"zy"[ab]: wrap(me + sign, size)})

    def blocks_view(array, count, lanes):
        if count > nz * ny:
            return array.at[pl.ds(0, count // (2 * ny)), :, :, lanes]
        return array.at[pl.ds(0, count // ny), :, rows_a, lanes]

    def ring_blocks(which, k):
        return sum((ny, nz)[ab] // (2 if piece else 1) for ab, _, _, _, piece in ring_hops(which, k))

    def ring_wait(which, k):
        if ring_blocks(which, k):
            arrived(blocks_view(wall, ring_blocks(which, k), lanes_of[which]), ring_r.at[which, k])

    def state_hops(ab, stage):
        me, size = ((z, nz), (y, ny))[ab]
        reach = 1 if size < 4 else 2
        for way in range(2):
            for d in range(1, size // 2 + 1):
                if (d > reach) != (stage == 1):
                    continue
                piece = 1 + way if d == size // 2 else 0
                yield way, d, piece, me, size

    def state_start(ab, stage):
        for way, d, piece, me, size in state_hops(ab, stage):
            sign = 1 - 2 * way
            source = wrap(me - sign * 2, size) if stage else me
            ref = ring_ref(ab, source, first_lanes, piece)
            target = wrap(me + sign * (d - 2 * stage), size)
            send(ref, ref, st_s.at[ab, stage], st_r.at[ab, stage], **{"zy"[ab]: target})
        if state_blocks(ab, stage):
            owe(blocks_view(wall, state_blocks(ab, stage), first_lanes), st_s.at[ab, stage])

    def state_blocks(ab, stage):
        return sum((ny, nz)[ab] // (2 if piece else 1) for _, _, piece, _, _ in state_hops(ab, stage))

    def state_wait(ab, stage):
        if state_blocks(ab, stage):
            arrived(blocks_view(wall, state_blocks(ab, stage), first_lanes), st_r.at[ab, stage])

    def service(which, k):
        ring_wait(which, k)
        ring_start(which, k + 1)

    def peer_pieces(turn):
        if turn == 0:
            return [(z, slice(None), rows_a), (slice(None), y, rows_b)]
        found = []
        for ab, way, me, size, piece in ring_hops(2, turn - 1):
            source = wrap(me - (1 - 2 * way) * turn, size)
            span = (ny, nz)[ab]
            cut = {0: pl.ds(0, span), 1: pl.ds(0, span // 2), 2: pl.ds(span // 2, span // 2)}[piece]
            found.append((source, cut, rows_a) if ab == 0 else (cut, source, rows_b))
        return found

    def peer_start(turn):
        for p in peer_pieces(turn):
            send(wall.at[(*p, out_lanes)], wpeer.at[p], peer_s.at[0], peer_r.at[0], c=other)

    width = 2 * tok.shape[3]

    def norm(block):
        def some_rows(i, carry):
            rows = pl.ds(pl.multiple_of(i * 32, 32), 32)
            a, b = tok[block, 0, rows, :].astype(F32), tok[block, 1, rows, :].astype(F32)
            mean = (jnp.sum(a * a, axis=1, keepdims=True) + jnp.sum(b * b, axis=1, keepdims=True)) / width
            scale = lax.rsqrt(mean + EPS)
            target = pl.ds(pl.multiple_of(block * ROWS + i * 32, 32), 32)
            normed[target, : width // 2] = (a * scale * gain_rows[0]).astype(BF16)
            normed[target, width // 2 :] = (b * scale * gain_rows[1]).astype(BF16)
            return carry

        lax.fori_loop(0, ROWS // 32, some_rows, 0)

    phase("norm_own")
    arrived(gains.at[other], one_r.at[0])
    for k in range(2):
        wide = gains[k].astype(F32)
        gain_rows[k] = jnp.concatenate([wide[i : i + 1] for i in range(wide.shape[0])], axis=1)
    passed_over(x, 0)
    norm(x)
    phase("phase1_state")
    for ab in range(2):
        spread_in(0, first_lanes, ab)
        state_start(ab, 0)
    phase("tok_forward")
    token_wait(xm, low, 0, 0)
    token_start(xm, low, 0, 2)
    token_wait(xp, high, 1, 0)
    token_start(xp, high, 1, 2)
    phase("phase1_rest")
    spread_in(1, later_lanes, 0)
    spread_in(1, later_lanes, 1)
    for which in range(3):
        ring_start(which, 0)
    peer_start(0)
    phase("tok_wait1")
    token_wait(xm, high, 0, 1)
    pass_over(xm, 1)
    token_wait(xp, low, 1, 1)
    pass_over(xp, 2)

    phase("documents")
    arrived(docs.at[pl.ds(0, PARTS - 1)], doc_r.at[0])
    row = lax.broadcasted_iota(jnp.int32, (ALL, ROWS), 0)
    lane = lax.broadcasted_iota(jnp.int32, (ALL, ROWS), 1)
    pick_t = ones_where(lane == ((row >> 2) & 7) * 16 + (row >> 5))
    part_row = lax.broadcasted_iota(jnp.int32, (ROWS, ROWS), 0)
    spread_docs = jnp.zeros((ROWS, ROWS), F32)
    for q in range(PARTS):
        spread_docs = jnp.where(part_row == q, docs[q].astype(F32), spread_docs)
    by_part = nt(pick_t.astype(BF16), spread_docs.astype(BF16))
    by_part = by_part * ones_where(lane == (row & 3))
    docext[64:] = nn(by_part.astype(BF16), jnp.ones((ROWS, LANES), BF16))
    docext[4:32] = docext[64 + 448 : 64 + 476]
    docext[36:64] = docext[64 + 480 : 64 + 508]

    phase("state_stage")
    for ab in range(2):
        state_wait(ab, 0)
        state_start(ab, 1)
    phase("norm_mid")
    passed_over(xm, 1)
    norm(xm)
    phase("tok_wait2")
    token_wait(xo, low, 0, 2)
    token_wait(xo, high, 1, 2)
    pass_over(xo, 3)
    phase("norm_mid2")
    passed_over(xp, 2)
    norm(xp)
    phase("ring_ab0")
    service(0, 0)
    service(1, 0)
    phase("norm_last")
    passed_over(xo, 3)
    norm(xo)

    phase("ring_o0")
    service(2, 0)
    peer_start(1)
    phase("state_w_wait")
    for ab in range(2):
        state_wait(ab, 1)
    phase("state_in")
    total_depth = nz * ny * depth
    state_in = wall[:, :, :, :LANES].reshape(total_depth, LANES)
    in_order = halves(nn, perm, halves(nn, normed, state_in).astype(BF16))
    driven[...] = in_order
    phase("ring_ab1")
    service(0, 1)
    service(1, 1)
    phase("push")
    pushed[...] = nn(in_order.astype(BF16), bmat[...])

    def lane_cut(k):
        return slice(k * LANES, (k + 1) * LANES), slice(STATES + k * LANES, STATES + (k + 1) * LANES)

    def rows_at(k):
        return slice(k * 32, (k + 1) * 32)

    def docs_at(k):
        return docext[64 + k * 32 : 96 + k * 32]

    phase("scan")
    for cut in range(STATES // LANES):
        re, im = lane_cut(cut)
        a_re, a_im = lam[0:1, re], lam[1:2, re]
        s_re, s_im = pushed[0:32, re], pushed[0:32, im]
        for k in range(1, 16):
            keep = ones_where(docs_at(k) == docs_at(k - 1))
            s_re, s_im = (
                pushed[rows_at(k), re] + keep * (a_re * s_re - a_im * s_im),
                pushed[rows_at(k), im] + keep * (a_re * s_im + a_im * s_re),
            )
            pushed[rows_at(k), re] = s_re
            pushed[rows_at(k), im] = s_im
    for seg in range(8):
        rows = slice(480 + seg * 4, 484 + seg * 4)
        ends[seg, 0:4, :STATES] = pushed[rows, :STATES]
        ends[seg, 4:8, :STATES] = pushed[rows, STATES:]
        last = docext[544 + seg * 4 : 548 + seg * 4]
        ends[seg, 0:4, STATES:] = last
        ends[seg, 4:8, STATES:] = last

    phase("fold_local")
    sign = jnp.where(lax.broadcasted_iota(jnp.int32, (8, STATES), 0) < 4, -1.0, 1.0)

    def joined(carry, piece, power):
        held, doc = carry
        piece, now = piece
        link = ones_where(now == doc)
        link = jnp.concatenate([link] * (STATES // LANES), axis=1)
        a_re, a_im = lam[2 * power : 2 * power + 1, :], lam[2 * power + 1 : 2 * power + 2, :]
        moved = a_re * held + (a_im * sign) * pltpu.roll(held, 4, 0)
        return piece + link * moved, now

    def of_ends(k):
        return ends[k, :, :STATES], ends[k, :, STATES:]

    wing = STATES // 2

    def pack(buffer, index, carry):
        held, doc = carry
        buffer[index, 0:8, :wing] = held[:, :wing].astype(BF16)
        buffer[index, 8:16, :wing] = held[:, wing:].astype(BF16)
        buffer[index, 0:8, wing:] = doc.astype(BF16)
        buffer[index, 8:16, wing:] = doc.astype(BF16)

    def of(buffer):
        def read(k):
            message = buffer[k].astype(F32)
            held = jnp.concatenate([message[0:8, :wing], message[8:16, :wing]], axis=1)
            return held, message[0:8, wing:]

        return read

    def fold(carry, pieces, count, limit, power):
        def step(k, carry):
            new = joined(carry, pieces(k), power)
            return tuple(jnp.where(k < limit, a, b) for a, b in zip(new, carry))

        return lax.fori_loop(0, count, step, carry)

    nothing = (jnp.zeros((8, STATES), F32), jnp.full((8, LANES), -1.0, F32))
    pack(chain1, y, fold(nothing, of_ends, 8, 8, 1))
    for d in range(1, ny):
        send(chain1.at[y], chain1.at[y], one_s.at[1], one_r.at[1], y=wrap(y + d, ny))
    phase("ring_o1")
    service(2, 1)
    peer_start(2)

    phase("ring_ab2")
    service(0, 2)
    service(1, 2)
    phase("chain1_wait")
    owe(chain1.at[pl.ds(0, ny - 1)], one_s.at[1])
    arrived(chain1.at[pl.ds(0, ny - 1)], one_r.at[1])
    pack(chain2, z, fold(nothing, of(chain1), ny, ny, 2))
    for d in range(1, nz):

        @pl.when(z + d < nz)
        def _(d=d):
            column_copy(d).start()
    phase("ring_o2")
    service(2, 2)
    peer_start(3)
    phase("ring_ab3")
    for k in range(3, most // 2):
        service(0, k)
        service(1, k)

    phase("conv_in")
    conv_in = wall[:, :, :, LANES : 4 * LANES].reshape(total_depth, 3 * LANES)
    projected = nn(perm[...], nn(normed[...], conv_in).astype(BF16))
    gate[...] = projected[:, :LANES]
    prodext[64:] = (projected[:, LANES : 2 * LANES] * projected[:, 2 * LANES :]).astype(BF16).astype(F32)
    rim_out[0:4, :LANES] = prodext[64 + 476 : 64 + 480]
    rim_out[4:8, :LANES] = prodext[64 + 508 : 64 + 512]
    rim_out[0:4, LANES:] = docext[64 + 476 : 64 + 480]
    rim_out[4:8, LANES:] = docext[64 + 508 : 64 + 512]
    prodext[4:32] = prodext[64 + 448 : 64 + 476]
    prodext[36:64] = prodext[64 + 480 : 64 + 508]
    send(rim_out, rim_in, one_s.at[2], one_r.at[2], z=after_z, y=after_y)
    owe(rim_out, one_s.at[2])
    phase("ring_o3")
    for k in range(3, most // 2):
        service(2, k)
        peer_start(k + 1)
    phase("chain2_wait")
    incoming[:, :STATES], incoming[:, STATES:] = nothing
    for d in range(1, nz):

        @pl.when(z >= d)
        def _(d=d):
            arrived(chain2.at[z - d], ch_r.at[d])

    phase("chain2_fold")

    @pl.when(z > 0)
    def _():
        def step(k, carry):
            return joined(carry, of(chain2)(k), 3)

        incoming[:, :STATES], incoming[:, STATES:] = lax.fori_loop(0, z, step, nothing)

    state = fold((incoming[:, :STATES], incoming[:, STATES:]), of(chain1), ny, y, 2)
    docext[32:36] = state[1][0:4]
    for seg in range(8):
        links[seg] = state[0]
        state = joined(state, of_ends(seg), 1)
    for seg in range(8):
        links[8 + seg // 2, (seg % 2) * 4 : (seg % 2) * 4 + 4] = links[seg, 0:4]
        links[12 + seg // 2, (seg % 2) * 4 : (seg % 2) * 4 + 4] = links[seg, 4:8]
    phase("fixup")
    previous = docext[32:64]
    for cut in range(STATES // LANES):
        re, im = lane_cut(cut)
        a_re, a_im = lam[0:1, re], lam[1:2, re]
        w_re = links[8:12, :, re].reshape(32, LANES)
        w_im = links[12:16, :, re].reshape(32, LANES)
        for k in range(16):
            w_re, w_im = a_re * w_re - a_im * w_im, a_re * w_im + a_im * w_re
            reach = ones_where(docs_at(k) == previous)
            pushed[rows_at(k), re] = pushed[rows_at(k), re] + reach * w_re
            pushed[rows_at(k), im] = pushed[rows_at(k), im] + reach * w_im
    phase("readout")
    reading = halves(nt, pushed[...].astype(BF16), rmat[...]) + skip[...] * driven[...]
    inner = 0.7978845608028654 * (reading + 0.044715 * (reading * reading * reading))
    ssm_out = (0.5 * reading * (1.0 + jnp.tanh(inner))).astype(BF16)
    acts[:, LANES:] = halves(nn, unperm, ssm_out).astype(BF16)
    mine, theirs = (pl.ds(pl.multiple_of(v * (ALL // 2), ALL // 2), ALL // 2) for v in (c, other))
    conv_lanes, ssm_lanes = pl.ds(0, LANES), pl.ds(LANES, LANES)
    send(acts.at[theirs, ssm_lanes], pacts.at[:, ssm_lanes], one_s.at[4], one_r.at[4], c=other)
    owe(pacts.at[:, ssm_lanes], one_s.at[4])

    phase("rim_wait")
    docext[0:4] = jnp.full((4, LANES), -1.0, F32)
    prodext[0:4] = jnp.zeros((4, LANES), F32)
    prodext[32:36] = jnp.zeros((4, LANES), F32)

    @pl.when(here > 0)
    def _():
        arrived(rim_in, one_r.at[2])
        prodext[0:4] = rim_in[0:4, :LANES]
        prodext[32:36] = rim_in[4:8, :LANES]
        docext[0:4] = rim_in[0:4, LANES:]

    phase("conv")
    now = docext[64:]
    mixed = (
        taps[0:1].astype(F32) * prodext[0:ALL] * ones_where(docext[0:ALL] == now)
        + taps[1:2].astype(F32) * prodext[32 : 32 + ALL] * ones_where(docext[32 : 32 + ALL] == now)
        + taps[2:3].astype(F32) * prodext[64:]
    )
    conv_out = (gate[...] * mixed).astype(BF16)
    acts[:, :LANES] = halves(nn, unperm, conv_out).astype(BF16)
    send(acts.at[theirs, conv_lanes], pacts.at[:, conv_lanes], one_s.at[3], one_r.at[3], c=other)
    owe(pacts.at[:, conv_lanes], one_s.at[3])

    columns = total_depth // 4

    def quarter(ref, cut, lanes):
        if nz % 4 == 0:
            return ref[cut * nz // 4 : (cut + 1) * nz // 4, :, :, lanes].reshape(columns, 2 * LANES)
        return ref[cut // 2, cut % 2, :, lanes]

    phase("peer_w_wait")
    arrived(wpeer, peer_r.at[0])
    for cut in (0, 2, 1, 3):
        phase(f"out_proj{cut}")
        total = nt(acts[mine, :], quarter(wall, cut, slice(4 * LANES, 6 * LANES)))
        if cut == 0:
            phase("pact_wait")
            arrived(pacts.at[:, ssm_lanes], one_r.at[4])
            arrived(pacts.at[:, conv_lanes], one_r.at[3])
        total = total + nt(pacts[...], quarter(wpeer, cut, slice(None)))
        part[cut] = total.astype(BF16).reshape(PARTS, ROWS // 2, columns)
        way, turn = cut // 2, cut % 2
        target = (xp, xm)[way]
        send(part.at[cut, xo], relay.at[way, turn], rs_s.at[0], rs_r.at[2 * way + turn], x=target)
    for turn in range(2):
        send(part.at[2 + turn, xp], final.at[0, 2 + turn], rs_s.at[0], rs_r.at[6 + turn], x=xp)
        send(part.at[turn, xm], final.at[1, turn], rs_s.at[0], rs_r.at[4 + turn], x=xm)
    for which in range(3):
        count = sum(ring_blocks(which, k) for k in range(most // 2))
        owe(blocks_view(wall, count, lanes_of[which]), ring_s.at[which])
    owe(wpeer, peer_s.at[0])
    settle()
    for turn in range(2):
        for way, target in ((0, xp), (1, xm)):
            phase(f"relay{way}{turn}")
            cut = 2 * way + turn
            arrived(relay.at[way, turn], rs_r.at[2 * way + turn])
            both = part[cut, target].astype(F32) + relay[way, turn].astype(F32)
            part[cut, target] = both.astype(BF16)
            send(part.at[cut, target], final.at[way, cut], rs_s.at[0], rs_r.at[4 + cut], x=target)
    for cut in (0, 2, 1, 3):
        phase(f"final{cut}")
        arrived(final.at[:, cut], rs_r.at[4 + cut])
        value = part[cut, x].astype(F32) + final[0, cut].astype(F32) + final[1, cut].astype(F32)
        out[:, cut * columns : (cut + 1) * columns] = value.astype(BF16)
    phase("drain")
    arrived(part.at[pl.ds(0, 3)], rs_s.at[0])

    @pl.when(here == 0)
    def _():
        arrived(rim_in, one_r.at[2])

    for d in range(1, nz):

        @pl.when(z + d < nz)
        def _(d=d):
            column_copy(d).wait_send()

    phase(None)


def shards(
    nz, ny, tokens, documents, norm_gain, out_gate_weight, in_gate_weight, value_weight,
    conv_taps, state_in_weight, decay_rate, frequency, step_log, input_real, input_imag,
    readout_real, readout_imag, skip_gain, conv_out_weight, state_out_weight,
):
    depth = state_in_weight.shape[0]
    width = tokens.shape[1]
    columns = nz * ny * depth // 4
    vmem = pl.BlockSpec(memory_space=pltpu.VMEM)
    hbm = pl.BlockSpec(memory_space=pltpu.HBM)
    dma = pltpu.SemaphoreType.DMA
    steps = max(nz, ny) // 2
    return pl.pallas_call(
        functools.partial(mixer_kernel, nz, ny, depth),
        out_shape=jax.ShapeDtypeStruct((ROWS // 2, 4 * columns), BF16),
        in_specs=[hbm] * 18,
        out_specs=vmem,
        scratch_shapes=[
            pltpu.VMEM((2, 8, 64), F32),
            pltpu.VMEM((1, 32), F32),
            pltpu.VMEM((4, 8, 16, 64), F32),
            pltpu.VMEM((3, LANES), BF16),
            pltpu.VMEM((1, LANES), F32),
            pltpu.VMEM((8, STATES), F32),
            pltpu.VMEM((PARTS, 2, ROWS, width), BF16),
            pltpu.VMEM((2, width // LANES, LANES), BF16),
            pltpu.VMEM((2, 1, width), F32),
            pltpu.VMEM((PARTS, 1, ROWS), jnp.int32),
            pltpu.VMEM((nz, ny, depth, 6 * LANES), BF16),
            pltpu.VMEM((nz, ny, depth, 2 * LANES), BF16),
            pltpu.VMEM((ALL, 2 * width), BF16),
            pltpu.VMEM((ALL, ALL), BF16),
            pltpu.VMEM((ALL, ALL), BF16),
            pltpu.VMEM((LANES, 2 * STATES), BF16),
            pltpu.VMEM((LANES, 2 * STATES), BF16),
            pltpu.VMEM((ALL, LANES), F32),
            pltpu.VMEM((ALL, 2 * STATES), F32),
            pltpu.VMEM((64 + ALL, LANES), F32),
            pltpu.VMEM((64 + ALL, LANES), F32),
            pltpu.VMEM((ALL, LANES), F32),
            pltpu.VMEM((8, 8, STATES + LANES), F32),
            pltpu.VMEM((ny, 16, STATES // 2 + LANES), BF16),
            pltpu.VMEM((nz, 16, STATES // 2 + LANES), BF16),
            pltpu.VMEM((8, STATES + LANES), F32),
            pltpu.VMEM((16, 8, STATES), F32),
            pltpu.VMEM((8, 2 * LANES), F32),
            pltpu.VMEM((8, 2 * LANES), F32),
            pltpu.VMEM((ALL, 2 * LANES), BF16),
            pltpu.VMEM((ALL // 2, 2 * LANES), BF16),
            pltpu.VMEM((4, PARTS, ROWS // 2, columns), BF16),
            pltpu.VMEM((2, 2, ROWS // 2, columns), BF16),
            pltpu.VMEM((2, 4, ROWS // 2, columns), BF16),
            dma((9,)),
            dma((1,)), dma((2, 3)),
            dma((1,)), dma((PARTS,)),
            dma((1,)), dma((1,)),
            dma((5,)), dma((5,)),
            dma((2, 2)), dma((2, 2)),
            dma((2, 2)), dma((2, 2)),
            dma((3,)), dma((3, steps)),
            dma((1,)), dma((1,)),
            dma((nz,)), dma((nz,)),
            dma((1,)), dma((8,)),
        ],
        compiler_params=pltpu.CompilerParams(
            collective_id=0, has_side_effects=True, vmem_limit_bytes=40 * 1024 * 1024
        ),
        name="mixer",
    )(*(
        pltpu.with_memory_space_constraint(operand, pltpu.HBM) for operand in (
            tokens, state_in_weight, out_gate_weight, in_gate_weight, value_weight, conv_out_weight.T,
            state_out_weight.T, documents[None, :], norm_gain.reshape(-1, LANES), decay_rate, frequency,
            step_log[None, :], input_real.transpose(0, 2, 1), input_imag.transpose(0, 2, 1),
            readout_real, readout_imag, conv_taps, skip_gain[None, :],
        )
    ))


def solution(mesh, nz=8, ny=8):
    torus = Mesh(
        mesh.devices.reshape(nz, ny, mesh.shape["fs"], mesh.shape["tp"]), ("sp_0", "sp_1", "fs", "tp")
    )
    in_specs = (
        P(FS_SP, "tp"),
        P(FS_SP),
        P("tp"),
        P(SP, "tp"),
        P(SP, "tp"),
        P(SP, "tp"),
        P(None, "tp"),
        P(SP, "tp"),
        P("tp", None),
        P("tp", None),
        P("tp"),
        P("tp", None, None),
        P("tp", None, None),
        P("tp", None, None),
        P("tp", None, None),
        P("tp"),
        P("tp", SP),
        P("tp", SP),
    )
    return jax.shard_map(
        functools.partial(shards, nz, ny), mesh=torus, in_specs=in_specs,
        out_specs=P(FS_SP_TP, None), check_vma=False,
    )
```

```python
import functools

import jax
import jax.numpy as jnp
from jax import lax
from jax.experimental import pallas as pl
from jax.experimental.pallas import tpu as pltpu
from jax.sharding import Mesh
from jax.sharding import PartitionSpec as P

SP = ("sp_0", "sp_1")
FS_SP = ("fs", "sp_0", "sp_1")
FS_SP_TP = ("fs", "sp_0", "sp_1", "tp")
EPS = 1e-06
PARTS = 4
ROWS = 128
LANES = 128
STATES = 512
ALL = PARTS * ROWS
BF16 = jnp.bfloat16
F32 = jnp.float32


def nn(a, b):
    return jnp.dot(a, b, preferred_element_type=F32)


def halves(product, a, b):
    middle = a.shape[0] // 2
    return jnp.concatenate([product(a[:middle], b), product(a[middle:], b)])


def nt(a, b):
    return lax.dot_general(a, b, (((1,), (1,)), ((), ())), preferred_element_type=F32)


def ones_where(mask):
    return jnp.where(mask, 1.0, 0.0)


def mixer_kernel(
    nz, ny, depth, tok_in, w_in_0, w_in_1, w_in_2, w_in_3, w_in_4, w_in_5, doc_in, gain_in,
    decay_in, freq_in, step_in, in_re, in_im, read_re, read_im, taps_in, skip_in, out,
    rates, step_row, mats, taps, skip, lam, tok, gains, gain_rows, docs, wall_s, wall_c, wall_o, wpeer, normed, perm, unperm, bmat, rmat, driven, pushed,
    docext, prodext, gate, ends, chain1, chain2, incoming, links, rim_out, rim_in, acts, pacts,
    part, relay, final, local_sem, tok_s, tok_r, d2d_s, d2d_r, doc_s, doc_r, one_s, one_r,
    ph_s, ph_r, st_s, st_r, ring_s, ring_r, peer_s, peer_r, rs_s, rs_r,
):
    z, y = lax.axis_index("sp_0"), lax.axis_index("sp_1")
    x, c = lax.axis_index("fs"), lax.axis_index("tp")
    half = depth // 2
    most = max(nz, ny)
    other = 1 - c
    owed, scopes = [], []

    def phase(name):
        if scopes:
            scopes.pop().__exit__(None, None, None)
        if name:
            scopes.append(jax.named_scope(name))
            scopes[-1].__enter__()

    def wrap(v, n):
        return lax.rem(v + 4 * n, n)

    def send(src, dst, ssem, rsem, **where):
        names = {"z": "sp_0", "y": "sp_1", "x": "fs", "c": "tp"}
        copy = pltpu.make_async_remote_copy(
            src_ref=src, dst_ref=dst, send_sem=ssem, recv_sem=rsem,
            device_id={names[k]: v for k, v in where.items()},
            device_id_type=pl.DeviceIdType.MESH,
        )
        copy.start()

    def arrived(dst, rsem):
        pltpu.make_async_copy(dst, dst, rsem).wait()

    def owe(view, ssem):
        owed.append((view, ssem))

    def settle():
        for view, ssem in owed:
            arrived(view, ssem)
        owed.clear()

    xp, xm, xo = wrap(x + 1, PARTS), wrap(x - 1, PARTS), wrap(x + 2, PARTS)
    here = z * ny + y
    after, before = wrap(here + 1, nz * ny), wrap(here - 1, nz * ny)
    after_z, after_y = lax.div(after, ny), lax.rem(after, ny)
    before_z, before_y = lax.div(before, ny), lax.rem(before, ny)

    phase("greet")
    barrier = pltpu.get_barrier_semaphore()
    count = 0

    def greet(**where):
        names = {"z": "sp_0", "y": "sp_1", "x": "fs", "c": "tp"}
        pl.semaphore_signal(
            barrier, inc=1, device_id={names[k]: v for k, v in where.items()},
            device_id_type=pl.DeviceIdType.MESH,
        )
        return 1

    for d in range(1, ny):
        count += greet(y=wrap(y + d, ny))
    for d in range(1, nz):
        count += greet(z=wrap(z + d, nz))
    for v in (xp, xm, xo):
        count += greet(x=v)
    count += greet(c=other)
    count += greet(z=after_z, y=after_y)
    count += greet(z=before_z, y=before_y)

    own_channels = pl.ds(pl.multiple_of(x * LANES, LANES), LANES)
    own_groups = pl.ds(pl.multiple_of(x * 8, 8), 8)
    moves = [(tok_in, tok.at[x, c], 0), (doc_in, docs.at[x], 1), (gain_in, gains.at[c], 2)]
    places = [(wall_s, 0, 3)] + [(wall_c, k, 9) for k in range(3)] + [(wall_o, k, 10) for k in range(2)]
    for w, (wall, k, index) in zip((w_in_0, w_in_1, w_in_2, w_in_3, w_in_4, w_in_5), places):
        moves.append((w.at[:, own_channels], wall.at[z, y, :, pl.ds(k * LANES, LANES)], index))
    moves += [(decay_in.at[own_groups], rates.at[0], 4), (freq_in.at[own_groups], rates.at[1], 4)]
    for k, m in enumerate((in_re, in_im, read_re, read_im)):
        moves.append((m.at[own_groups], mats.at[k], 5))
    moves += [(step_in, step_row, 6), (taps_in.at[:, own_channels], taps, 7)]
    moves.append((skip_in.at[:, own_channels], skip, 8))
    for source, target, k in moves:
        pltpu.make_async_copy(source, target, local_sem.at[k]).start()
    phase("enter")
    for k, ref in enumerate((tok.at[x, c], docs.at[x], gains.at[c], wall_s.at[z, y])):
        arrived(ref, local_sem.at[k])
    for k, ref in enumerate((wall_c.at[z, y], wall_o.at[z, y])):
        arrived(ref, local_sem.at[9 + k])
    phase("barrier")
    pl.semaphore_wait(barrier, count)

    low, high = pl.ds(0, ROWS // 2), pl.ds(ROWS // 2, ROWS // 2)

    def column_copy(d):
        return pltpu.make_async_remote_copy(
            src_ref=chain2.at[z], dst_ref=chain2.at[z], send_sem=one_s.at[5], recv_sem=one_r.at[5],
            device_id={"sp_0": wrap(z + d, nz)}, device_id_type=pl.DeviceIdType.MESH,
        )

    def token_send(block, rows, way):
        ref = tok.at[block, c, rows]
        return ref, (xp if way == 0 else xm)

    def token_start(block, rows, way, turn):
        ref, target = token_send(block, rows, way)
        send(ref, ref, tok_s.at[0], tok_r.at[way, turn], x=target)

    def token_wait(block, rows, way, turn):
        arrived(tok.at[block, c, rows], tok_r.at[way, turn])

    def pass_over(block, turn):
        ref = tok.at[block, c]
        send(ref, ref, d2d_s.at[0], d2d_r.at[turn], c=other)

    def passed_over(block, turn):
        arrived(tok.at[block, other], d2d_r.at[turn])

    phase("first_sends")
    rows_a, rows_b = pl.ds(0, half), pl.ds(half, half)

    def blocks_view(wall, count):
        if count > nz * ny:
            return wall.at[pl.ds(0, count // (2 * ny))]
        if count % ny:
            return wall.at[0, pl.ds(0, count // 2)]
        return wall.at[pl.ds(0, count // ny), :, rows_a]

    def spread_view(wall, ab):
        if ab == 0:
            return wall.at[0, pl.ds(0, ny - 1), rows_a]
        return wall.at[pl.ds(0, nz - 1), 0, rows_b]

    def spread_out(turn, wall):
        for d in range(1, ny):
            ref = wall.at[z, y, rows_a]
            send(ref, ref, ph_s.at[turn], ph_r.at[turn, 0], y=wrap(y + d, ny))
        for d in range(1, nz):
            ref = wall.at[z, y, rows_b]
            send(ref, ref, ph_s.at[turn], ph_r.at[turn, 1], z=wrap(z + d, nz))
        owe(blocks_view(wall, ny - 1 + nz - 1), ph_s.at[turn])

    def spread_in(turn, wall, ab):
        arrived(spread_view(wall, ab), ph_r.at[turn, ab])

    for v in (xp, xm, xo):
        send(docs.at[x], docs.at[x], doc_s.at[0], doc_r.at[0], x=v)
    owe(docs.at[pl.ds(0, PARTS - 1)], doc_s.at[0])
    send(gains.at[c], gains.at[c], one_s.at[0], one_r.at[0], c=other)
    owe(gains.at[c], one_s.at[0])
    owe(tok.at[pl.ds(0, PARTS - 1), 0], tok_s.at[0])
    owe(tok.at[:, 0], d2d_s.at[0])
    spread_out(0, wall_s)
    token_start(x, low, 0, 0)
    token_start(x, high, 1, 0)
    pass_over(x, 0)
    spread_out(1, wall_c)
    token_start(x, high, 0, 1)
    token_start(x, low, 1, 1)
    spread_out(2, wall_o)

    phase("tables")
    shape = (ALL, ALL)
    r, n = lax.broadcasted_iota(jnp.int32, shape, 0), lax.broadcasted_iota(jnp.int32, shape, 1)
    natural = (r & 3) * ROWS + ((r >> 2) & 7) * 16 + (r >> 5)
    perm[...] = ones_where(n == natural).astype(BF16)
    t = (r >> 8) * (ROWS // 2) + (r & 63)
    turned = (t & 15) * 32 + (t >> 4) * 4 + ((r >> 6) & 3)
    unperm[...] = ones_where(n == turned).astype(BF16)
    for k, ref in enumerate((rates, mats, step_row, taps, skip)):
        arrived(ref, local_sem.at[4 + k])
    group = lax.broadcasted_iota(jnp.int32, (8, 32), 0) + x * 8
    step_log = jnp.broadcast_to(step_row[...], (8, 32))
    mine_only = lax.broadcasted_iota(jnp.int32, (8, 32), 1) == group
    step = jnp.exp(jnp.sum(jnp.where(mine_only, step_log, 0.0), axis=1, keepdims=True))
    decay, frequency = rates[0], rates[1]
    damping, turning = decay * step, frequency * step
    fading = jnp.exp(-damping)
    coef_real, coef_imag = fading * jnp.cos(turning), fading * jnp.sin(turning)
    half_sine = jnp.sin(turning * 0.5)
    series = jnp.ones_like(damping)
    for k in range(11, 1, -1):
        series = 1.0 - damping * (1.0 / k) * series
    less_real = -damping * series * jnp.cos(turning) - 2.0 * half_sine * half_sine
    denominator = decay * decay + frequency * frequency
    ratio_real = (-less_real * decay + coef_imag * frequency) / denominator
    ratio_imag = (-coef_imag * decay - less_real * frequency) / denominator

    def widened(value):
        value = jnp.concatenate([value, value], axis=1)
        return jnp.concatenate([value] * (STATES // LANES), axis=1)

    own_lane = (
        lax.broadcasted_iota(jnp.int32, (8, STATES), 1) >> 6
    ) == lax.broadcasted_iota(jnp.int32, (8, STATES), 0)

    def flat(value):
        return jnp.sum(jnp.where(own_lane, widened(value), 0.0), axis=0, keepdims=True)

    power_re, power_im, squared = coef_real, coef_imag, 1
    for index, length in enumerate((1, 16, ROWS, ROWS * ny)):
        while squared < length:
            power_re, power_im = power_re * power_re - power_im * power_im, 2.0 * power_re * power_im
            squared *= 2
        lam[2 * index : 2 * index + 1, :] = flat(power_re)
        lam[2 * index + 1 : 2 * index + 2, :] = flat(power_im)
    ratio_real, ratio_imag = flat(ratio_real), flat(ratio_imag)
    own_state = (lax.broadcasted_iota(jnp.int32, (LANES, STATES), 0) >> 4) == (
        lax.broadcasted_iota(jnp.int32, (LANES, STATES), 1) >> 6
    )
    input_real, input_imag = (widened(mats[k].reshape(LANES, 64)) for k in range(2))
    bmat[:, :STATES] = jnp.where(own_state, ratio_real * input_real - ratio_imag * input_imag, 0.0).astype(BF16)
    bmat[:, STATES:] = jnp.where(own_state, ratio_real * input_imag + ratio_imag * input_real, 0.0).astype(BF16)
    rmat[:, :STATES] = jnp.where(own_state, widened(mats[2].reshape(LANES, 64)), 0.0).astype(BF16)
    rmat[:, STATES:] = jnp.where(own_state, -widened(mats[3].reshape(LANES, 64)), 0.0).astype(BF16)

    def ring_ref(ab, source, wall, piece):
        count = (ny, nz)[ab]
        cut = {0: pl.ds(0, count), 1: pl.ds(0, count // 2), 2: pl.ds(count // 2, count // 2)}[piece]
        if ab == 0:
            return wall.at[source, cut, rows_a]
        return wall.at[cut, source, rows_b]

    walls = (wall_c, wall_c, wall_o)

    def ring_hops(which, k):
        for ab in range(2):
            me, size = ((z, nz), (y, ny))[ab]
            last = size // 2 - 1
            for way in range(2):
                if k > last or (k == last and which == 1 - way):
                    continue
                piece = which + 1 if which < 2 else (1 + way if k == last else 0)
                yield ab, way, me, size, piece

    def ring_start(which, k):
        for ab, way, me, size, piece in ring_hops(which, k):
            sign = 1 - 2 * way
            ref = ring_ref(ab, wrap(me - sign * k, size), walls[which], piece)
            send(ref, ref, ring_s.at[which], ring_r.at[which, k], **{"zy"[ab]: wrap(me + sign, size)})

    def ring_blocks(which, k):
        return sum((ny, nz)[ab] // (2 if piece else 1) for ab, _, _, _, piece in ring_hops(which, k))

    def ring_wait(which, k):
        if ring_blocks(which, k):
            arrived(blocks_view(walls[which], ring_blocks(which, k)), ring_r.at[which, k])

    def state_hops(ab, stage):
        me, size = ((z, nz), (y, ny))[ab]
        reach = 1 if size < 4 else 2
        for way in range(2):
            for d in range(1, size // 2 + 1):
                if (d > reach) != (stage == 1):
                    continue
                piece = 1 + way if d == size // 2 else 0
                yield way, d, piece, me, size

    def state_start(ab, stage):
        for way, d, piece, me, size in state_hops(ab, stage):
            sign = 1 - 2 * way
            source = wrap(me - sign * 2, size) if stage else me
            ref = ring_ref(ab, source, wall_s, piece)
            target = wrap(me + sign * (d - 2 * stage), size)
            send(ref, ref, st_s.at[0], st_r.at[ab, stage], **{"zy"[ab]: target})

    def state_blocks(ab, stage):
        return sum((ny, nz)[ab] // (2 if piece else 1) for _, _, piece, _, _ in state_hops(ab, stage))

    def state_wait(ab, stage):
        if state_blocks(ab, stage):
            arrived(blocks_view(wall_s, state_blocks(ab, stage)), st_r.at[ab, stage])

    def service(which, k):
        ring_wait(which, k)
        ring_start(which, k + 1)

    def peer_pieces(turn):
        if turn == 0:
            return [(z, slice(None), rows_a), (slice(None), y, rows_b)]
        found = []
        for ab, way, me, size, piece in ring_hops(2, turn - 1):
            source = wrap(me - (1 - 2 * way) * turn, size)
            span = (ny, nz)[ab]
            cut = {0: pl.ds(0, span), 1: pl.ds(0, span // 2), 2: pl.ds(span // 2, span // 2)}[piece]
            found.append((source, cut, rows_a) if ab == 0 else (cut, source, rows_b))
        return found

    def peer_start(turn):
        for p in peer_pieces(turn):
            send(wall_o.at[p], wpeer.at[p], peer_s.at[0], peer_r.at[0], c=other)

    width = 2 * tok.shape[3]

    def norm(block):
        def some_rows(i, carry):
            rows = pl.ds(pl.multiple_of(i * 32, 32), 32)
            a, b = tok[block, 0, rows, :].astype(F32), tok[block, 1, rows, :].astype(F32)
            mean = (jnp.sum(a * a, axis=1, keepdims=True) + jnp.sum(b * b, axis=1, keepdims=True)) / width
            scale = lax.rsqrt(mean + EPS)
            target = pl.ds(pl.multiple_of(block * ROWS + i * 32, 32), 32)
            normed[target, : width // 2] = (a * scale * gain_rows[0]).astype(BF16)
            normed[target, width // 2 :] = (b * scale * gain_rows[1]).astype(BF16)
            return carry

        lax.fori_loop(0, ROWS // 32, some_rows, 0)

    phase("norm_own")
    arrived(gains.at[other], one_r.at[0])
    for k in range(2):
        wide = gains[k].astype(F32)
        gain_rows[k] = jnp.concatenate([wide[i : i + 1] for i in range(wide.shape[0])], axis=1)
    passed_over(x, 0)
    norm(x)
    phase("phase1_state")
    for ab in range(2):
        spread_in(0, wall_s, ab)
        state_start(ab, 0)
    phase("tok_forward")
    token_wait(xm, low, 0, 0)
    token_start(xm, low, 0, 2)
    token_wait(xp, high, 1, 0)
    token_start(xp, high, 1, 2)
    phase("phase1_rest")
    spread_in(1, wall_c, 0)
    spread_in(1, wall_c, 1)
    for which in range(2):
        ring_start(which, 0)
    phase("tok_wait1")
    token_wait(xm, high, 0, 1)
    pass_over(xm, 1)
    token_wait(xp, low, 1, 1)
    pass_over(xp, 2)

    phase("documents")
    arrived(docs.at[pl.ds(0, PARTS - 1)], doc_r.at[0])
    row = lax.broadcasted_iota(jnp.int32, (ALL, ROWS), 0)
    lane = lax.broadcasted_iota(jnp.int32, (ALL, ROWS), 1)
    pick_t = ones_where(lane == ((row >> 2) & 7) * 16 + (row >> 5))
    part_row = lax.broadcasted_iota(jnp.int32, (ROWS, ROWS), 0)
    spread_docs = jnp.zeros((ROWS, ROWS), F32)
    for q in range(PARTS):
        spread_docs = jnp.where(part_row == q, docs[q].astype(F32), spread_docs)
    by_part = nt(pick_t.astype(BF16), spread_docs.astype(BF16))
    by_part = by_part * ones_where(lane == (row & 3))
    docext[64:] = nn(by_part.astype(BF16), jnp.ones((ROWS, LANES), BF16))
    docext[4:32] = docext[64 + 448 : 64 + 476]
    docext[36:64] = docext[64 + 480 : 64 + 508]

    phase("phase1_out")
    spread_in(2, wall_o, 0)
    spread_in(2, wall_o, 1)
    ring_start(2, 0)
    peer_start(0)
    phase("state_stage")
    for ab in range(2):
        state_wait(ab, 0)
        state_start(ab, 1)
    phase("norm_mid")
    passed_over(xm, 1)
    norm(xm)
    phase("tok_wait2")
    token_wait(xo, low, 0, 2)
    token_wait(xo, high, 1, 2)
    pass_over(xo, 3)
    phase("norm_mid2")
    passed_over(xp, 2)
    norm(xp)
    phase("ring_ab0")
    service(0, 0)
    service(1, 0)
    phase("norm_last")
    passed_over(xo, 3)
    norm(xo)

    phase("ring_o0")
    service(2, 0)
    peer_start(1)
    phase("state_w_wait")
    for ab in range(2):
        state_wait(ab, 1)
    phase("state_in")
    total_depth = nz * ny * depth
    state_in = wall_s[...].reshape(total_depth, LANES)
    in_order = halves(nn, perm, halves(nn, normed, state_in).astype(BF16))
    driven[...] = in_order
    phase("ring_ab1")
    service(0, 1)
    service(1, 1)
    phase("push")
    pushed[...] = nn(in_order.astype(BF16), bmat[...])

    def lane_cut(k):
        return slice(k * LANES, (k + 1) * LANES), slice(STATES + k * LANES, STATES + (k + 1) * LANES)

    def rows_at(k):
        return slice(k * 32, (k + 1) * 32)

    def docs_at(k):
        return docext[64 + k * 32 : 96 + k * 32]

    phase("scan")
    for cut in range(STATES // LANES):
        re, im = lane_cut(cut)
        a_re, a_im = lam[0:1, re], lam[1:2, re]
        s_re, s_im = pushed[0:32, re], pushed[0:32, im]
        for k in range(1, 16):
            keep = ones_where(docs_at(k) == docs_at(k - 1))
            s_re, s_im = (
                pushed[rows_at(k), re] + keep * (a_re * s_re - a_im * s_im),
                pushed[rows_at(k), im] + keep * (a_re * s_im + a_im * s_re),
            )
            pushed[rows_at(k), re] = s_re
            pushed[rows_at(k), im] = s_im
    for seg in range(8):
        rows = slice(480 + seg * 4, 484 + seg * 4)
        ends[seg, 0:4, :STATES] = pushed[rows, :STATES]
        ends[seg, 4:8, :STATES] = pushed[rows, STATES:]
        last = docext[544 + seg * 4 : 548 + seg * 4]
        ends[seg, 0:4, STATES:] = last
        ends[seg, 4:8, STATES:] = last

    phase("fold_local")
    sign = jnp.where(lax.broadcasted_iota(jnp.int32, (8, STATES), 0) < 4, -1.0, 1.0)

    def joined(carry, piece, power):
        held, doc = carry
        piece, now = piece
        link = ones_where(now == doc)
        link = jnp.concatenate([link] * (STATES // LANES), axis=1)
        a_re, a_im = lam[2 * power : 2 * power + 1, :], lam[2 * power + 1 : 2 * power + 2, :]
        moved = a_re * held + (a_im * sign) * pltpu.roll(held, 4, 0)
        return piece + link * moved, now

    def of_ends(k):
        return ends[k, :, :STATES], ends[k, :, STATES:]

    wing = STATES // 2

    def pack(buffer, index, carry):
        held, doc = carry
        buffer[index, 0:8, :wing] = held[:, :wing].astype(BF16)
        buffer[index, 8:16, :wing] = held[:, wing:].astype(BF16)
        buffer[index, 0:8, wing:] = doc.astype(BF16)
        buffer[index, 8:16, wing:] = doc.astype(BF16)

    def of(buffer):
        def read(k):
            message = buffer[k].astype(F32)
            held = jnp.concatenate([message[0:8, :wing], message[8:16, :wing]], axis=1)
            return held, message[0:8, wing:]

        return read

    def fold(carry, pieces, count, limit, power):
        def step(k, carry):
            new = joined(carry, pieces(k), power)
            return tuple(jnp.where(k < limit, a, b) for a, b in zip(new, carry))

        return lax.fori_loop(0, count, step, carry)

    nothing = (jnp.zeros((8, STATES), F32), jnp.full((8, LANES), -1.0, F32))
    pack(chain1, y, fold(nothing, of_ends, 8, 8, 1))
    for d in range(1, ny):
        send(chain1.at[y], chain1.at[y], one_s.at[1], one_r.at[1], y=wrap(y + d, ny))
    phase("ring_o1")
    service(2, 1)
    peer_start(2)

    phase("ring_ab2")
    service(0, 2)
    service(1, 2)
    phase("chain1_wait")
    owe(chain1.at[pl.ds(0, ny - 1)], one_s.at[1])
    arrived(chain1.at[pl.ds(0, ny - 1)], one_r.at[1])
    pack(chain2, z, fold(nothing, of(chain1), ny, ny, 2))
    for d in range(1, nz):

        @pl.when(z + d < nz)
        def _(d=d):
            column_copy(d).start()
    phase("ring_o2")
    service(2, 2)
    peer_start(3)
    phase("ring_ab3")
    for k in range(3, most // 2):
        service(0, k)
        service(1, k)

    phase("conv_in")
    conv_in = wall_c[...].reshape(total_depth, 3 * LANES)
    projected = nn(perm[...], nn(normed[...], conv_in).astype(BF16))
    gate[...] = projected[:, :LANES]
    prodext[64:] = (projected[:, LANES : 2 * LANES] * projected[:, 2 * LANES :]).astype(BF16).astype(F32)
    rim_out[0:4, :LANES] = prodext[64 + 476 : 64 + 480]
    rim_out[4:8, :LANES] = prodext[64 + 508 : 64 + 512]
    rim_out[0:4, LANES:] = docext[64 + 476 : 64 + 480]
    rim_out[4:8, LANES:] = docext[64 + 508 : 64 + 512]
    prodext[4:32] = prodext[64 + 448 : 64 + 476]
    prodext[36:64] = prodext[64 + 480 : 64 + 508]
    send(rim_out, rim_in, one_s.at[2], one_r.at[2], z=after_z, y=after_y)
    owe(rim_out, one_s.at[2])
    phase("chain2_wait")
    incoming[:, :STATES], incoming[:, STATES:] = nothing
    for d in range(1, nz):

        @pl.when(z == d)
        def _(d=d):
            arrived(chain2.at[pl.ds(0, d)], one_r.at[5])

    phase("chain2_fold")

    @pl.when(z > 0)
    def _():
        def step(k, carry):
            return joined(carry, of(chain2)(k), 3)

        incoming[:, :STATES], incoming[:, STATES:] = lax.fori_loop(0, z, step, nothing)

    state = fold((incoming[:, :STATES], incoming[:, STATES:]), of(chain1), ny, y, 2)
    docext[32:36] = state[1][0:4]
    for seg in range(8):
        links[seg] = state[0]
        state = joined(state, of_ends(seg), 1)
    for seg in range(8):
        links[8 + seg // 2, (seg % 2) * 4 : (seg % 2) * 4 + 4] = links[seg, 0:4]
        links[12 + seg // 2, (seg % 2) * 4 : (seg % 2) * 4 + 4] = links[seg, 4:8]
    phase("fixup")
    previous = docext[32:64]
    for cut in range(STATES // LANES):
        re, im = lane_cut(cut)
        a_re, a_im = lam[0:1, re], lam[1:2, re]
        w_re = links[8:12, :, re].reshape(32, LANES)
        w_im = links[12:16, :, re].reshape(32, LANES)
        for k in range(16):
            w_re, w_im = a_re * w_re - a_im * w_im, a_re * w_im + a_im * w_re
            reach = ones_where(docs_at(k) == previous)
            pushed[rows_at(k), re] = pushed[rows_at(k), re] + reach * w_re
            pushed[rows_at(k), im] = pushed[rows_at(k), im] + reach * w_im
    phase("readout")
    reading = halves(nt, pushed[...].astype(BF16), rmat[...]) + skip[...] * driven[...]
    inner = 0.7978845608028654 * (reading + 0.044715 * (reading * reading * reading))
    ssm_out = (0.5 * reading * (1.0 + jnp.tanh(inner))).astype(BF16)
    acts[:, LANES:] = halves(nn, unperm, ssm_out).astype(BF16)
    mine, theirs = (pl.ds(pl.multiple_of(v * (ALL // 2), ALL // 2), ALL // 2) for v in (c, other))
    conv_lanes, ssm_lanes = pl.ds(0, LANES), pl.ds(LANES, LANES)
    send(acts.at[theirs, ssm_lanes], pacts.at[:, ssm_lanes], one_s.at[4], one_r.at[4], c=other)
    owe(pacts.at[:, ssm_lanes], one_s.at[4])

    phase("ring_o3")
    for k in range(3, most // 2):
        service(2, k)
        peer_start(k + 1)

    phase("rim_wait")
    docext[0:4] = jnp.full((4, LANES), -1.0, F32)
    prodext[0:4] = jnp.zeros((4, LANES), F32)
    prodext[32:36] = jnp.zeros((4, LANES), F32)

    @pl.when(here > 0)
    def _():
        arrived(rim_in, one_r.at[2])
        prodext[0:4] = rim_in[0:4, :LANES]
        prodext[32:36] = rim_in[4:8, :LANES]
        docext[0:4] = rim_in[0:4, LANES:]

    phase("conv")
    now = docext[64:]
    mixed = (
        taps[0:1].astype(F32) * prodext[0:ALL] * ones_where(docext[0:ALL] == now)
        + taps[1:2].astype(F32) * prodext[32 : 32 + ALL] * ones_where(docext[32 : 32 + ALL] == now)
        + taps[2:3].astype(F32) * prodext[64:]
    )
    conv_out = (gate[...] * mixed).astype(BF16)
    acts[:, :LANES] = halves(nn, unperm, conv_out).astype(BF16)
    send(acts.at[theirs, conv_lanes], pacts.at[:, conv_lanes], one_s.at[3], one_r.at[3], c=other)
    owe(pacts.at[:, conv_lanes], one_s.at[3])

    columns = total_depth // 4

    def quarter(ref, cut):
        if nz % 4 == 0:
            return ref[cut * nz // 4 : (cut + 1) * nz // 4].reshape(columns, 2 * LANES)
        return ref[cut // 2, cut % 2]

    phase("peer_w_wait")
    arrived(wpeer, peer_r.at[0])
    for cut in (0, 2, 1, 3):
        phase(f"out_proj{cut}")
        total = nt(acts[mine, :], quarter(wall_o, cut))
        if cut == 0:
            phase("pact_wait")
            arrived(pacts.at[:, ssm_lanes], one_r.at[4])
            arrived(pacts.at[:, conv_lanes], one_r.at[3])
        total = total + nt(pacts[...], quarter(wpeer, cut))
        part[cut] = total.astype(BF16).reshape(PARTS, ROWS // 2, columns)
        way, turn = cut // 2, cut % 2
        target = (xp, xm)[way]
        send(part.at[cut, xo], relay.at[way, turn], rs_s.at[0], rs_r.at[2 * way + turn], x=target)
    for turn in range(2):
        send(part.at[2 + turn, xp], final.at[0, 2 + turn], rs_s.at[0], rs_r.at[6 + turn], x=xp)
        send(part.at[turn, xm], final.at[1, turn], rs_s.at[0], rs_r.at[4 + turn], x=xm)
    for which in range(3):
        count = sum(ring_blocks(which, k) for k in range(most // 2))
        owe(blocks_view(walls[which], count), ring_s.at[which])
    owe(blocks_view(wall_s, sum(state_blocks(ab, stage) for ab in range(2) for stage in range(2))), st_s.at[0])
    owe(wpeer, peer_s.at[0])
    settle()
    for turn in range(2):
        for way, target in ((0, xp), (1, xm)):
            phase(f"relay{way}{turn}")
            cut = 2 * way + turn
            arrived(relay.at[way, turn], rs_r.at[2 * way + turn])
            both = part[cut, target].astype(F32) + relay[way, turn].astype(F32)
            part[cut, target] = both.astype(BF16)
            send(part.at[cut, target], final.at[way, cut], rs_s.at[0], rs_r.at[4 + cut], x=target)
    for cut in (0, 2, 1, 3):
        phase(f"final{cut}")
        arrived(final.at[:, cut], rs_r.at[4 + cut])
        value = part[cut, x].astype(F32) + final[0, cut].astype(F32) + final[1, cut].astype(F32)
        out[:, cut * columns : (cut + 1) * columns] = value.astype(BF16)
    phase("drain")
    arrived(part.at[pl.ds(0, 3)], rs_s.at[0])

    @pl.when(here == 0)
    def _():
        arrived(rim_in, one_r.at[2])

    for d in range(1, nz):

        @pl.when(z + d == nz - 1)
        def _(d=d):
            arrived(chain2.at[pl.ds(0, d)], one_s.at[5])

    phase(None)


def shards(
    nz, ny, tokens, documents, norm_gain, out_gate_weight, in_gate_weight, value_weight,
    conv_taps, state_in_weight, decay_rate, frequency, step_log, input_real, input_imag,
    readout_real, readout_imag, skip_gain, conv_out_weight, state_out_weight,
):
    depth = state_in_weight.shape[0]
    width = tokens.shape[1]
    columns = nz * ny * depth // 4
    vmem = pl.BlockSpec(memory_space=pltpu.VMEM)
    hbm = pl.BlockSpec(memory_space=pltpu.HBM)
    dma = pltpu.SemaphoreType.DMA
    steps = max(nz, ny) // 2
    return pl.pallas_call(
        functools.partial(mixer_kernel, nz, ny, depth),
        out_shape=jax.ShapeDtypeStruct((ROWS // 2, 4 * columns), BF16),
        in_specs=[hbm] * 18,
        out_specs=vmem,
        scratch_shapes=[
            pltpu.VMEM((2, 8, 64), F32),
            pltpu.VMEM((1, 32), F32),
            pltpu.VMEM((4, 8, 16, 64), F32),
            pltpu.VMEM((3, LANES), BF16),
            pltpu.VMEM((1, LANES), F32),
            pltpu.VMEM((8, STATES), F32),
            pltpu.VMEM((PARTS, 2, ROWS, width), BF16),
            pltpu.VMEM((2, width // LANES, LANES), BF16),
            pltpu.VMEM((2, 1, width), F32),
            pltpu.VMEM((PARTS, 1, ROWS), jnp.int32),
            pltpu.VMEM((nz, ny, depth, LANES), BF16),
            pltpu.VMEM((nz, ny, depth, 3 * LANES), BF16),
            pltpu.VMEM((nz, ny, depth, 2 * LANES), BF16),
            pltpu.VMEM((nz, ny, depth, 2 * LANES), BF16),
            pltpu.VMEM((ALL, 2 * width), BF16),
            pltpu.VMEM((ALL, ALL), BF16),
            pltpu.VMEM((ALL, ALL), BF16),
            pltpu.VMEM((LANES, 2 * STATES), BF16),
            pltpu.VMEM((LANES, 2 * STATES), BF16),
            pltpu.VMEM((ALL, LANES), F32),
            pltpu.VMEM((ALL, 2 * STATES), F32),
            pltpu.VMEM((64 + ALL, LANES), F32),
            pltpu.VMEM((64 + ALL, LANES), F32),
            pltpu.VMEM((ALL, LANES), F32),
            pltpu.VMEM((8, 8, STATES + LANES), F32),
            pltpu.VMEM((ny, 16, STATES // 2 + LANES), BF16),
            pltpu.VMEM((nz, 16, STATES // 2 + LANES), BF16),
            pltpu.VMEM((8, STATES + LANES), F32),
            pltpu.VMEM((16, 8, STATES), F32),
            pltpu.VMEM((8, 2 * LANES), F32),
            pltpu.VMEM((8, 2 * LANES), F32),
            pltpu.VMEM((ALL, 2 * LANES), BF16),
            pltpu.VMEM((ALL // 2, 2 * LANES), BF16),
            pltpu.VMEM((4, PARTS, ROWS // 2, columns), BF16),
            pltpu.VMEM((2, 2, ROWS // 2, columns), BF16),
            pltpu.VMEM((2, 4, ROWS // 2, columns), BF16),
            dma((11,)),
            dma((1,)), dma((2, 3)),
            dma((1,)), dma((PARTS,)),
            dma((1,)), dma((1,)),
            dma((6,)), dma((6,)),
            dma((3,)), dma((3, 2)),
            dma((1,)), dma((2, 2)),
            dma((3,)), dma((3, steps)),
            dma((1,)), dma((1,)),
            dma((1,)), dma((8,)),
        ],
        compiler_params=pltpu.CompilerParams(
            collective_id=0, has_side_effects=True, vmem_limit_bytes=40 * 1024 * 1024
        ),
        name="mixer",
    )(*(
        pltpu.with_memory_space_constraint(operand, pltpu.HBM) for operand in (
            tokens, state_in_weight, out_gate_weight, in_gate_weight, value_weight, conv_out_weight.T,
            state_out_weight.T, documents[None, :], norm_gain.reshape(-1, LANES), decay_rate, frequency,
            step_log[None, :], input_real.transpose(0, 2, 1), input_imag.transpose(0, 2, 1),
            readout_real, readout_imag, conv_taps, skip_gain[None, :],
        )
    ))


def solution(mesh, nz=8, ny=8):
    torus = Mesh(
        mesh.devices.reshape(nz, ny, mesh.shape["fs"], mesh.shape["tp"]), ("sp_0", "sp_1", "fs", "tp")
    )
    in_specs = (
        P(FS_SP, "tp"),
        P(FS_SP),
        P("tp"),
        P(SP, "tp"),
        P(SP, "tp"),
        P(SP, "tp"),
        P(None, "tp"),
        P(SP, "tp"),
        P("tp", None),
        P("tp", None),
        P("tp"),
        P("tp", None, None),
        P("tp", None, None),
        P("tp", None, None),
        P("tp", None, None),
        P("tp"),
        P("tp", SP),
        P("tp", SP),
    )
    return jax.shard_map(
        functools.partial(shards, nz, ny), mesh=torus, in_specs=in_specs,
        out_specs=P(FS_SP_TP, None), check_vma=False,
    )
```

```python
import functools

import jax
import jax.numpy as jnp
from jax import lax
from jax.experimental import pallas as pl
from jax.experimental.pallas import tpu as pltpu
from jax.sharding import Mesh
from jax.sharding import PartitionSpec as P

SP = ("sp_0", "sp_1")
FS_SP = ("fs", "sp_0", "sp_1")
FS_SP_TP = ("fs", "sp_0", "sp_1", "tp")
EPS = 1e-06
PARTS = 4
ROWS = 128
LANES = 128
STATES = 512
ALL = PARTS * ROWS
BF16 = jnp.bfloat16
F32 = jnp.float32


def nn(a, b):
    return jnp.dot(a, b, preferred_element_type=F32)


def halves(product, a, b):
    middle = a.shape[0] // 2
    return jnp.concatenate([product(a[:middle], b), product(a[middle:], b)])


def nt(a, b):
    return lax.dot_general(a, b, (((1,), (1,)), ((), ())), preferred_element_type=F32)


def ones_where(mask):
    return jnp.where(mask, 1.0, 0.0)


def mixer_kernel(
    nz, ny, depth, tok_in, w_in_0, w_in_1, w_in_2, w_in_3, w_in_4, w_in_5, doc_in, gain_in,
    decay_in, freq_in, step_in, in_re, in_im, read_re, read_im, taps_in, skip_in, out,
    rates, step_row, mats, taps, skip, lam, tok, gains, gain_rows, docs, wall_s, wall_c, wall_o, wpeer, normed, perm, unperm, bmat, rmat, driven, pushed,
    docext, prodext, gate, ends, chain1, chain2, incoming, links, rimtok, rimdoc, rimprod, acts, pacts,
    part, relay, final, local_sem, tok_s, tok_r, d2d_s, d2d_r, doc_s, doc_r, one_s, one_r,
    ph_s, ph_r, st_s, st_r, ring_s, ring_r, peer_s, peer_r, rs_s, rs_r, rim_s, rim_r,
):
    z, y = lax.axis_index("sp_0"), lax.axis_index("sp_1")
    x, c = lax.axis_index("fs"), lax.axis_index("tp")
    half = depth // 2
    most = max(nz, ny)
    other = 1 - c
    owed, scopes = [], []

    def phase(name):
        if scopes:
            scopes.pop().__exit__(None, None, None)
        if name:
            scopes.append(jax.named_scope(name))
            scopes[-1].__enter__()

    def wrap(v, n):
        return lax.rem(v + 4 * n, n)

    def send(src, dst, ssem, rsem, **where):
        names = {"z": "sp_0", "y": "sp_1", "x": "fs", "c": "tp"}
        copy = pltpu.make_async_remote_copy(
            src_ref=src, dst_ref=dst, send_sem=ssem, recv_sem=rsem,
            device_id={names[k]: v for k, v in where.items()},
            device_id_type=pl.DeviceIdType.MESH,
        )
        copy.start()

    def arrived(dst, rsem):
        pltpu.make_async_copy(dst, dst, rsem).wait()

    def owe(view, ssem):
        owed.append((view, ssem))

    def settle():
        for view, ssem in owed:
            arrived(view, ssem)
        owed.clear()

    xp, xm, xo = wrap(x + 1, PARTS), wrap(x - 1, PARTS), wrap(x + 2, PARTS)
    here = z * ny + y
    after, before = wrap(here + 1, nz * ny), wrap(here - 1, nz * ny)
    after_z, after_y = lax.div(after, ny), lax.rem(after, ny)
    before_z, before_y = lax.div(before, ny), lax.rem(before, ny)

    phase("greet")
    barrier = pltpu.get_barrier_semaphore()
    count = 0

    def greet(**where):
        names = {"z": "sp_0", "y": "sp_1", "x": "fs", "c": "tp"}
        pl.semaphore_signal(
            barrier, inc=1, device_id={names[k]: v for k, v in where.items()},
            device_id_type=pl.DeviceIdType.MESH,
        )
        return 1

    for d in range(1, ny):
        count += greet(y=wrap(y + d, ny))
    for d in range(1, nz):
        count += greet(z=wrap(z + d, nz))
    for v in (xp, xm, xo):
        count += greet(x=v)
    count += greet(c=other)
    count += greet(z=after_z, y=after_y)
    count += greet(z=before_z, y=before_y)

    own_channels = pl.ds(pl.multiple_of(x * LANES, LANES), LANES)
    own_groups = pl.ds(pl.multiple_of(x * 8, 8), 8)
    moves = [(tok_in, tok.at[x, c], 0), (doc_in, docs.at[x], 1), (gain_in, gains.at[c], 2)]
    places = [(wall_s, 0, 3)] + [(wall_c, k, 9) for k in range(3)] + [(wall_o, k, 10) for k in range(2)]
    for w, (wall, k, index) in zip((w_in_0, w_in_1, w_in_2, w_in_3, w_in_4, w_in_5), places):
        moves.append((w.at[:, own_channels], wall.at[z, y, :, pl.ds(k * LANES, LANES)], index))
    moves += [(decay_in.at[own_groups], rates.at[0], 4), (freq_in.at[own_groups], rates.at[1], 4)]
    for k, m in enumerate((in_re, in_im, read_re, read_im)):
        moves.append((m.at[own_groups], mats.at[k], 5))
    moves += [(step_in, step_row, 6), (taps_in.at[:, own_channels], taps, 7)]
    moves.append((skip_in.at[:, own_channels], skip, 8))
    for source, target, k in moves:
        pltpu.make_async_copy(source, target, local_sem.at[k]).start()
    phase("enter")
    for k, ref in enumerate((tok.at[x, c], docs.at[x], gains.at[c], wall_s.at[z, y])):
        arrived(ref, local_sem.at[k])
    for k, ref in enumerate((wall_c.at[z, y], wall_o.at[z, y])):
        arrived(ref, local_sem.at[9 + k])
    phase("barrier")
    pl.semaphore_wait(barrier, count)

    low, high = pl.ds(0, ROWS // 2), pl.ds(ROWS // 2, ROWS // 2)

    def column_copy(d):
        return pltpu.make_async_remote_copy(
            src_ref=chain2.at[z], dst_ref=chain2.at[z], send_sem=one_s.at[5], recv_sem=one_r.at[5],
            device_id={"sp_0": wrap(z + d, nz)}, device_id_type=pl.DeviceIdType.MESH,
        )

    def token_send(block, rows, way):
        ref = tok.at[block, c, rows]
        return ref, (xp if way == 0 else xm)

    def token_start(block, rows, way, turn):
        ref, target = token_send(block, rows, way)
        send(ref, ref, tok_s.at[0], tok_r.at[way, turn], x=target)

    def token_wait(block, rows, way, turn):
        arrived(tok.at[block, c, rows], tok_r.at[way, turn])

    def pass_over(block, turn):
        ref = tok.at[block, c]
        send(ref, ref, d2d_s.at[0], d2d_r.at[turn], c=other)

    def passed_over(block, turn):
        arrived(tok.at[block, other], d2d_r.at[turn])

    phase("first_sends")
    rows_a, rows_b = pl.ds(0, half), pl.ds(half, half)

    def blocks_view(wall, count):
        if count > nz * ny:
            return wall.at[pl.ds(0, count // (2 * ny))]
        if count % ny:
            return wall.at[0, pl.ds(0, count // 2)]
        return wall.at[pl.ds(0, count // ny), :, rows_a]

    def spread_view(wall, ab):
        if ab == 0:
            return wall.at[0, pl.ds(0, ny - 1), rows_a]
        return wall.at[pl.ds(0, nz - 1), 0, rows_b]

    def spread_out(turn, wall):
        for d in range(1, ny):
            ref = wall.at[z, y, rows_a]
            send(ref, ref, ph_s.at[turn], ph_r.at[turn, 0], y=wrap(y + d, ny))
        for d in range(1, nz):
            ref = wall.at[z, y, rows_b]
            send(ref, ref, ph_s.at[turn], ph_r.at[turn, 1], z=wrap(z + d, nz))
        owe(blocks_view(wall, ny - 1 + nz - 1), ph_s.at[turn])

    def spread_in(turn, wall, ab):
        arrived(spread_view(wall, ab), ph_r.at[turn, ab])

    for v in (xp, xm, xo):
        send(docs.at[x], docs.at[x], doc_s.at[0], doc_r.at[0], x=v)
    owe(docs.at[pl.ds(0, PARTS - 1)], doc_s.at[0])
    send(gains.at[c], gains.at[c], one_s.at[0], one_r.at[0], c=other)
    owe(gains.at[c], one_s.at[0])
    owe(tok.at[pl.ds(0, PARTS - 1), 0], tok_s.at[0])
    owe(tok.at[:, 0], d2d_s.at[0])
    spread_out(0, wall_s)
    token_start(x, low, 0, 0)
    token_start(x, high, 1, 0)
    pass_over(x, 0)
    spread_out(1, wall_c)
    token_start(x, high, 0, 1)
    token_start(x, low, 1, 1)
    spread_out(2, wall_o)
    last_rows = tok.at[x, c, pl.ds(ROWS - 16, 16)]
    send(last_rows, rimtok.at[x, c], rim_s.at[0], rim_r.at[0], z=after_z, y=after_y)
    send(docs.at[x], rimdoc.at[x], rim_s.at[1], rim_r.at[1], z=after_z, y=after_y)
    owe(last_rows, rim_s.at[0])
    owe(docs.at[x], rim_s.at[1])

    phase("tables")
    shape = (ALL, ALL)
    r, n = lax.broadcasted_iota(jnp.int32, shape, 0), lax.broadcasted_iota(jnp.int32, shape, 1)
    natural = (r & 3) * ROWS + ((r >> 2) & 7) * 16 + (r >> 5)
    perm[...] = ones_where(n == natural).astype(BF16)
    t = (r >> 8) * (ROWS // 2) + (r & 63)
    turned = (t & 15) * 32 + (t >> 4) * 4 + ((r >> 6) & 3)
    unperm[...] = ones_where(n == turned).astype(BF16)
    for k, ref in enumerate((rates, mats, step_row, taps, skip)):
        arrived(ref, local_sem.at[4 + k])
    group = lax.broadcasted_iota(jnp.int32, (8, 32), 0) + x * 8
    step_log = jnp.broadcast_to(step_row[...], (8, 32))
    mine_only = lax.broadcasted_iota(jnp.int32, (8, 32), 1) == group
    step = jnp.exp(jnp.sum(jnp.where(mine_only, step_log, 0.0), axis=1, keepdims=True))
    decay, frequency = rates[0], rates[1]
    damping, turning = decay * step, frequency * step
    fading = jnp.exp(-damping)
    coef_real, coef_imag = fading * jnp.cos(turning), fading * jnp.sin(turning)
    half_sine = jnp.sin(turning * 0.5)
    series = jnp.ones_like(damping)
    for k in range(11, 1, -1):
        series = 1.0 - damping * (1.0 / k) * series
    less_real = -damping * series * jnp.cos(turning) - 2.0 * half_sine * half_sine
    denominator = decay * decay + frequency * frequency
    ratio_real = (-less_real * decay + coef_imag * frequency) / denominator
    ratio_imag = (-coef_imag * decay - less_real * frequency) / denominator

    def widened(value):
        value = jnp.concatenate([value, value], axis=1)
        return jnp.concatenate([value] * (STATES // LANES), axis=1)

    own_lane = (
        lax.broadcasted_iota(jnp.int32, (8, STATES), 1) >> 6
    ) == lax.broadcasted_iota(jnp.int32, (8, STATES), 0)

    def flat(value):
        return jnp.sum(jnp.where(own_lane, widened(value), 0.0), axis=0, keepdims=True)

    power_re, power_im, squared = coef_real, coef_imag, 1
    for index, length in enumerate((1, 16, ROWS, ROWS * ny)):
        while squared < length:
            power_re, power_im = power_re * power_re - power_im * power_im, 2.0 * power_re * power_im
            squared *= 2
        lam[2 * index : 2 * index + 1, :] = flat(power_re)
        lam[2 * index + 1 : 2 * index + 2, :] = flat(power_im)
    ratio_real, ratio_imag = flat(ratio_real), flat(ratio_imag)
    own_state = (lax.broadcasted_iota(jnp.int32, (LANES, STATES), 0) >> 4) == (
        lax.broadcasted_iota(jnp.int32, (LANES, STATES), 1) >> 6
    )
    input_real, input_imag = (widened(mats[k].reshape(LANES, 64)) for k in range(2))
    bmat[:, :STATES] = jnp.where(own_state, ratio_real * input_real - ratio_imag * input_imag, 0.0).astype(BF16)
    bmat[:, STATES:] = jnp.where(own_state, ratio_real * input_imag + ratio_imag * input_real, 0.0).astype(BF16)
    rmat[:, :STATES] = jnp.where(own_state, widened(mats[2].reshape(LANES, 64)), 0.0).astype(BF16)
    rmat[:, STATES:] = jnp.where(own_state, -widened(mats[3].reshape(LANES, 64)), 0.0).astype(BF16)

    def ring_ref(ab, source, wall, piece):
        count = (ny, nz)[ab]
        cut = {0: pl.ds(0, count), 1: pl.ds(0, count // 2), 2: pl.ds(count // 2, count // 2)}[piece]
        if ab == 0:
            return wall.at[source, cut, rows_a]
        return wall.at[cut, source, rows_b]

    walls = (wall_c, wall_c, wall_o)

    def ring_hops(which, k):
        for ab in range(2):
            me, size = ((z, nz), (y, ny))[ab]
            last = size // 2 - 1
            for way in range(2):
                if k > last or (k == last and which == 1 - way):
                    continue
                piece = which + 1 if which < 2 else (1 + way if k == last else 0)
                yield ab, way, me, size, piece

    def ring_start(which, k):
        for ab, way, me, size, piece in ring_hops(which, k):
            sign = 1 - 2 * way
            ref = ring_ref(ab, wrap(me - sign * k, size), walls[which], piece)
            send(ref, ref, ring_s.at[which], ring_r.at[which, k], **{"zy"[ab]: wrap(me + sign, size)})

    def ring_blocks(which, k):
        return sum((ny, nz)[ab] // (2 if piece else 1) for ab, _, _, _, piece in ring_hops(which, k))

    def ring_wait(which, k):
        if ring_blocks(which, k):
            arrived(blocks_view(walls[which], ring_blocks(which, k)), ring_r.at[which, k])

    def state_hops(ab, stage):
        me, size = ((z, nz), (y, ny))[ab]
        reach = 1 if size < 4 else 2
        for way in range(2):
            for d in range(1, size // 2 + 1):
                if (d > reach) != (stage == 1):
                    continue
                piece = 1 + way if d == size // 2 else 0
                yield way, d, piece, me, size

    def state_start(ab, stage):
        for way, d, piece, me, size in state_hops(ab, stage):
            sign = 1 - 2 * way
            source = wrap(me - sign * 2, size) if stage else me
            ref = ring_ref(ab, source, wall_s, piece)
            target = wrap(me + sign * (d - 2 * stage), size)
            send(ref, ref, st_s.at[0], st_r.at[ab, stage], **{"zy"[ab]: target})

    def state_blocks(ab, stage):
        return sum((ny, nz)[ab] // (2 if piece else 1) for _, _, piece, _, _ in state_hops(ab, stage))

    def state_wait(ab, stage):
        if state_blocks(ab, stage):
            arrived(blocks_view(wall_s, state_blocks(ab, stage)), st_r.at[ab, stage])

    def service(which, k):
        ring_wait(which, k)
        ring_start(which, k + 1)

    def peer_pieces(turn):
        if turn == 0:
            return [(z, slice(None), rows_a), (slice(None), y, rows_b)]
        found = []
        for ab, way, me, size, piece in ring_hops(2, turn - 1):
            source = wrap(me - (1 - 2 * way) * turn, size)
            span = (ny, nz)[ab]
            cut = {0: pl.ds(0, span), 1: pl.ds(0, span // 2), 2: pl.ds(span // 2, span // 2)}[piece]
            found.append((source, cut, rows_a) if ab == 0 else (cut, source, rows_b))
        return found

    def peer_start(turn):
        for p in peer_pieces(turn):
            send(wall_o.at[p], wpeer.at[p], peer_s.at[0], peer_r.at[0], c=other)

    width = 2 * tok.shape[3]

    def norm(block):
        def some_rows(i, carry):
            rows = pl.ds(pl.multiple_of(i * 32, 32), 32)
            a, b = tok[block, 0, rows, :].astype(F32), tok[block, 1, rows, :].astype(F32)
            mean = (jnp.sum(a * a, axis=1, keepdims=True) + jnp.sum(b * b, axis=1, keepdims=True)) / width
            scale = lax.rsqrt(mean + EPS)
            target = pl.ds(pl.multiple_of(block * ROWS + i * 32, 32), 32)
            normed[target, : width // 2] = (a * scale * gain_rows[0]).astype(BF16)
            normed[target, width // 2 :] = (b * scale * gain_rows[1]).astype(BF16)
            return carry

        lax.fori_loop(0, ROWS // 32, some_rows, 0)

    phase("norm_own")
    arrived(gains.at[other], one_r.at[0])
    for k in range(2):
        wide = gains[k].astype(F32)
        gain_rows[k] = jnp.concatenate([wide[i : i + 1] for i in range(wide.shape[0])], axis=1)
    passed_over(x, 0)
    norm(x)
    phase("phase1_state")
    for ab in range(2):
        spread_in(0, wall_s, ab)
        state_start(ab, 0)
    phase("tok_forward")
    token_wait(xm, low, 0, 0)
    token_start(xm, low, 0, 2)
    token_wait(xp, high, 1, 0)
    token_start(xp, high, 1, 2)
    phase("phase1_rest")
    spread_in(1, wall_c, 0)
    spread_in(1, wall_c, 1)
    for which in range(2):
        ring_start(which, 0)
    phase("tok_wait1")
    token_wait(xm, high, 0, 1)
    pass_over(xm, 1)
    token_wait(xp, low, 1, 1)
    pass_over(xp, 2)

    phase("documents")
    arrived(docs.at[pl.ds(0, PARTS - 1)], doc_r.at[0])
    row = lax.broadcasted_iota(jnp.int32, (ALL, ROWS), 0)
    lane = lax.broadcasted_iota(jnp.int32, (ALL, ROWS), 1)
    pick_t = ones_where(lane == ((row >> 2) & 7) * 16 + (row >> 5))
    part_row = lax.broadcasted_iota(jnp.int32, (ROWS, ROWS), 0)
    spread_docs = jnp.zeros((ROWS, ROWS), F32)
    for q in range(PARTS):
        spread_docs = jnp.where(part_row == q, docs[q].astype(F32), spread_docs)
    by_part = nt(pick_t.astype(BF16), spread_docs.astype(BF16))
    by_part = by_part * ones_where(lane == (row & 3))
    docext[64:] = nn(by_part.astype(BF16), jnp.ones((ROWS, LANES), BF16))
    docext[4:32] = docext[64 + 448 : 64 + 476]
    docext[36:64] = docext[64 + 480 : 64 + 508]

    phase("phase1_out")
    spread_in(2, wall_o, 0)
    spread_in(2, wall_o, 1)
    ring_start(2, 0)
    peer_start(0)
    phase("state_stage")
    for ab in range(2):
        state_wait(ab, 0)
        state_start(ab, 1)
    phase("norm_mid")
    passed_over(xm, 1)
    norm(xm)
    phase("tok_wait2")
    token_wait(xo, low, 0, 2)
    token_wait(xo, high, 1, 2)
    pass_over(xo, 3)
    phase("norm_mid2")
    passed_over(xp, 2)
    norm(xp)
    phase("ring_ab0")
    service(0, 0)
    service(1, 0)
    phase("norm_last")
    passed_over(xo, 3)
    norm(xo)

    arrived(rimtok.at[x, c], rim_r.at[0])
    arrived(rimdoc.at[x], rim_r.at[1])
    for v in (xp, xm, xo):
        send(rimtok.at[x, c], rimtok.at[x, c], rim_s.at[2], rim_r.at[2], x=v)
        send(rimdoc.at[x], rimdoc.at[x], rim_s.at[3], rim_r.at[3], x=v)
    owe(rimtok.at[pl.ds(0, PARTS - 1), 0], rim_s.at[2])
    owe(rimdoc.at[pl.ds(0, PARTS - 1)], rim_s.at[3])

    phase("ring_o0")
    service(2, 0)
    peer_start(1)
    phase("state_w_wait")
    for ab in range(2):
        state_wait(ab, 1)
    phase("state_in")
    total_depth = nz * ny * depth
    state_in = wall_s[...].reshape(total_depth, LANES)
    in_order = halves(nn, perm, halves(nn, normed[:ALL], state_in).astype(BF16))
    driven[...] = in_order
    phase("ring_ab1")
    service(0, 1)
    service(1, 1)
    arrived(rimtok.at[pl.ds(0, PARTS - 1), 0], rim_r.at[2])
    arrived(rimdoc.at[pl.ds(0, PARTS - 1)], rim_r.at[3])
    send(rimtok.at[:, c], rimtok.at[:, c], rim_s.at[4], rim_r.at[4], c=other)
    owe(rimtok.at[:, c], rim_s.at[4])
    phase("push")
    pushed[...] = nn(in_order.astype(BF16), bmat[...])

    def lane_cut(k):
        return slice(k * LANES, (k + 1) * LANES), slice(STATES + k * LANES, STATES + (k + 1) * LANES)

    def rows_at(k):
        return slice(k * 32, (k + 1) * 32)

    def docs_at(k):
        return docext[64 + k * 32 : 96 + k * 32]

    phase("scan")
    for cut in range(STATES // LANES):
        re, im = lane_cut(cut)
        a_re, a_im = lam[0:1, re], lam[1:2, re]
        s_re, s_im = pushed[0:32, re], pushed[0:32, im]
        for k in range(1, 16):
            keep = ones_where(docs_at(k) == docs_at(k - 1))
            s_re, s_im = (
                pushed[rows_at(k), re] + keep * (a_re * s_re - a_im * s_im),
                pushed[rows_at(k), im] + keep * (a_re * s_im + a_im * s_re),
            )
            pushed[rows_at(k), re] = s_re
            pushed[rows_at(k), im] = s_im
    for seg in range(8):
        rows = slice(480 + seg * 4, 484 + seg * 4)
        ends[seg, 0:4, :STATES] = pushed[rows, :STATES]
        ends[seg, 4:8, :STATES] = pushed[rows, STATES:]
        last = docext[544 + seg * 4 : 548 + seg * 4]
        ends[seg, 0:4, STATES:] = last
        ends[seg, 4:8, STATES:] = last

    phase("fold_local")
    sign = jnp.where(lax.broadcasted_iota(jnp.int32, (8, STATES), 0) < 4, -1.0, 1.0)

    def joined(carry, piece, power):
        held, doc = carry
        piece, now = piece
        link = ones_where(now == doc)
        link = jnp.concatenate([link] * (STATES // LANES), axis=1)
        a_re, a_im = lam[2 * power : 2 * power + 1, :], lam[2 * power + 1 : 2 * power + 2, :]
        moved = a_re * held + (a_im * sign) * pltpu.roll(held, 4, 0)
        return piece + link * moved, now

    def of_ends(k):
        return ends[k, :, :STATES], ends[k, :, STATES:]

    wing = STATES // 2

    def pack(buffer, index, carry):
        held, doc = carry
        buffer[index, 0:8, :wing] = held[:, :wing].astype(BF16)
        buffer[index, 8:16, :wing] = held[:, wing:].astype(BF16)
        buffer[index, 0:8, wing:] = doc.astype(BF16)
        buffer[index, 8:16, wing:] = doc.astype(BF16)

    def of(buffer):
        def read(k):
            message = buffer[k].astype(F32)
            held = jnp.concatenate([message[0:8, :wing], message[8:16, :wing]], axis=1)
            return held, message[0:8, wing:]

        return read

    def fold(carry, pieces, count, limit, power):
        def step(k, carry):
            new = joined(carry, pieces(k), power)
            return tuple(jnp.where(k < limit, a, b) for a, b in zip(new, carry))

        return lax.fori_loop(0, count, step, carry)

    nothing = (jnp.zeros((8, STATES), F32), jnp.full((8, LANES), -1.0, F32))
    pack(chain1, y, fold(nothing, of_ends, 8, 8, 1))
    for d in range(1, ny):
        send(chain1.at[y], chain1.at[y], one_s.at[1], one_r.at[1], y=wrap(y + d, ny))
    phase("ring_o1")
    service(2, 1)
    peer_start(2)

    phase("rim_norm")
    arrived(rimtok.at[:, other], rim_r.at[4])
    for q in range(PARTS):
        a, b = rimtok[q, 0].astype(F32), rimtok[q, 1].astype(F32)
        mean = (jnp.sum(a * a, axis=1, keepdims=True) + jnp.sum(b * b, axis=1, keepdims=True)) / width
        scale = lax.rsqrt(mean + EPS)
        target = slice(ALL + 16 * q, ALL + 16 * q + 16)
        normed[target, : width // 2] = (a * scale * gain_rows[0]).astype(BF16)
        normed[target, width // 2 :] = (b * scale * gain_rows[1]).astype(BF16)
        at_two = lax.broadcasted_iota(jnp.int32, (1, ROWS), 1) == ROWS - 2
        two_back = jnp.sum(jnp.where(at_two, rimdoc[q].astype(F32), 0.0), axis=1, keepdims=True)
        docext[q : q + 1] = jnp.broadcast_to(jnp.where(here == 0, -1.0, two_back), (1, LANES))
    phase("ring_ab2")
    service(0, 2)
    service(1, 2)
    phase("chain1_wait")
    owe(chain1.at[pl.ds(0, ny - 1)], one_s.at[1])
    arrived(chain1.at[pl.ds(0, ny - 1)], one_r.at[1])
    pack(chain2, z, fold(nothing, of(chain1), ny, ny, 2))
    for d in range(1, nz):

        @pl.when(z + d < nz)
        def _(d=d):
            column_copy(d).start()
    phase("ring_o2")
    service(2, 2)
    peer_start(3)
    phase("ring_ab3")
    for k in range(3, most // 2):
        service(0, k)
        service(1, k)

    phase("conv_in")
    conv_in = wall_c[...].reshape(total_depth, 3 * LANES)
    straight = nn(normed[...], conv_in).astype(BF16)
    ahead = straight[ALL:].astype(F32)
    rimprod[...] = (ahead[:, LANES : 2 * LANES] * ahead[:, 2 * LANES :]).astype(BF16).astype(F32)
    projected = nn(perm[...], straight[:ALL])
    gate[...] = projected[:, :LANES]
    prodext[64:] = (projected[:, LANES : 2 * LANES] * projected[:, 2 * LANES :]).astype(BF16).astype(F32)
    for q in range(PARTS):
        prodext[q : q + 1] = rimprod[16 * q + 14 : 16 * q + 15]
        prodext[32 + q : 33 + q] = rimprod[16 * q + 15 : 16 * q + 16]
    prodext[4:32] = prodext[64 + 448 : 64 + 476]
    prodext[36:64] = prodext[64 + 480 : 64 + 508]
    phase("chain2_wait")
    incoming[:, :STATES], incoming[:, STATES:] = nothing
    for d in range(1, nz):

        @pl.when(z == d)
        def _(d=d):
            arrived(chain2.at[pl.ds(0, d)], one_r.at[5])

    phase("chain2_fold")

    @pl.when(z > 0)
    def _():
        def step(k, carry):
            return joined(carry, of(chain2)(k), 3)

        incoming[:, :STATES], incoming[:, STATES:] = lax.fori_loop(0, z, step, nothing)

    state = fold((incoming[:, :STATES], incoming[:, STATES:]), of(chain1), ny, y, 2)
    docext[32:36] = state[1][0:4]
    for seg in range(8):
        links[seg] = state[0]
        state = joined(state, of_ends(seg), 1)
    for seg in range(8):
        links[8 + seg // 2, (seg % 2) * 4 : (seg % 2) * 4 + 4] = links[seg, 0:4]
        links[12 + seg // 2, (seg % 2) * 4 : (seg % 2) * 4 + 4] = links[seg, 4:8]
    phase("fixup")
    previous = docext[32:64]
    for cut in range(STATES // LANES):
        re, im = lane_cut(cut)
        a_re, a_im = lam[0:1, re], lam[1:2, re]
        w_re = links[8:12, :, re].reshape(32, LANES)
        w_im = links[12:16, :, re].reshape(32, LANES)
        for k in range(16):
            w_re, w_im = a_re * w_re - a_im * w_im, a_re * w_im + a_im * w_re
            reach = ones_where(docs_at(k) == previous)
            pushed[rows_at(k), re] = pushed[rows_at(k), re] + reach * w_re
            pushed[rows_at(k), im] = pushed[rows_at(k), im] + reach * w_im
    phase("readout")
    reading = halves(nt, pushed[...].astype(BF16), rmat[...]) + skip[...] * driven[...]
    inner = 0.7978845608028654 * (reading + 0.044715 * (reading * reading * reading))
    ssm_out = (0.5 * reading * (1.0 + jnp.tanh(inner))).astype(BF16)
    acts[:, LANES:] = halves(nn, unperm, ssm_out).astype(BF16)
    mine, theirs = (pl.ds(pl.multiple_of(v * (ALL // 2), ALL // 2), ALL // 2) for v in (c, other))
    conv_lanes, ssm_lanes = pl.ds(0, LANES), pl.ds(LANES, LANES)
    send(acts.at[theirs, ssm_lanes], pacts.at[:, ssm_lanes], one_s.at[4], one_r.at[4], c=other)
    owe(pacts.at[:, ssm_lanes], one_s.at[4])

    phase("ring_o3")
    for k in range(3, most // 2):
        service(2, k)
        peer_start(k + 1)

    phase("conv")
    now = docext[64:]
    mixed = (
        taps[0:1].astype(F32) * prodext[0:ALL] * ones_where(docext[0:ALL] == now)
        + taps[1:2].astype(F32) * prodext[32 : 32 + ALL] * ones_where(docext[32 : 32 + ALL] == now)
        + taps[2:3].astype(F32) * prodext[64:]
    )
    conv_out = (gate[...] * mixed).astype(BF16)
    acts[:, :LANES] = halves(nn, unperm, conv_out).astype(BF16)
    send(acts.at[theirs, conv_lanes], pacts.at[:, conv_lanes], one_s.at[3], one_r.at[3], c=other)
    owe(pacts.at[:, conv_lanes], one_s.at[3])

    columns = total_depth // 4

    def quarter(ref, cut):
        if nz % 4 == 0:
            return ref[cut * nz // 4 : (cut + 1) * nz // 4].reshape(columns, 2 * LANES)
        return ref[cut // 2, cut % 2]

    phase("peer_w_wait")
    arrived(wpeer, peer_r.at[0])
    for cut in (0, 2, 1, 3):
        phase(f"out_proj{cut}")
        total = nt(acts[mine, :], quarter(wall_o, cut))
        if cut == 0:
            phase("pact_wait")
            arrived(pacts.at[:, ssm_lanes], one_r.at[4])
            arrived(pacts.at[:, conv_lanes], one_r.at[3])
        total = total + nt(pacts[...], quarter(wpeer, cut))
        part[cut] = total.astype(BF16).reshape(PARTS, ROWS // 2, columns)
        way, turn = cut // 2, cut % 2
        target = (xp, xm)[way]
        send(part.at[cut, xo], relay.at[way, turn], rs_s.at[0], rs_r.at[2 * way + turn], x=target)
    for turn in range(2):
        send(part.at[2 + turn, xp], final.at[0, 2 + turn], rs_s.at[0], rs_r.at[6 + turn], x=xp)
        send(part.at[turn, xm], final.at[1, turn], rs_s.at[0], rs_r.at[4 + turn], x=xm)
    for which in range(3):
        count = sum(ring_blocks(which, k) for k in range(most // 2))
        owe(blocks_view(walls[which], count), ring_s.at[which])
    owe(blocks_view(wall_s, sum(state_blocks(ab, stage) for ab in range(2) for stage in range(2))), st_s.at[0])
    owe(wpeer, peer_s.at[0])
    settle()
    for turn in range(2):
        for way, target in ((0, xp), (1, xm)):
            phase(f"relay{way}{turn}")
            cut = 2 * way + turn
            arrived(relay.at[way, turn], rs_r.at[2 * way + turn])
            both = part[cut, target].astype(F32) + relay[way, turn].astype(F32)
            part[cut, target] = both.astype(BF16)
            send(part.at[cut, target], final.at[way, cut], rs_s.at[0], rs_r.at[4 + cut], x=target)
    for cut in (0, 2, 1, 3):
        phase(f"final{cut}")
        arrived(final.at[:, cut], rs_r.at[4 + cut])
        value = part[cut, x].astype(F32) + final[0, cut].astype(F32) + final[1, cut].astype(F32)
        out[:, cut * columns : (cut + 1) * columns] = value.astype(BF16)
    phase("drain")
    arrived(part.at[pl.ds(0, 3)], rs_s.at[0])

    for d in range(1, nz):

        @pl.when(z + d == nz - 1)
        def _(d=d):
            arrived(chain2.at[pl.ds(0, d)], one_s.at[5])

    phase(None)


def shards(
    nz, ny, tokens, documents, norm_gain, out_gate_weight, in_gate_weight, value_weight,
    conv_taps, state_in_weight, decay_rate, frequency, step_log, input_real, input_imag,
    readout_real, readout_imag, skip_gain, conv_out_weight, state_out_weight,
):
    depth = state_in_weight.shape[0]
    width = tokens.shape[1]
    columns = nz * ny * depth // 4
    vmem = pl.BlockSpec(memory_space=pltpu.VMEM)
    hbm = pl.BlockSpec(memory_space=pltpu.HBM)
    dma = pltpu.SemaphoreType.DMA
    steps = max(nz, ny) // 2
    return pl.pallas_call(
        functools.partial(mixer_kernel, nz, ny, depth),
        out_shape=jax.ShapeDtypeStruct((ROWS // 2, 4 * columns), BF16),
        in_specs=[hbm] * 18,
        out_specs=vmem,
        scratch_shapes=[
            pltpu.VMEM((2, 8, 64), F32),
            pltpu.VMEM((1, 32), F32),
            pltpu.VMEM((4, 8, 16, 64), F32),
            pltpu.VMEM((3, LANES), BF16),
            pltpu.VMEM((1, LANES), F32),
            pltpu.VMEM((8, STATES), F32),
            pltpu.VMEM((PARTS, 2, ROWS, width), BF16),
            pltpu.VMEM((2, width // LANES, LANES), BF16),
            pltpu.VMEM((2, 1, width), F32),
            pltpu.VMEM((PARTS, 1, ROWS), jnp.int32),
            pltpu.VMEM((nz, ny, depth, LANES), BF16),
            pltpu.VMEM((nz, ny, depth, 3 * LANES), BF16),
            pltpu.VMEM((nz, ny, depth, 2 * LANES), BF16),
            pltpu.VMEM((nz, ny, depth, 2 * LANES), BF16),
            pltpu.VMEM((ALL + 16 * PARTS, 2 * width), BF16),
            pltpu.VMEM((ALL, ALL), BF16),
            pltpu.VMEM((ALL, ALL), BF16),
            pltpu.VMEM((LANES, 2 * STATES), BF16),
            pltpu.VMEM((LANES, 2 * STATES), BF16),
            pltpu.VMEM((ALL, LANES), F32),
            pltpu.VMEM((ALL, 2 * STATES), F32),
            pltpu.VMEM((64 + ALL, LANES), F32),
            pltpu.VMEM((64 + ALL, LANES), F32),
            pltpu.VMEM((ALL, LANES), F32),
            pltpu.VMEM((8, 8, STATES + LANES), F32),
            pltpu.VMEM((ny, 16, STATES // 2 + LANES), BF16),
            pltpu.VMEM((nz, 16, STATES // 2 + LANES), BF16),
            pltpu.VMEM((8, STATES + LANES), F32),
            pltpu.VMEM((16, 8, STATES), F32),
            pltpu.VMEM((PARTS, 2, 16, width), BF16),
            pltpu.VMEM((PARTS, 1, ROWS), jnp.int32),
            pltpu.VMEM((16 * PARTS, LANES), F32),
            pltpu.VMEM((ALL, 2 * LANES), BF16),
            pltpu.VMEM((ALL // 2, 2 * LANES), BF16),
            pltpu.VMEM((4, PARTS, ROWS // 2, columns), BF16),
            pltpu.VMEM((2, 2, ROWS // 2, columns), BF16),
            pltpu.VMEM((2, 4, ROWS // 2, columns), BF16),
            dma((11,)),
            dma((1,)), dma((2, 3)),
            dma((1,)), dma((PARTS,)),
            dma((1,)), dma((1,)),
            dma((6,)), dma((6,)),
            dma((3,)), dma((3, 2)),
            dma((1,)), dma((2, 2)),
            dma((3,)), dma((3, steps)),
            dma((1,)), dma((1,)),
            dma((1,)), dma((8,)),
            dma((5,)), dma((5,)),
        ],
        compiler_params=pltpu.CompilerParams(
            collective_id=0, has_side_effects=True, vmem_limit_bytes=40 * 1024 * 1024
        ),
        name="mixer",
    )(*(
        pltpu.with_memory_space_constraint(operand, pltpu.HBM) for operand in (
            tokens, state_in_weight, out_gate_weight, in_gate_weight, value_weight, conv_out_weight.T,
            state_out_weight.T, documents[None, :], norm_gain.reshape(-1, LANES), decay_rate, frequency,
            step_log[None, :], input_real.transpose(0, 2, 1), input_imag.transpose(0, 2, 1),
            readout_real, readout_imag, conv_taps, skip_gain[None, :],
        )
    ))


def solution(mesh, nz=8, ny=8):
    torus = Mesh(
        mesh.devices.reshape(nz, ny, mesh.shape["fs"], mesh.shape["tp"]), ("sp_0", "sp_1", "fs", "tp")
    )
    in_specs = (
        P(FS_SP, "tp"),
        P(FS_SP),
        P("tp"),
        P(SP, "tp"),
        P(SP, "tp"),
        P(SP, "tp"),
        P(None, "tp"),
        P(SP, "tp"),
        P("tp", None),
        P("tp", None),
        P("tp"),
        P("tp", None, None),
        P("tp", None, None),
        P("tp", None, None),
        P("tp", None, None),
        P("tp"),
        P("tp", SP),
        P("tp", SP),
    )
    return jax.shard_map(
        functools.partial(shards, nz, ny), mesh=torus, in_specs=in_specs,
        out_specs=P(FS_SP_TP, None), check_vma=False,
    )
```

```python
import functools

import jax
import jax.numpy as jnp
from jax import lax
from jax.experimental import pallas as pl
from jax.experimental.pallas import tpu as pltpu
from jax.sharding import Mesh
from jax.sharding import PartitionSpec as P

SP = ("sp_0", "sp_1")
FS_SP = ("fs", "sp_0", "sp_1")
FS_SP_TP = ("fs", "sp_0", "sp_1", "tp")
EPS = 1e-06
PARTS = 4
ROWS = 128
LANES = 128
STATES = 512
ALL = PARTS * ROWS
BF16 = jnp.bfloat16
F32 = jnp.float32


def nn(a, b):
    return jnp.dot(a, b, preferred_element_type=F32)


def halves(product, a, b):
    middle = a.shape[0] // 2
    return jnp.concatenate([product(a[:middle], b), product(a[middle:], b)])


def nt(a, b):
    return lax.dot_general(a, b, (((1,), (1,)), ((), ())), preferred_element_type=F32)


def ones_where(mask):
    return jnp.where(mask, 1.0, 0.0)


def mixer_kernel(
    nz, ny, depth, tok_in, w_in_0, w_in_1, w_in_2, w_in_3, w_in_4, w_in_5, doc_in, gain_in,
    decay_in, freq_in, step_in, in_re, in_im, read_re, read_im, taps_in, skip_in, out,
    rates, step_row, mats, taps, skip, lam, tok, gains, gain_rows, docs, wall_s, wall_c, wall_o, wpeer, normed, perm, unperm, bmat, rmat, driven, pushed,
    docext, prodext, gate, ends, chain1, chain2, incoming, links, rimtok, rimdoc, rimprod, acts, pacts,
    part, relay, final, local_sem, tok_s, tok_r, d2d_s, d2d_r, doc_s, doc_r, one_s, one_r,
    ph_s, ph_r, st_s, st_r, ring_s, ring_r, peer_s, peer_r, rs_s, rs_r, rim_s, rim_r,
):
    z, y = lax.axis_index("sp_0"), lax.axis_index("sp_1")
    x, c = lax.axis_index("fs"), lax.axis_index("tp")
    half = depth // 2
    most = max(nz, ny)
    other = 1 - c
    owed, scopes = [], []

    def phase(name):
        if scopes:
            scopes.pop().__exit__(None, None, None)
        if name:
            scopes.append(jax.named_scope(name))
            scopes[-1].__enter__()

    def wrap(v, n):
        return lax.rem(v + 4 * n, n)

    def send(src, dst, ssem, rsem, **where):
        names = {"z": "sp_0", "y": "sp_1", "x": "fs", "c": "tp"}
        copy = pltpu.make_async_remote_copy(
            src_ref=src, dst_ref=dst, send_sem=ssem, recv_sem=rsem,
            device_id={names[k]: v for k, v in where.items()},
            device_id_type=pl.DeviceIdType.MESH,
        )
        copy.start()

    def arrived(dst, rsem):
        pltpu.make_async_copy(dst, dst, rsem).wait()

    def owe(view, ssem):
        owed.append((view, ssem))

    def settle():
        for view, ssem in owed:
            arrived(view, ssem)
        owed.clear()

    xp, xm, xo = wrap(x + 1, PARTS), wrap(x - 1, PARTS), wrap(x + 2, PARTS)
    here = z * ny + y
    after, before = wrap(here + 1, nz * ny), wrap(here - 1, nz * ny)
    after_z, after_y = lax.div(after, ny), lax.rem(after, ny)
    before_z, before_y = lax.div(before, ny), lax.rem(before, ny)

    phase("greet")
    barrier = pltpu.get_barrier_semaphore()
    count = 0

    def greet(**where):
        names = {"z": "sp_0", "y": "sp_1", "x": "fs", "c": "tp"}
        pl.semaphore_signal(
            barrier, inc=1, device_id={names[k]: v for k, v in where.items()},
            device_id_type=pl.DeviceIdType.MESH,
        )
        return 1

    for d in range(1, ny):
        count += greet(y=wrap(y + d, ny))
    for d in range(1, nz):
        count += greet(z=wrap(z + d, nz))
    for v in (xp, xm, xo):
        count += greet(x=v)
    count += greet(c=other)
    count += greet(z=after_z, y=after_y)
    count += greet(z=before_z, y=before_y)

    own_channels = pl.ds(pl.multiple_of(x * LANES, LANES), LANES)
    own_groups = pl.ds(pl.multiple_of(x * 8, 8), 8)
    moves = [(tok_in, tok.at[x, c], 0), (doc_in, docs.at[x], 1), (gain_in, gains.at[c], 2)]
    places = [(wall_s, 0, 3)] + [(wall_c, k, 9) for k in range(3)] + [(wall_o, k, 10) for k in range(2)]
    for w, (wall, k, index) in zip((w_in_0, w_in_1, w_in_2, w_in_3, w_in_4, w_in_5), places):
        moves.append((w.at[:, own_channels], wall.at[z, y, :, pl.ds(k * LANES, LANES)], index))
    moves += [(decay_in.at[own_groups], rates.at[0], 4), (freq_in.at[own_groups], rates.at[1], 4)]
    for k, m in enumerate((in_re, in_im, read_re, read_im)):
        moves.append((m.at[own_groups], mats.at[k], 5))
    moves += [(step_in, step_row, 6), (taps_in.at[:, own_channels], taps, 7)]
    moves.append((skip_in.at[:, own_channels], skip, 8))
    for source, target, k in moves:
        pltpu.make_async_copy(source, target, local_sem.at[k]).start()
    phase("enter")
    for k, ref in enumerate((tok.at[x, c], docs.at[x], gains.at[c], wall_s.at[z, y])):
        arrived(ref, local_sem.at[k])
    for k, ref in enumerate((wall_c.at[z, y], wall_o.at[z, y])):
        arrived(ref, local_sem.at[9 + k])
    phase("barrier")
    pl.semaphore_wait(barrier, count)

    low, high = pl.ds(0, ROWS // 2), pl.ds(ROWS // 2, ROWS // 2)

    def column_copy(d):
        return pltpu.make_async_remote_copy(
            src_ref=chain2.at[z], dst_ref=chain2.at[z], send_sem=one_s.at[5], recv_sem=one_r.at[5],
            device_id={"sp_0": wrap(z + d, nz)}, device_id_type=pl.DeviceIdType.MESH,
        )

    def token_send(block, rows, way):
        ref = tok.at[block, c, rows]
        return ref, (xp if way == 0 else xm)

    def token_start(block, rows, way, turn):
        ref, target = token_send(block, rows, way)
        send(ref, ref, tok_s.at[0], tok_r.at[way, turn], x=target)

    def token_wait(block, rows, way, turn):
        arrived(tok.at[block, c, rows], tok_r.at[way, turn])

    def pass_over(block, turn):
        ref = tok.at[block, c]
        send(ref, ref, d2d_s.at[0], d2d_r.at[turn], c=other)

    def passed_over(block, turn):
        arrived(tok.at[block, other], d2d_r.at[turn])

    phase("first_sends")
    rows_a, rows_b = pl.ds(0, half), pl.ds(half, half)

    def blocks_view(wall, count):
        if count > nz * ny:
            return wall.at[pl.ds(0, count // (2 * ny))]
        if count % ny:
            return wall.at[0, pl.ds(0, count // 2)]
        return wall.at[pl.ds(0, count // ny), :, rows_a]

    def spread_view(wall, ab):
        if ab == 0:
            return wall.at[0, pl.ds(0, ny - 1), rows_a]
        return wall.at[pl.ds(0, nz - 1), 0, rows_b]

    def spread_out(turn, wall):
        for d in range(1, ny):
            ref = wall.at[z, y, rows_a]
            send(ref, ref, ph_s.at[turn], ph_r.at[turn, 0], y=wrap(y + d, ny))
        for d in range(1, nz):
            ref = wall.at[z, y, rows_b]
            send(ref, ref, ph_s.at[turn], ph_r.at[turn, 1], z=wrap(z + d, nz))
        owe(blocks_view(wall, ny - 1 + nz - 1), ph_s.at[turn])

    def spread_in(turn, wall, ab):
        arrived(spread_view(wall, ab), ph_r.at[turn, ab])

    for v in (xp, xm, xo):
        send(docs.at[x], docs.at[x], doc_s.at[0], doc_r.at[0], x=v)
    owe(docs.at[pl.ds(0, PARTS - 1)], doc_s.at[0])
    send(gains.at[c], gains.at[c], one_s.at[0], one_r.at[0], c=other)
    owe(gains.at[c], one_s.at[0])
    owe(tok.at[pl.ds(0, PARTS - 1), 0], tok_s.at[0])
    owe(tok.at[:, 0], d2d_s.at[0])
    spread_out(0, wall_s)
    token_start(x, low, 0, 0)
    token_start(x, high, 1, 0)
    pass_over(x, 0)
    spread_out(1, wall_c)
    token_start(x, high, 0, 1)
    token_start(x, low, 1, 1)
    spread_out(2, wall_o)
    last_rows = tok.at[x, c, pl.ds(ROWS - 16, 16)]
    send(last_rows, rimtok.at[x, c], rim_s.at[0], rim_r.at[0], z=after_z, y=after_y)
    send(docs.at[x], rimdoc.at[x], rim_s.at[1], rim_r.at[1], z=after_z, y=after_y)
    owe(last_rows, rim_s.at[0])
    owe(docs.at[x], rim_s.at[1])

    phase("tables")
    shape = (ALL, ALL)
    r, n = lax.broadcasted_iota(jnp.int32, shape, 0), lax.broadcasted_iota(jnp.int32, shape, 1)
    natural = (r & 3) * ROWS + ((r >> 2) & 7) * 16 + (r >> 5)
    perm[...] = ones_where(n == natural).astype(BF16)
    t = (r >> 8) * (ROWS // 2) + (r & 63)
    turned = (t & 15) * 32 + (t >> 4) * 4 + ((r >> 6) & 3)
    unperm[...] = ones_where(n == turned).astype(BF16)
    for k, ref in enumerate((rates, mats, step_row, taps, skip)):
        arrived(ref, local_sem.at[4 + k])
    group = lax.broadcasted_iota(jnp.int32, (8, 32), 0) + x * 8
    step_log = jnp.broadcast_to(step_row[...], (8, 32))
    mine_only = lax.broadcasted_iota(jnp.int32, (8, 32), 1) == group
    step = jnp.exp(jnp.sum(jnp.where(mine_only, step_log, 0.0), axis=1, keepdims=True))
    decay, frequency = rates[0], rates[1]
    damping, turning = decay * step, frequency * step
    fading = jnp.exp(-damping)
    coef_real, coef_imag = fading * jnp.cos(turning), fading * jnp.sin(turning)
    half_sine = jnp.sin(turning * 0.5)
    series = jnp.ones_like(damping)
    for k in range(11, 1, -1):
        series = 1.0 - damping * (1.0 / k) * series
    less_real = -damping * series * jnp.cos(turning) - 2.0 * half_sine * half_sine
    denominator = decay * decay + frequency * frequency
    ratio_real = (-less_real * decay + coef_imag * frequency) / denominator
    ratio_imag = (-coef_imag * decay - less_real * frequency) / denominator

    def widened(value):
        value = jnp.concatenate([value, value], axis=1)
        return jnp.concatenate([value] * (STATES // LANES), axis=1)

    own_lane = (
        lax.broadcasted_iota(jnp.int32, (8, STATES), 1) >> 6
    ) == lax.broadcasted_iota(jnp.int32, (8, STATES), 0)

    def flat(value):
        return jnp.sum(jnp.where(own_lane, widened(value), 0.0), axis=0, keepdims=True)

    power_re, power_im, squared = coef_real, coef_imag, 1
    for index, length in enumerate((1, 16, ROWS, ROWS * ny)):
        while squared < length:
            power_re, power_im = power_re * power_re - power_im * power_im, 2.0 * power_re * power_im
            squared *= 2
        lam[2 * index : 2 * index + 1, :] = flat(power_re)
        lam[2 * index + 1 : 2 * index + 2, :] = flat(power_im)
    ratio_real, ratio_imag = flat(ratio_real), flat(ratio_imag)
    own_state = (lax.broadcasted_iota(jnp.int32, (LANES, STATES), 0) >> 4) == (
        lax.broadcasted_iota(jnp.int32, (LANES, STATES), 1) >> 6
    )
    input_real, input_imag = (widened(mats[k].reshape(LANES, 64)) for k in range(2))
    bmat[:, :STATES] = jnp.where(own_state, ratio_real * input_real - ratio_imag * input_imag, 0.0).astype(BF16)
    bmat[:, STATES:] = jnp.where(own_state, ratio_real * input_imag + ratio_imag * input_real, 0.0).astype(BF16)
    rmat[:, :STATES] = jnp.where(own_state, widened(mats[2].reshape(LANES, 64)), 0.0).astype(BF16)
    rmat[:, STATES:] = jnp.where(own_state, -widened(mats[3].reshape(LANES, 64)), 0.0).astype(BF16)

    def ring_ref(ab, source, wall, piece):
        count = (ny, nz)[ab]
        cut = {0: pl.ds(0, count), 1: pl.ds(0, count // 2), 2: pl.ds(count // 2, count // 2)}[piece]
        if ab == 0:
            return wall.at[source, cut, rows_a]
        return wall.at[cut, source, rows_b]

    walls = (wall_c, wall_c, wall_o)

    def ring_hops(which, k):
        for ab in range(2):
            me, size = ((z, nz), (y, ny))[ab]
            last = size // 2 - 1
            for way in range(2):
                if k > last or (k == last and which == 1 - way):
                    continue
                piece = which + 1 if which < 2 else (1 + way if k == last else 0)
                yield ab, way, me, size, piece

    def ring_start(which, k):
        for ab, way, me, size, piece in ring_hops(which, k):
            sign = 1 - 2 * way
            ref = ring_ref(ab, wrap(me - sign * k, size), walls[which], piece)
            send(ref, ref, ring_s.at[which], ring_r.at[which, k], **{"zy"[ab]: wrap(me + sign, size)})

    def ring_blocks(which, k):
        return sum((ny, nz)[ab] // (2 if piece else 1) for ab, _, _, _, piece in ring_hops(which, k))

    def ring_wait(which, k):
        if ring_blocks(which, k):
            arrived(blocks_view(walls[which], ring_blocks(which, k)), ring_r.at[which, k])

    def state_hops(ab, stage):
        me, size = ((z, nz), (y, ny))[ab]
        reach = 1 if size < 4 else 2
        for way in range(2):
            for d in range(1, size // 2 + 1):
                if (d > reach) != (stage == 1):
                    continue
                piece = 1 + way if d == size // 2 else 0
                yield way, d, piece, me, size

    def state_start(ab, stage):
        for way, d, piece, me, size in state_hops(ab, stage):
            sign = 1 - 2 * way
            source = wrap(me - sign * 2, size) if stage else me
            ref = ring_ref(ab, source, wall_s, piece)
            target = wrap(me + sign * (d - 2 * stage), size)
            send(ref, ref, st_s.at[0], st_r.at[ab, stage], **{"zy"[ab]: target})

    def state_blocks(ab, stage):
        return sum((ny, nz)[ab] // (2 if piece else 1) for _, _, piece, _, _ in state_hops(ab, stage))

    def state_wait(ab, stage):
        if state_blocks(ab, stage):
            arrived(blocks_view(wall_s, state_blocks(ab, stage)), st_r.at[ab, stage])

    def service(which, k):
        ring_wait(which, k)
        ring_start(which, k + 1)

    def peer_pieces(turn):
        if turn == 0:
            return [(z, slice(None), rows_a), (slice(None), y, rows_b)]
        found = []
        for ab, way, me, size, piece in ring_hops(2, turn - 1):
            source = wrap(me - (1 - 2 * way) * turn, size)
            span = (ny, nz)[ab]
            cut = {0: pl.ds(0, span), 1: pl.ds(0, span // 2), 2: pl.ds(span // 2, span // 2)}[piece]
            found.append((source, cut, rows_a) if ab == 0 else (cut, source, rows_b))
        return found

    def peer_start(turn):
        for p in peer_pieces(turn):
            send(wall_o.at[p], wpeer.at[p], peer_s.at[0], peer_r.at[0], c=other)

    width = 2 * tok.shape[3]

    def norm(block):
        def some_rows(i, carry):
            rows = pl.ds(pl.multiple_of(i * 32, 32), 32)
            a, b = tok[block, 0, rows, :].astype(F32), tok[block, 1, rows, :].astype(F32)
            mean = (jnp.sum(a * a, axis=1, keepdims=True) + jnp.sum(b * b, axis=1, keepdims=True)) / width
            scale = lax.rsqrt(mean + EPS)
            target = pl.ds(pl.multiple_of(block * ROWS + i * 32, 32), 32)
            normed[target, : width // 2] = (a * scale * gain_rows[0]).astype(BF16)
            normed[target, width // 2 :] = (b * scale * gain_rows[1]).astype(BF16)
            return carry

        lax.fori_loop(0, ROWS // 32, some_rows, 0)

    phase("norm_own")
    arrived(gains.at[other], one_r.at[0])
    for k in range(2):
        wide = gains[k].astype(F32)
        gain_rows[k] = jnp.concatenate([wide[i : i + 1] for i in range(wide.shape[0])], axis=1)
    passed_over(x, 0)
    norm(x)
    phase("phase1_state")
    for ab in range(2):
        spread_in(0, wall_s, ab)
        state_start(ab, 0)
    phase("tok_forward")
    token_wait(xm, low, 0, 0)
    token_start(xm, low, 0, 2)
    token_wait(xp, high, 1, 0)
    token_start(xp, high, 1, 2)
    phase("phase1_rest")
    spread_in(1, wall_c, 0)
    spread_in(1, wall_c, 1)
    for which in range(2):
        ring_start(which, 0)
    phase("tok_wait1")
    token_wait(xm, high, 0, 1)
    pass_over(xm, 1)
    token_wait(xp, low, 1, 1)
    pass_over(xp, 2)

    phase("documents")
    arrived(docs.at[pl.ds(0, PARTS - 1)], doc_r.at[0])
    row = lax.broadcasted_iota(jnp.int32, (ALL, ROWS), 0)
    lane = lax.broadcasted_iota(jnp.int32, (ALL, ROWS), 1)
    pick_t = ones_where(lane == ((row >> 2) & 7) * 16 + (row >> 5))
    part_row = lax.broadcasted_iota(jnp.int32, (ROWS, ROWS), 0)
    spread_docs = jnp.zeros((ROWS, ROWS), F32)
    for q in range(PARTS):
        spread_docs = jnp.where(part_row == q, docs[q].astype(F32), spread_docs)
    by_part = nt(pick_t.astype(BF16), spread_docs.astype(BF16))
    by_part = by_part * ones_where(lane == (row & 3))
    docext[64:] = nn(by_part.astype(BF16), jnp.ones((ROWS, LANES), BF16))
    docext[4:32] = docext[64 + 448 : 64 + 476]
    docext[36:64] = docext[64 + 480 : 64 + 508]

    phase("phase1_out")
    spread_in(2, wall_o, 0)
    spread_in(2, wall_o, 1)
    ring_start(2, 0)
    peer_start(0)
    phase("state_stage")
    for ab in range(2):
        state_wait(ab, 0)
        state_start(ab, 1)
    phase("norm_mid")
    passed_over(xm, 1)
    norm(xm)
    phase("tok_wait2")
    token_wait(xo, low, 0, 2)
    token_wait(xo, high, 1, 2)
    pass_over(xo, 3)
    phase("norm_mid2")
    passed_over(xp, 2)
    norm(xp)
    phase("ring_ab0")
    service(0, 0)
    service(1, 0)
    phase("norm_last")
    passed_over(xo, 3)
    norm(xo)

    arrived(rimtok.at[x, c], rim_r.at[0])
    arrived(rimdoc.at[x], rim_r.at[1])
    for v in (xp, xm, xo):
        send(rimtok.at[x, c], rimtok.at[x, c], rim_s.at[2], rim_r.at[2], x=v)
        send(rimdoc.at[x], rimdoc.at[x], rim_s.at[3], rim_r.at[3], x=v)
    owe(rimtok.at[pl.ds(0, PARTS - 1), 0], rim_s.at[2])
    owe(rimdoc.at[pl.ds(0, PARTS - 1)], rim_s.at[3])

    phase("ring_o0")
    service(2, 0)
    peer_start(1)
    phase("state_w_wait")
    for ab in range(2):
        state_wait(ab, 1)
    phase("state_in")
    total_depth = nz * ny * depth
    state_in = wall_s[...].reshape(total_depth, LANES)
    in_order = halves(nn, perm, halves(nn, normed[:ALL], state_in).astype(BF16))
    driven[...] = in_order
    phase("ring_ab1")
    service(0, 1)
    service(1, 1)
    arrived(rimtok.at[pl.ds(0, PARTS - 1), 0], rim_r.at[2])
    arrived(rimdoc.at[pl.ds(0, PARTS - 1)], rim_r.at[3])
    send(rimtok.at[:, c], rimtok.at[:, c], rim_s.at[4], rim_r.at[4], c=other)
    owe(rimtok.at[:, c], rim_s.at[4])
    phase("push")
    pushed[...] = nn(in_order.astype(BF16), bmat[...])

    def lane_cut(k):
        return slice(k * LANES, (k + 1) * LANES), slice(STATES + k * LANES, STATES + (k + 1) * LANES)

    def rows_at(k):
        return slice(k * 32, (k + 1) * 32)

    def docs_at(k):
        return docext[64 + k * 32 : 96 + k * 32]

    phase("scan")
    for cut in range(STATES // LANES):
        re, im = lane_cut(cut)
        a_re, a_im = lam[0:1, re], lam[1:2, re]
        s_re, s_im = pushed[0:32, re], pushed[0:32, im]
        for k in range(1, 16):
            keep = ones_where(docs_at(k) == docs_at(k - 1))
            s_re, s_im = (
                pushed[rows_at(k), re] + keep * (a_re * s_re - a_im * s_im),
                pushed[rows_at(k), im] + keep * (a_re * s_im + a_im * s_re),
            )
            pushed[rows_at(k), re] = s_re
            pushed[rows_at(k), im] = s_im
    for seg in range(8):
        rows = slice(480 + seg * 4, 484 + seg * 4)
        ends[seg, 0:4, :STATES] = pushed[rows, :STATES]
        ends[seg, 4:8, :STATES] = pushed[rows, STATES:]
        last = docext[544 + seg * 4 : 548 + seg * 4]
        ends[seg, 0:4, STATES:] = last
        ends[seg, 4:8, STATES:] = last

    phase("fold_local")
    sign = jnp.where(lax.broadcasted_iota(jnp.int32, (8, STATES), 0) < 4, -1.0, 1.0)

    def joined(carry, piece, power):
        held, doc = carry
        piece, now = piece
        link = ones_where(now == doc)
        link = jnp.concatenate([link] * (STATES // LANES), axis=1)
        a_re, a_im = lam[2 * power : 2 * power + 1, :], lam[2 * power + 1 : 2 * power + 2, :]
        moved = a_re * held + (a_im * sign) * pltpu.roll(held, 4, 0)
        return piece + link * moved, now

    def of_ends(k):
        return ends[k, :, :STATES], ends[k, :, STATES:]

    wing = STATES // 2

    def pack(buffer, index, carry):
        held, doc = carry
        buffer[index, 0:8, :wing] = held[:, :wing].astype(BF16)
        buffer[index, 8:16, :wing] = held[:, wing:].astype(BF16)
        buffer[index, 0:8, wing:] = doc.astype(BF16)
        buffer[index, 8:16, wing:] = doc.astype(BF16)

    def of(buffer):
        def read(k):
            message = buffer[k].astype(F32)
            held = jnp.concatenate([message[0:8, :wing], message[8:16, :wing]], axis=1)
            return held, message[0:8, wing:]

        return read

    def fold(carry, pieces, count, limit, power):
        def step(k, carry):
            new = joined(carry, pieces(k), power)
            return tuple(jnp.where(k < limit, a, b) for a, b in zip(new, carry))

        return lax.fori_loop(0, count, step, carry)

    nothing = (jnp.zeros((8, STATES), F32), jnp.full((8, LANES), -1.0, F32))
    pack(chain1, y, fold(nothing, of_ends, 8, 8, 1))
    for d in range(1, ny):
        send(chain1.at[y], chain1.at[y], one_s.at[1], one_r.at[1], y=wrap(y + d, ny))
    phase("ring_o1")
    service(2, 1)
    peer_start(2)

    phase("rim_norm")
    arrived(rimtok.at[:, other], rim_r.at[4])
    for q in range(PARTS):
        a, b = rimtok[q, 0].astype(F32), rimtok[q, 1].astype(F32)
        mean = (jnp.sum(a * a, axis=1, keepdims=True) + jnp.sum(b * b, axis=1, keepdims=True)) / width
        scale = lax.rsqrt(mean + EPS)
        target = slice(ALL + 16 * q, ALL + 16 * q + 16)
        normed[target, : width // 2] = (a * scale * gain_rows[0]).astype(BF16)
        normed[target, width // 2 :] = (b * scale * gain_rows[1]).astype(BF16)
        for back in (2, 1):
            there = lax.broadcasted_iota(jnp.int32, (1, ROWS), 1) == ROWS - back
            number = jnp.sum(jnp.where(there, rimdoc[q].astype(F32), 0.0), axis=1, keepdims=True)
            target = 32 * (2 - back) + q
            docext[target : target + 1] = jnp.broadcast_to(jnp.where(here == 0, -1.0, number), (1, LANES))
    phase("ring_ab2")
    service(0, 2)
    service(1, 2)
    phase("chain1_wait")
    owe(chain1.at[pl.ds(0, ny - 1)], one_s.at[1])
    arrived(chain1.at[pl.ds(0, ny - 1)], one_r.at[1])
    pack(chain2, z, fold(nothing, of(chain1), ny, ny, 2))
    for d in range(1, nz):

        @pl.when(z + d < nz)
        def _(d=d):
            column_copy(d).start()
    phase("ring_o2")
    service(2, 2)
    peer_start(3)
    phase("ring_ab3")
    for k in range(3, most // 2):
        service(0, k)
        service(1, k)

    phase("conv_in")
    conv_in = wall_c[...].reshape(total_depth, 3 * LANES)
    straight = nn(normed[...], conv_in).astype(BF16)
    ahead = straight[ALL:].astype(F32)
    rimprod[...] = (ahead[:, LANES : 2 * LANES] * ahead[:, 2 * LANES :]).astype(BF16).astype(F32)
    projected = nn(perm[...], straight[:ALL])
    gate[...] = projected[:, :LANES]
    prodext[64:] = (projected[:, LANES : 2 * LANES] * projected[:, 2 * LANES :]).astype(BF16).astype(F32)
    for q in range(PARTS):
        prodext[q : q + 1] = rimprod[16 * q + 14 : 16 * q + 15]
        prodext[32 + q : 33 + q] = rimprod[16 * q + 15 : 16 * q + 16]
    prodext[4:32] = prodext[64 + 448 : 64 + 476]
    prodext[36:64] = prodext[64 + 480 : 64 + 508]
    mine, theirs = (pl.ds(pl.multiple_of(v * (ALL // 2), ALL // 2), ALL // 2) for v in (c, other))
    conv_lanes, ssm_lanes = pl.ds(0, LANES), pl.ds(LANES, LANES)

    phase("conv")
    now = docext[64:]
    mixed = (
        taps[0:1].astype(F32) * prodext[0:ALL] * ones_where(docext[0:ALL] == now)
        + taps[1:2].astype(F32) * prodext[32 : 32 + ALL] * ones_where(docext[32 : 32 + ALL] == now)
        + taps[2:3].astype(F32) * prodext[64:]
    )
    conv_out = (gate[...] * mixed).astype(BF16)
    acts[:, :LANES] = halves(nn, unperm, conv_out).astype(BF16)
    send(acts.at[theirs, conv_lanes], pacts.at[:, conv_lanes], one_s.at[3], one_r.at[3], c=other)
    owe(pacts.at[:, conv_lanes], one_s.at[3])

    phase("chain2_wait")
    incoming[:, :STATES], incoming[:, STATES:] = nothing
    for d in range(1, nz):

        @pl.when(z == d)
        def _(d=d):
            arrived(chain2.at[pl.ds(0, d)], one_r.at[5])

    phase("chain2_fold")

    @pl.when(z > 0)
    def _():
        def step(k, carry):
            return joined(carry, of(chain2)(k), 3)

        incoming[:, :STATES], incoming[:, STATES:] = lax.fori_loop(0, z, step, nothing)

    state = fold((incoming[:, :STATES], incoming[:, STATES:]), of(chain1), ny, y, 2)
    for seg in range(8):
        links[seg] = state[0]
        state = joined(state, of_ends(seg), 1)
    for seg in range(8):
        links[8 + seg // 2, (seg % 2) * 4 : (seg % 2) * 4 + 4] = links[seg, 0:4]
        links[12 + seg // 2, (seg % 2) * 4 : (seg % 2) * 4 + 4] = links[seg, 4:8]
    phase("fixup")
    previous = docext[32:64]
    for cut in range(STATES // LANES):
        re, im = lane_cut(cut)
        a_re, a_im = lam[0:1, re], lam[1:2, re]
        w_re = links[8:12, :, re].reshape(32, LANES)
        w_im = links[12:16, :, re].reshape(32, LANES)
        for k in range(16):
            w_re, w_im = a_re * w_re - a_im * w_im, a_re * w_im + a_im * w_re
            reach = ones_where(docs_at(k) == previous)
            pushed[rows_at(k), re] = pushed[rows_at(k), re] + reach * w_re
            pushed[rows_at(k), im] = pushed[rows_at(k), im] + reach * w_im
    phase("readout")
    reading = halves(nt, pushed[...].astype(BF16), rmat[...]) + skip[...] * driven[...]
    inner = 0.7978845608028654 * (reading + 0.044715 * (reading * reading * reading))
    ssm_out = (0.5 * reading * (1.0 + jnp.tanh(inner))).astype(BF16)
    acts[:, LANES:] = halves(nn, unperm, ssm_out).astype(BF16)
    send(acts.at[theirs, ssm_lanes], pacts.at[:, ssm_lanes], one_s.at[4], one_r.at[4], c=other)
    owe(pacts.at[:, ssm_lanes], one_s.at[4])
    phase("ring_o3")
    for k in range(3, most // 2):
        service(2, k)
        peer_start(k + 1)

    columns = total_depth // 4

    def quarter(ref, cut):
        if nz % 4 == 0:
            return ref[cut * nz // 4 : (cut + 1) * nz // 4].reshape(columns, 2 * LANES)
        return ref[cut // 2, cut % 2]

    phase("peer_w_wait")
    arrived(wpeer, peer_r.at[0])
    for cut in (0, 2, 1, 3):
        phase(f"out_proj{cut}")
        total = nt(acts[mine, :], quarter(wall_o, cut))
        if cut == 0:
            phase("pact_wait")
            arrived(pacts.at[:, ssm_lanes], one_r.at[4])
            arrived(pacts.at[:, conv_lanes], one_r.at[3])
        total = total + nt(pacts[...], quarter(wpeer, cut))
        part[cut] = total.astype(BF16).reshape(PARTS, ROWS // 2, columns)
        way, turn = cut // 2, cut % 2
        target = (xp, xm)[way]
        send(part.at[cut, xo], relay.at[way, turn], rs_s.at[0], rs_r.at[2 * way + turn], x=target)
    for turn in range(2):
        send(part.at[2 + turn, xp], final.at[0, 2 + turn], rs_s.at[0], rs_r.at[6 + turn], x=xp)
        send(part.at[turn, xm], final.at[1, turn], rs_s.at[0], rs_r.at[4 + turn], x=xm)
    for which in range(3):
        count = sum(ring_blocks(which, k) for k in range(most // 2))
        owe(blocks_view(walls[which], count), ring_s.at[which])
    owe(blocks_view(wall_s, sum(state_blocks(ab, stage) for ab in range(2) for stage in range(2))), st_s.at[0])
    owe(wpeer, peer_s.at[0])
    settle()
    for turn in range(2):
        for way, target in ((0, xp), (1, xm)):
            phase(f"relay{way}{turn}")
            cut = 2 * way + turn
            arrived(relay.at[way, turn], rs_r.at[2 * way + turn])
            both = part[cut, target].astype(F32) + relay[way, turn].astype(F32)
            part[cut, target] = both.astype(BF16)
            send(part.at[cut, target], final.at[way, cut], rs_s.at[0], rs_r.at[4 + cut], x=target)
    for cut in (0, 2, 1, 3):
        phase(f"final{cut}")
        arrived(final.at[:, cut], rs_r.at[4 + cut])
        value = part[cut, x].astype(F32) + final[0, cut].astype(F32) + final[1, cut].astype(F32)
        out[:, cut * columns : (cut + 1) * columns] = value.astype(BF16)
    phase("drain")
    arrived(part.at[pl.ds(0, 3)], rs_s.at[0])

    for d in range(1, nz):

        @pl.when(z + d == nz - 1)
        def _(d=d):
            arrived(chain2.at[pl.ds(0, d)], one_s.at[5])

    phase(None)


def shards(
    nz, ny, tokens, documents, norm_gain, out_gate_weight, in_gate_weight, value_weight,
    conv_taps, state_in_weight, decay_rate, frequency, step_log, input_real, input_imag,
    readout_real, readout_imag, skip_gain, conv_out_weight, state_out_weight,
):
    depth = state_in_weight.shape[0]
    width = tokens.shape[1]
    columns = nz * ny * depth // 4
    vmem = pl.BlockSpec(memory_space=pltpu.VMEM)
    hbm = pl.BlockSpec(memory_space=pltpu.HBM)
    dma = pltpu.SemaphoreType.DMA
    steps = max(nz, ny) // 2
    return pl.pallas_call(
        functools.partial(mixer_kernel, nz, ny, depth),
        out_shape=jax.ShapeDtypeStruct((ROWS // 2, 4 * columns), BF16),
        in_specs=[hbm] * 18,
        out_specs=vmem,
        scratch_shapes=[
            pltpu.VMEM((2, 8, 64), F32),
            pltpu.VMEM((1, 32), F32),
            pltpu.VMEM((4, 8, 16, 64), F32),
            pltpu.VMEM((3, LANES), BF16),
            pltpu.VMEM((1, LANES), F32),
            pltpu.VMEM((8, STATES), F32),
            pltpu.VMEM((PARTS, 2, ROWS, width), BF16),
            pltpu.VMEM((2, width // LANES, LANES), BF16),
            pltpu.VMEM((2, 1, width), F32),
            pltpu.VMEM((PARTS, 1, ROWS), jnp.int32),
            pltpu.VMEM((nz, ny, depth, LANES), BF16),
            pltpu.VMEM((nz, ny, depth, 3 * LANES), BF16),
            pltpu.VMEM((nz, ny, depth, 2 * LANES), BF16),
            pltpu.VMEM((nz, ny, depth, 2 * LANES), BF16),
            pltpu.VMEM((ALL + 16 * PARTS, 2 * width), BF16),
            pltpu.VMEM((ALL, ALL), BF16),
            pltpu.VMEM((ALL, ALL), BF16),
            pltpu.VMEM((LANES, 2 * STATES), BF16),
            pltpu.VMEM((LANES, 2 * STATES), BF16),
            pltpu.VMEM((ALL, LANES), F32),
            pltpu.VMEM((ALL, 2 * STATES), F32),
            pltpu.VMEM((64 + ALL, LANES), F32),
            pltpu.VMEM((64 + ALL, LANES), F32),
            pltpu.VMEM((ALL, LANES), F32),
            pltpu.VMEM((8, 8, STATES + LANES), F32),
            pltpu.VMEM((ny, 16, STATES // 2 + LANES), BF16),
            pltpu.VMEM((nz, 16, STATES // 2 + LANES), BF16),
            pltpu.VMEM((8, STATES + LANES), F32),
            pltpu.VMEM((16, 8, STATES), F32),
            pltpu.VMEM((PARTS, 2, 16, width), BF16),
            pltpu.VMEM((PARTS, 1, ROWS), jnp.int32),
            pltpu.VMEM((16 * PARTS, LANES), F32),
            pltpu.VMEM((ALL, 2 * LANES), BF16),
            pltpu.VMEM((ALL // 2, 2 * LANES), BF16),
            pltpu.VMEM((4, PARTS, ROWS // 2, columns), BF16),
            pltpu.VMEM((2, 2, ROWS // 2, columns), BF16),
            pltpu.VMEM((2, 4, ROWS // 2, columns), BF16),
            dma((11,)),
            dma((1,)), dma((2, 3)),
            dma((1,)), dma((PARTS,)),
            dma((1,)), dma((1,)),
            dma((6,)), dma((6,)),
            dma((3,)), dma((3, 2)),
            dma((1,)), dma((2, 2)),
            dma((3,)), dma((3, steps)),
            dma((1,)), dma((1,)),
            dma((1,)), dma((8,)),
            dma((5,)), dma((5,)),
        ],
        compiler_params=pltpu.CompilerParams(
            collective_id=0, has_side_effects=True, vmem_limit_bytes=40 * 1024 * 1024
        ),
        name="mixer",
    )(*(
        pltpu.with_memory_space_constraint(operand, pltpu.HBM) for operand in (
            tokens, state_in_weight, out_gate_weight, in_gate_weight, value_weight, conv_out_weight.T,
            state_out_weight.T, documents[None, :], norm_gain.reshape(-1, LANES), decay_rate, frequency,
            step_log[None, :], input_real.transpose(0, 2, 1), input_imag.transpose(0, 2, 1),
            readout_real, readout_imag, conv_taps, skip_gain[None, :],
        )
    ))


def solution(mesh, nz=8, ny=8):
    torus = Mesh(
        mesh.devices.reshape(nz, ny, mesh.shape["fs"], mesh.shape["tp"]), ("sp_0", "sp_1", "fs", "tp")
    )
    in_specs = (
        P(FS_SP, "tp"),
        P(FS_SP),
        P("tp"),
        P(SP, "tp"),
        P(SP, "tp"),
        P(SP, "tp"),
        P(None, "tp"),
        P(SP, "tp"),
        P("tp", None),
        P("tp", None),
        P("tp"),
        P("tp", None, None),
        P("tp", None, None),
        P("tp", None, None),
        P("tp", None, None),
        P("tp"),
        P("tp", SP),
        P("tp", SP),
    )
    return jax.shard_map(
        functools.partial(shards, nz, ny), mesh=torus, in_specs=in_specs,
        out_specs=P(FS_SP_TP, None), check_vma=False,
    )
```
